32 devices in a mesh: grp: 2 (over x), sp: 4 (over y, core), tp: 4 (over z).
Axes of the slice: x: 2, y: 2, z: 4, core: 2. Of those that a mesh axis runs over, the one named last changes fastest.
Arguments:
- resid_in: bfloat16 [4096, 2048], P(('grp', 'sp', 'tp')), parts along dimension 0, may hold values from -6 to 6
- pool_input: bfloat16 [4096, 1024], P(('grp', 'sp'), 'tp'), parts along dimension 0, may hold values from -6 to 6
- pool_weight: bfloat16 [4, 256, 256], replicated, may hold values from -0.375 to 0.375
- pool_scale: float32 [1024], replicated, may hold values from 0.2 to 0.8
- out_weight: bfloat16 [1024, 2048], replicated, may hold values from -0.1875 to 0.1875
- mix_gain: float32 [2048], replicated, may hold values from 0.1 to 1.9
- ffn_gain: float32 [2048], replicated, may hold values from 0.1 to 1.9
- w_gate: bfloat16 [32, 2048, 1024], P('sp', None, 'tp'), may hold values from -0.375 to 0.375
- w_up: bfloat16 [32, 2048, 1024], P('sp', None, 'tp'), may hold values from -0.375 to 0.375
- w_down: bfloat16 [32, 1024, 2048], P('sp', 'tp'), may hold values from -0.1875 to 0.1875
- routes: int32 [4096, 2], P(('grp', 'sp', 'tp')), parts along dimension 0, may hold values from 0 to 31, all different within a row; in each aligned block of 128 rows (0 to 127, 128 to 255, ...) at most 9 rows name the same one
- route_weight: float32 [4096, 2], P(('grp', 'sp', 'tp')), parts along dimension 0, may hold values from 0.1 to 1
- post_gain: float32 [2048], replicated, may hold values from 0.1 to 1.9
Outputs:
- layer_out: bfloat16 [4096, 2048], P(('grp', 'sp', 'tp')), parts along dimension 0
The draws below stay inside these ranges and needn't reach their ends.
There are 2 independent parts, one for each index of `grp`. The reference program is written for one: setup_inputs(seed, part) draws one part's arguments, and reference() takes and returns one part's arrays. A program takes and returns all parts, laid end to end along the dimension named above; an argument that names none is the same for every part. Nothing has to cross between parts.
Inputs may be any that keep to these rules, and one draw needn't show every extreme that they name: `routes`: each row names 2 different experts. The rows of one device name any one expert at most 9 times, and in every draw some device's rows name some expert exactly 9 times.
All inputs are finite; a program needn't handle non-finite values.
Results may differ from the reference program's by a relative error of at most 0.011.
Values may be sent and summed in bfloat16 or wider, within the bound.
No kernel may reach another device: no remote copies, remote signals or barrier semaphores. Data moves between devices by JAX's collectives and lax.ppermute only.
A program may use at most 128 MiB of HBM per device.

```python
import math
import jax
import jax.numpy as jnp
import numpy as np
from jax import lax

D = 2048
POOL_WIDTH = 1024
GROUPS = 4
GROUP_DIM = 256
FF = 1024
EXPERTS = 32
TOP = 2
TOK_DEV = 128
CAP = 9
SEQ = 2048
N_TP = 4


def shard_levels(key, shape, cuts, smallest, high):
    gain, own = 1.0, jax.random.fold_in(key, 6)
    for axis_at, shards_of in cuts:
        draws = jnp.exp(jax.random.uniform(jax.random.fold_in(own, axis_at), (shards_of,), jnp.float32, smallest / len(cuts), high / len(cuts)))
        gain = gain * jnp.repeat(draws, shape[axis_at] // shards_of).reshape([-1 if axis == axis_at else 1 for axis in range(len(shape))])
    return gain


def assign_block(own_key, own, number, rows, number_of, top, bound, skew):
    order = jax.random.permutation(own_key, number_of)
    packed, ordinary = shares(number_of, rows * top, bound, skew, True), shares(number_of, rows * top, bound, skew, False)
    places = jnp.arange(number_of)

    def named(sizes, offset_by):
        used = int((sizes > 0).sum())
        fixed = max(1, used // 4)
        passed = fixed + (places - fixed + offset_by * (used - fixed)) % max(1, number_of - fixed)
        return jnp.zeros((number_of,), jnp.int32).at[order[jnp.where(places < fixed, places, passed)]].set(jnp.asarray(sizes, jnp.int32))

    sizes = jnp.where(number % 4 == 0, named(packed, number // 4), named(ordinary, number - number // 4 - 1))
    mixed = jax.random.permutation(jax.random.fold_in(own, 3), number_of)
    source_of, sink = mixed[0:number_of // 2 * 2:2], mixed[1:number_of // 2 * 2:2]
    margin = jnp.minimum(sizes[source_of] - 1, bound - sizes[sink]) // 2
    margin = jnp.where((source_of == order[0]) | (sink == order[0]) | (sizes[sink] == 0), 0, jnp.maximum(margin, 0))
    passed = jax.random.randint(jax.random.fold_in(own, 4), (number_of // 2,), 0, 1 << 20) % (margin + 1)
    sizes = sizes.at[source_of].add(-passed).at[sink].add(passed)
    labels = jnp.searchsorted(jnp.cumsum(sizes), jnp.arange(rows * top), side="right").astype(jnp.int32)
    listing = labels.reshape(top, rows).T
    listing = listing[jax.random.permutation(jax.random.fold_in(own, 1), rows)]
    offset_by = jax.random.randint(jax.random.fold_in(own, 2), (rows, 1), 0, top)
    return jnp.take_along_axis(listing, (jnp.arange(top)[None, :] + offset_by) % top, axis=1)


def shares(count, total, limit, slope, full):
    portions = [(1 << 20) // math.isqrt(standing ** slope) + 1 for standing in range(1, count + 1)]
    largest = limit if full else min(limit, max(-(-total // count), total * portions[0] // sum(portions)))
    least = 1 if total - largest >= count - 1 else 0
    given, surplus = [largest] + [least] * (count - 1), total - largest - least * (count - 1)
    while surplus > 0:
        candidates = [i for i in range(1, count) if given[i] < largest] or [i for i in range(1, count) if given[i] < limit]
        pool, budget = sum([portions[i] for i in candidates]), surplus
        for i in candidates:
            more = min(limit - given[i], max(1, budget * portions[i] // pool), surplus)
            given[i] = given[i] + more
            surplus = surplus - more
    return np.array(given)


def gaussian(stream_key, extent, width, limit, split=(), kind=jnp.bfloat16):
    gain = shard_levels(stream_key, extent, split, -0.22, 0.18) if split else 1.0
    array = jax.random.normal(stream_key, extent, jnp.float32) * width * gain
    return jnp.minimum(jnp.maximum(array, -limit), limit).astype(kind)


def setup_inputs(seed: int = 0, part: int = 0) -> dict:
    seeds = jax.random.split(jax.random.key(seed), 14)
    own_keys = jax.random.split(jax.random.fold_in(seeds[13], part), 14)
    resid_in = gaussian(own_keys[0], (SEQ, D), 1.0, 6.0, ((0, 16),))
    pool_input = gaussian(own_keys[1], (SEQ, POOL_WIDTH), 1.0, 6.0, ((0, 4), (1, 4)))
    pool_weight = gaussian(seeds[2], (GROUPS, GROUP_DIM, GROUP_DIM), GROUP_DIM ** -0.5, 0.375)
    pool_scale = jnp.clip(jax.random.uniform(seeds[3], (POOL_WIDTH,), jnp.float32, 0.2, 0.8), 0.2, 0.8)
    out_weight = gaussian(seeds[4], (POOL_WIDTH, D), POOL_WIDTH ** -0.5, 0.1875)
    mix_gain = jnp.clip(1.0 + 0.18 * jax.random.normal(seeds[5], (D,), jnp.float32), 0.1, 1.9)
    ffn_gain = jnp.clip(1.0 + 0.18 * jax.random.normal(seeds[6], (D,), jnp.float32), 0.1, 1.9)
    w_gate = gaussian(seeds[7], (EXPERTS, D, FF), (D // 8) ** -0.5, 0.375, ((0, 4), (2, 4)))
    w_up = gaussian(seeds[8], (EXPERTS, D, FF), (D // 8) ** -0.5, 0.375, ((0, 4), (2, 4)))
    w_down = gaussian(seeds[9], (EXPERTS, FF, D), FF ** -0.5, 0.1875, ((0, 4), (1, 4)))
    routes_keys = jax.random.split(jax.random.fold_in(own_keys[10], 1), SEQ // TOK_DEV)
    routes_turns = jax.random.permutation(jax.random.fold_in(own_keys[10], 3), SEQ // TOK_DEV)
    routes = jax.vmap(lambda own, number: assign_block(jax.random.fold_in(own_keys[10], 2), own, number, TOK_DEV, EXPERTS, TOP, CAP, 1))(routes_keys, routes_turns).reshape((SEQ, TOP))
    route_weight = jnp.clip(jnp.exp(math.log(1.0) - 2.3025851 * jax.random.uniform(own_keys[11], (SEQ, TOP), jnp.float32) ** shard_levels(own_keys[11], (SEQ, TOP), ((0, 16),), -0.2, 0.2)), 0.1, 1.0)
    post_gain = jnp.clip(1.0 + 0.18 * jax.random.normal(seeds[12], (D,), jnp.float32), 0.1, 1.9)
    return {"resid_in": resid_in, "pool_input": pool_input, "pool_weight": pool_weight, "pool_scale": pool_scale, "out_weight": out_weight, "mix_gain": mix_gain, "ffn_gain": ffn_gain, "w_gate": w_gate, "w_up": w_up, "w_down": w_down, "routes": routes, "route_weight": route_weight, "post_gain": post_gain}


pool_windows = (2, 4, 8, 16)
reach_back = 15
norm_eps = 1e-06
clamp_limit = 7.0
glu_alpha = 1.702

def rms_scale(values, gain_vec):
    inverse = lax.rsqrt(lax.optimization_barrier(jnp.mean(values * values, axis=-1, keepdims=True)) + norm_eps)
    return values * inverse * gain_vec

def clamped_unit(gate_pre, upward):
    gate_clip = jnp.minimum(gate_pre, clamp_limit)
    linear = jnp.clip(upward, -clamp_limit, clamp_limit)
    return gate_clip * jax.nn.sigmoid(glu_alpha * gate_clip) * (linear + 1.0)

def reference(resid_in, pool_input, pool_weight, pool_scale, out_weight, mix_gain, ffn_gain, w_gate, w_up, w_down, routes, route_weight, post_gain):
    source = pool_input.astype(jnp.float32)
    positions = jnp.arange(SEQ, dtype=jnp.int32)
    pieces = []
    for group_level, win_len in enumerate(pool_windows):
        group_cols = source[:, group_level * GROUP_DIM:(group_level + 1) * GROUP_DIM]
        padded = jnp.concatenate([jnp.zeros((reach_back, GROUP_DIM), jnp.float32), group_cols], axis=0)
        running = jnp.zeros((SEQ, GROUP_DIM), jnp.float32)
        for offset in range(win_len):
            running = running + padded[reach_back - offset:reach_back - offset + SEQ]
        divisor = jnp.minimum(positions + 1, win_len).astype(jnp.float32)[:, None]
        pieces.append(running / divisor - group_cols)
    mixed_rows = jnp.concatenate(pieces, axis=1).astype(jnp.bfloat16)
    pooled = jnp.einsum('tgc,gcd->tgd', mixed_rows.reshape(SEQ, GROUPS, GROUP_DIM).astype(jnp.float32), pool_weight.astype(jnp.float32))
    pooled = (pooled * pool_scale.reshape(GROUPS, GROUP_DIM)).astype(jnp.bfloat16).reshape(SEQ, POOL_WIDTH)
    mix_out = jnp.dot(pooled, out_weight, preferred_element_type=jnp.float32)
    residual = (resid_in.astype(jnp.float32) + rms_scale(mix_out, mix_gain)).astype(jnp.bfloat16)
    normed = rms_scale(residual.astype(jnp.float32), ffn_gain).astype(jnp.bfloat16)
    flat_route = routes.reshape(-1).astype(jnp.int32)
    total = SEQ * TOP
    sort_order = jnp.argsort(flat_route, stable=True).astype(jnp.int32)
    token_of = (sort_order // TOP).astype(jnp.int32)
    counts = lax.optimization_barrier(jnp.sum((flat_route[:, None] == jnp.arange(EXPERTS, dtype=jnp.int32)[None, :]).astype(jnp.int32), axis=0))
    starts = (jnp.cumsum(counts) - counts).astype(jnp.int32)
    most_rows = SEQ // TOK_DEV * CAP
    block_ff = FF // N_TP

    def one_expert(expert):
        row_index = jnp.minimum(starts[expert] + jnp.arange(most_rows, dtype=jnp.int32), total - 1)
        taken_rows = normed[token_of[row_index]]
        gate_pre = jnp.dot(taken_rows, w_gate[expert], preferred_element_type=jnp.float32)
        upward = jnp.dot(taken_rows, w_up[expert], preferred_element_type=jnp.float32)
        activated = clamped_unit(gate_pre, upward).astype(jnp.bfloat16)
        partials = jnp.einsum('rnf,nfd->rnd', activated.reshape(most_rows, N_TP, block_ff).astype(jnp.float32), w_down[expert].reshape(N_TP, block_ff, D).astype(jnp.float32))
        partials = lax.optimization_barrier(partials.astype(jnp.bfloat16))
        return lax.optimization_barrier(jnp.sum(partials.astype(jnp.float32), axis=1)).astype(jnp.bfloat16)
    expert_outs = lax.map(one_expert, jnp.arange(EXPERTS, dtype=jnp.int32))
    sorted_e = flat_route[sort_order]
    local_pos = (jnp.arange(total, dtype=jnp.int32) - starts[sorted_e]).astype(jnp.int32)
    picked = expert_outs[sorted_e, local_pos]
    assigned = jnp.zeros((total, D), jnp.bfloat16).at[sort_order].set(picked)
    expert_mix = lax.optimization_barrier(jnp.sum(assigned.reshape(SEQ, TOP, D).astype(jnp.float32) * route_weight[:, :, None], axis=1))
    return (residual.astype(jnp.float32) + rms_scale(expert_mix, post_gain)).astype(jnp.bfloat16)
```

```python
import jax
import jax.numpy as jnp
from jax import lax
from jax.sharding import PartitionSpec as P

GROUPS = 4
GROUP_DIM = 256
TOP = 2
CAP = 9


pool_windows = (2, 4, 8, 16)
reach_back = 15
norm_eps = 1e-06
clamp_limit = 7.0
glu_alpha = 1.702


def passed_along(x, axis, by):
    size = lax.axis_size(axis)
    pairs = [(i, i + by) for i in range(size) if 0 <= i + by < size]
    return lax.ppermute(x, axis, pairs)


def rotated(x, axis, by):
    size = lax.axis_size(axis)
    return lax.ppermute(x, axis, [(i, (i + by) % size) for i in range(size)])


def rms_scale(values, gain_vec):
    inverse = lax.rsqrt(jnp.mean(values * values, axis=-1, keepdims=True) + norm_eps)
    return values * inverse * gain_vec


def clamped_unit(gate_pre, upward):
    gate_clip = jnp.minimum(gate_pre, clamp_limit)
    linear = jnp.clip(upward, -clamp_limit, clamp_limit)
    return gate_clip * jax.nn.sigmoid(glu_alpha * gate_clip) * (linear + 1.0)


def mixed_window(pool_input):
    seg_rows, channels = pool_input.shape
    last_rows = pool_input[seg_rows - reach_back :]
    before = passed_along(last_rows, "sp", 1)
    extended = jnp.concatenate([before, pool_input], axis=0).astype(jnp.float32)
    first_chan = lax.axis_index("tp") * channels
    chan_group = (first_chan + lax.iota(jnp.int32, channels)) // GROUP_DIM
    positions = lax.axis_index("sp") * seg_rows + lax.iota(jnp.int32, seg_rows)
    window = jnp.zeros((channels,), jnp.int32)
    for group_level, win_len in enumerate(pool_windows):
        window = jnp.where(chan_group == group_level, win_len, window)
    running = jnp.zeros((seg_rows, channels), jnp.float32)
    window_sum = running
    for offset in range(pool_windows[-1]):
        running = running + extended[reach_back - offset : reach_back - offset + seg_rows]
        if offset + 1 in pool_windows:
            window_sum = jnp.where(window[None, :] == offset + 1, running, window_sum)
    divisor = jnp.minimum(positions[:, None] + 1, window[None, :]).astype(jnp.float32)
    return (window_sum / divisor - extended[reach_back:]).astype(jnp.bfloat16)


def per_device(
    resid_in,
    pool_input,
    pool_weight,
    pool_scale,
    out_weight,
    mix_gain,
    ffn_gain,
    w_gate,
    w_up,
    w_down,
    routes,
    route_weight,
    post_gain,
):
    n_sp = lax.axis_size("sp")
    n_tp = lax.axis_size("tp")
    tok_rows, width = resid_in.shape
    channels = pool_input.shape[1]
    local_experts = w_gate.shape[0]
    n_experts = local_experts * n_sp
    assert n_experts <= 256
    slot_rows = local_experts * CAP
    slot_total = n_sp * slot_rows

    fields = jnp.concatenate([routes.astype(jnp.bfloat16).T, route_weight.astype(jnp.bfloat16).T])
    n_fields = fields.size
    field_rows = -(-n_fields // (8 * channels)) * 8
    fields = jnp.pad(fields.reshape(-1), (0, field_rows * channels - n_fields))
    fields = jnp.broadcast_to(fields.reshape(1, field_rows, channels), (n_tp, field_rows, channels))
    mixed_rows = mixed_window(pool_input).reshape(n_tp, tok_rows, channels)
    sent = jnp.concatenate([mixed_rows, fields], axis=1)
    got = lax.all_to_all(sent, "tp", split_axis=0, concat_axis=0, tiled=True)
    token_mixed = got[:, :tok_rows].transpose(1, 0, 2).reshape(tok_rows, n_tp * channels)
    fields = got[:, tok_rows:].reshape(n_tp, -1)[:, :n_fields].reshape(n_tp, 2 * TOP, tok_rows)

    pooled = jnp.einsum(
        "tgc,gcd->tgd",
        token_mixed.reshape(tok_rows, GROUPS, GROUP_DIM),
        pool_weight,
        preferred_element_type=jnp.float32,
    )
    pooled = (
        (pooled * pool_scale.reshape(GROUPS, GROUP_DIM)).astype(jnp.bfloat16).reshape(tok_rows, -1)
    )
    mix_out = jnp.dot(pooled, out_weight, preferred_element_type=jnp.float32)
    residual = (resid_in.astype(jnp.float32) + rms_scale(mix_out, mix_gain)).astype(jnp.bfloat16)
    normed = rms_scale(residual.astype(jnp.float32), ffn_gain).astype(jnp.bfloat16)

    order = [0] + [k for pair in zip(range(1, n_tp), range(n_tp - 1, 0, -1)) for k in pair]
    order = list(dict.fromkeys(order))
    blocks = {k: rotated(normed, "tp", k) if k else normed for k in order}

    here = lax.axis_index("tp")
    fields = jnp.take(fields, (here - jnp.array(order)) % n_tp, axis=0)
    route = fields[:, :TOP].astype(jnp.int32)
    weight = fields[:, TOP:].astype(jnp.float32)
    onehot = route[..., None] == lax.iota(jnp.int32, n_experts)
    named = jnp.sum(onehot.astype(jnp.float32), axis=1)
    earlier = lax.iota(jnp.int32, tok_rows)[:, None] > lax.iota(jnp.int32, tok_rows)[None, :]
    rank = jnp.einsum(
        "ut,bte->bue",
        earlier.astype(jnp.bfloat16),
        named.astype(jnp.bfloat16),
        preferred_element_type=jnp.float32,
    )
    slot_rank = jnp.sum(rank[:, None] * onehot, axis=-1).astype(jnp.int32)
    slot_index = route * CAP + slot_rank
    picker = slot_index[..., None] == lax.iota(jnp.int32, slot_total)
    token_pick = jnp.sum(picker.astype(jnp.float32), axis=1).astype(jnp.bfloat16)
    token_weight = jnp.sum(jnp.where(picker, weight[..., None], 0.0), axis=1).astype(jnp.bfloat16)

    arrived = []
    for at, k in enumerate(order):
        rows = lax.dot_general(
            token_pick[at], blocks[k], (((0,), (0,)), ((), ())), preferred_element_type=jnp.float32
        )
        rows = rows.astype(jnp.bfloat16).reshape(n_sp, slot_rows, width)
        arrived.append(lax.all_to_all(rows, "sp", split_axis=0, concat_axis=0, tiled=True))
    arrived = jnp.stack(arrived).reshape(n_tp, n_sp, local_experts, CAP, width)
    gate_pre = jnp.einsum("sklcd,ldf->sklcf", arrived, w_gate, preferred_element_type=jnp.float32)
    upward = jnp.einsum("sklcd,ldf->sklcf", arrived, w_up, preferred_element_type=jnp.float32)
    activated = clamped_unit(gate_pre, upward).astype(jnp.bfloat16)
    terms = jnp.einsum("sklcf,lfd->sklcd", activated, w_down, preferred_element_type=jnp.float32)
    terms = terms.astype(jnp.bfloat16).reshape(n_tp, n_sp, slot_rows, width)

    parts = {}
    for at, k in reversed(list(enumerate(order))):
        back = lax.all_to_all(terms[at], "sp", split_axis=0, concat_axis=0, tiled=True)
        part = jnp.dot(
            token_weight[at], back.reshape(slot_total, width), preferred_element_type=jnp.float32
        )
        parts[k] = rotated(part.astype(jnp.bfloat16), "tp", -k).astype(jnp.float32) if k else part
    expert_mix = sum(parts[k] for k in reversed(order))
    return (residual.astype(jnp.float32) + rms_scale(expert_mix, post_gain)).astype(jnp.bfloat16)


def solution(mesh):
    in_specs = (
        P(("grp", "sp", "tp"), None),
        P(("grp", "sp"), "tp"),
        P(),
        P(),
        P(),
        P(),
        P(),
        P("sp", None, "tp"),
        P("sp", None, "tp"),
        P("sp", "tp", None),
        P(("grp", "sp", "tp"), None),
        P(("grp", "sp", "tp"), None),
        P(),
    )
    out_specs = P(("grp", "sp", "tp"), None)
    return jax.shard_map(
        per_device, mesh=mesh, in_specs=in_specs, out_specs=out_specs, check_vma=False
    )
```

```python
import jax
import jax.numpy as jnp
from jax import lax
from jax.experimental import pallas as pl
from jax.experimental.pallas import tpu as pltpu
from jax.sharding import PartitionSpec as P

GROUPS = 4
GROUP_DIM = 256
TOP = 2
CAP = 9


pool_windows = (2, 4, 8, 16)
reach_back = 15
norm_eps = 1e-06
clamp_limit = 7.0
glu_alpha = 1.702


def passed_along(x, axis, by):
    size = lax.axis_size(axis)
    pairs = [(i, i + by) for i in range(size) if 0 <= i + by < size]
    return lax.ppermute(x, axis, pairs)


def rotated(x, axis, by):
    size = lax.axis_size(axis)
    return lax.ppermute(x, axis, [(i, (i + by) % size) for i in range(size)])


def rms_scale(values, gain_vec):
    inverse = lax.rsqrt(jnp.mean(values * values, axis=-1, keepdims=True) + norm_eps)
    return values * inverse * gain_vec


def clamped_unit(gate_pre, upward):
    gate_clip = jnp.minimum(gate_pre, clamp_limit)
    linear = jnp.clip(upward, -clamp_limit, clamp_limit)
    return gate_clip * jax.nn.sigmoid(glu_alpha * gate_clip) * (linear + 1.0)


def mixed_window(pool_input):
    seg_rows, channels = pool_input.shape
    last_rows = pool_input[seg_rows - reach_back :]
    before = passed_along(last_rows, "sp", 1)
    extended = jnp.concatenate([before, pool_input], axis=0).astype(jnp.float32)
    first_chan = lax.axis_index("tp") * channels
    chan_group = (first_chan + lax.iota(jnp.int32, channels)) // GROUP_DIM
    positions = lax.axis_index("sp") * seg_rows + lax.iota(jnp.int32, seg_rows)
    window = jnp.zeros((channels,), jnp.int32)
    for group_level, win_len in enumerate(pool_windows):
        window = jnp.where(chan_group == group_level, win_len, window)
    running = jnp.zeros((seg_rows, channels), jnp.float32)
    window_sum = running
    for offset in range(pool_windows[-1]):
        running = running + extended[reach_back - offset : reach_back - offset + seg_rows]
        if offset + 1 in pool_windows:
            window_sum = jnp.where(window[None, :] == offset + 1, running, window_sum)
    divisor = jnp.minimum(positions[:, None] + 1, window[None, :]).astype(jnp.float32)
    return (window_sum / divisor - extended[reach_back:]).astype(jnp.bfloat16)


def reached(i, d, n):
    return i ^ d if n & (n - 1) == 0 else (i + d) % n


def offset_to(target, i, n):
    return target ^ i if n & (n - 1) == 0 else (target - i) % n


def moved(x, axis, d, back=False):
    size = lax.axis_size(axis)
    pairs = [(i, reached(i, d, size)) for i in range(size)]
    return lax.ppermute(x, axis, [(b, a) for a, b in pairs] if back else pairs)


def pick_body(slot, block, *outs):
    rows = outs[0].shape[0]
    for d, out in enumerate(outs):
        ids = lax.broadcasted_iota(jnp.int32, (rows, slot.shape[1]), 0) + d * rows
        hit = ids == slot[0:1, :]
        for k in range(1, slot.shape[0]):
            hit = hit | (ids == slot[k : k + 1, :])
        chosen = jnp.where(hit, 1.0, 0.0).astype(jnp.bfloat16)
        out[...] = jnp.dot(chosen, block[...], preferred_element_type=jnp.float32).astype(out.dtype)


def pick(slot, block, n_sp, slot_rows):
    shape = jax.ShapeDtypeStruct((slot_rows, block.shape[1]), block.dtype)
    return pl.pallas_call(pick_body, out_shape=[shape] * n_sp, name="pick")(slot, block)


def combine_body(slot, weight, *refs):
    backs, out = refs[:-1], refs[-1]
    rows = backs[0].shape[0]
    total = None
    for d, back in enumerate(backs):
        ids = lax.broadcasted_iota(jnp.int32, (slot.shape[0], rows), 1) + d * rows
        share = jnp.zeros((slot.shape[0], rows), jnp.float32)
        for k in range(slot.shape[1]):
            share = share + jnp.where(ids == slot[:, k : k + 1], weight[:, k : k + 1], 0.0)
        term = jnp.dot(share.astype(jnp.bfloat16), back[...], preferred_element_type=jnp.float32)
        total = term if total is None else total + term
    out[...] = total.astype(out.dtype)


def combine(slot, weight, backs):
    shape = jax.ShapeDtypeStruct((slot.shape[0], backs[0].shape[1]), jnp.bfloat16)
    return pl.pallas_call(combine_body, out_shape=shape, name="combine")(slot, weight, *backs)


LANES = 128


def experts_body(n_src, count, *refs):
    xs, (wg, wu, wd) = refs[:n_src], refs[n_src : n_src + 3]
    outs, (into, outof) = refs[n_src + 3 : 2 * n_src + 3], refs[2 * n_src + 3 :]
    rows, width = xs[0].shape
    total = n_src * rows // count
    step = pl.program_id(0)
    tiles = width // LANES

    @pl.when(step == 0)
    def _():
        for s, x in enumerate(xs):
            for j in range(tiles):
                into[j, s * rows : (s + 1) * rows, :] = x[:, j * LANES : (j + 1) * LANES].astype(
                    jnp.float32
                )

    own = pl.ds(step, total, stride=count)
    taken = jnp.concatenate([into[j, own, :].astype(jnp.bfloat16) for j in range(tiles)], axis=1)
    gate_pre = jnp.dot(taken, wg[0], preferred_element_type=jnp.float32)
    upward = jnp.dot(taken, wu[0], preferred_element_type=jnp.float32)
    activated = clamped_unit(gate_pre, upward).astype(jnp.bfloat16)
    result = jnp.dot(activated, wd[0], preferred_element_type=jnp.float32)
    for j in range(tiles):
        outof[j, own, :] = result[:, j * LANES : (j + 1) * LANES]

    @pl.when(step == count - 1)
    def _():
        for s, out in enumerate(outs):
            for j in range(tiles):
                out[:, j * LANES : (j + 1) * LANES] = outof[
                    j, s * rows : (s + 1) * rows, :
                ].astype(out.dtype)


def experts(xs, w_gate, w_up, w_down):
    count, width, hidden = w_gate.shape
    rows, n_src = xs[0].shape[0], len(xs)
    whole = pl.BlockSpec((rows, width), lambda e: (0, 0))
    scratch = pltpu.VMEM((width // LANES, n_src * rows, LANES), jnp.float32)
    flops = 6 * n_src * rows * width * hidden
    moved_bytes = 3 * count * width * hidden * 2 + 4 * n_src * rows * width
    return pl.pallas_call(
        lambda *refs: experts_body(n_src, count, *refs),
        grid=(count,),
        in_specs=[whole] * n_src
        + [
            pl.BlockSpec((1, width, hidden), lambda e: (e, 0, 0)),
            pl.BlockSpec((1, width, hidden), lambda e: (e, 0, 0)),
            pl.BlockSpec((1, hidden, width), lambda e: (e, 0, 0)),
        ],
        out_specs=[whole] * n_src,
        out_shape=[jax.ShapeDtypeStruct((rows, width), jnp.bfloat16)] * n_src,
        scratch_shapes=[scratch, scratch],
        cost_estimate=pl.CostEstimate(flops=flops, bytes_accessed=moved_bytes, transcendentals=0),
        name="experts",
    )(*xs, w_gate, w_up, w_down)


def per_device(
    resid_in,
    pool_input,
    pool_weight,
    pool_scale,
    out_weight,
    mix_gain,
    ffn_gain,
    w_gate,
    w_up,
    w_down,
    routes,
    route_weight,
    post_gain,
):
    n_sp = lax.axis_size("sp")
    n_tp = lax.axis_size("tp")
    tok_rows, width = resid_in.shape
    channels = pool_input.shape[1]
    local_experts = w_gate.shape[0]
    n_experts = local_experts * n_sp
    assert n_experts <= 256
    slot_rows = local_experts * CAP
    slot_total = n_sp * slot_rows

    fields = jnp.concatenate([routes.astype(jnp.bfloat16).T, route_weight.astype(jnp.bfloat16).T])
    n_fields = fields.size
    field_rows = -(-n_fields // (8 * channels)) * 8
    fields = jnp.pad(fields.reshape(-1), (0, field_rows * channels - n_fields))
    fields = jnp.broadcast_to(fields.reshape(1, field_rows, channels), (n_tp, field_rows, channels))
    mixed_rows = mixed_window(pool_input).reshape(n_tp, tok_rows, channels)
    sent = jnp.concatenate([mixed_rows, fields], axis=1)
    got = lax.all_to_all(sent, "tp", split_axis=0, concat_axis=0, tiled=True)
    token_mixed = got[:, :tok_rows].transpose(1, 0, 2).reshape(tok_rows, n_tp * channels)
    fields = got[:, tok_rows:].reshape(n_tp, -1)[:, :n_fields].reshape(n_tp, 2 * TOP, tok_rows)

    pooled = jnp.einsum(
        "tgc,gcd->tgd",
        token_mixed.reshape(tok_rows, GROUPS, GROUP_DIM),
        pool_weight,
        preferred_element_type=jnp.float32,
    )
    pooled = (
        (pooled * pool_scale.reshape(GROUPS, GROUP_DIM)).astype(jnp.bfloat16).reshape(tok_rows, -1)
    )
    mix_out = jnp.dot(pooled, out_weight, preferred_element_type=jnp.float32)
    residual = (resid_in.astype(jnp.float32) + rms_scale(mix_out, mix_gain)).astype(jnp.bfloat16)
    normed = rms_scale(residual.astype(jnp.float32), ffn_gain).astype(jnp.bfloat16)

    half = n_tp // 2
    order = [0, half] + [k for i in range(1, half) for k in (i, n_tp - i)] if half else [0]
    order = list(dict.fromkeys(order))
    blocks = {k: rotated(normed, "tp", k) if k else normed for k in order}

    here = lax.axis_index("tp")
    sp_here = lax.axis_index("sp")
    fields = jnp.take(fields, (here - jnp.array(order)) % n_tp, axis=0)
    route = fields[:, :TOP].astype(jnp.int32)
    weight = fields[:, TOP:].astype(jnp.float32)
    onehot = route[..., None] == lax.iota(jnp.int32, n_experts)
    named = jnp.sum(onehot.astype(jnp.float32), axis=1)
    earlier = lax.iota(jnp.int32, tok_rows)[:, None] > lax.iota(jnp.int32, tok_rows)[None, :]
    rank = jnp.einsum(
        "ut,bte->bue",
        earlier.astype(jnp.bfloat16),
        named.astype(jnp.bfloat16),
        preferred_element_type=jnp.float32,
    )
    slot_rank = jnp.sum(rank[:, None] * onehot, axis=-1).astype(jnp.int32)

    if slot_rows % 8 == 0 and n_sp <= 4:
        owner = route // local_experts
        slot = (offset_to(owner, sp_here, n_sp) * CAP + slot_rank) * local_experts
        slot = slot + route % local_experts
        by_row = slot.transpose(0, 2, 1)
        weight = weight.transpose(0, 2, 1)
        arrived = []
        for at, k in enumerate(order):
            rows = pick(slot[at], blocks[k], n_sp, slot_rows)
            arrived.append([moved(x, "sp", d) if d else x for d, x in enumerate(rows)])
        size = max(1, n_tp // 2)
        parts = {}
        for first in range(0, n_tp, size):
            group = arrived[first : first + size]
            terms = experts([x for xs in group for x in xs], w_gate, w_up, w_down)
            for at in range(first, first + size):
                k = order[at]
                back = terms[(at - first) * n_sp : (at - first + 1) * n_sp]
                back = [moved(x, "sp", d, True) if d else x for d, x in enumerate(back)]
                part = combine(by_row[at], weight[at], back)
                parts[k] = rotated(part, "tp", -k) if k else part
    else:
        slot_index = route * CAP + slot_rank
        picker = slot_index[..., None] == lax.iota(jnp.int32, slot_total)
        token_pick = jnp.sum(picker.astype(jnp.float32), axis=1).astype(jnp.bfloat16)
        token_weight = jnp.sum(jnp.where(picker, weight[..., None], 0.0), axis=1)
        token_weight = token_weight.astype(jnp.bfloat16)
        arrived = []
        for at, k in enumerate(order):
            rows = lax.dot_general(
                token_pick[at],
                blocks[k],
                (((0,), (0,)), ((), ())),
                preferred_element_type=jnp.float32,
            )
            rows = rows.astype(jnp.bfloat16).reshape(n_sp, slot_rows, width)
            arrived.append(lax.all_to_all(rows, "sp", split_axis=0, concat_axis=0, tiled=True))
        arrived = jnp.stack(arrived).reshape(n_tp, n_sp, local_experts, CAP, width)
        f32 = {"preferred_element_type": jnp.float32}
        gate_pre = jnp.einsum("sklcd,ldf->sklcf", arrived, w_gate, **f32)
        upward = jnp.einsum("sklcd,ldf->sklcf", arrived, w_up, **f32)
        activated = clamped_unit(gate_pre, upward).astype(jnp.bfloat16)
        terms = jnp.einsum("sklcf,lfd->sklcd", activated, w_down, **f32)
        terms = terms.astype(jnp.bfloat16).reshape(n_tp, n_sp, slot_rows, width)
        parts = {}
        for at, k in enumerate(order):
            back = lax.all_to_all(terms[at], "sp", split_axis=0, concat_axis=0, tiled=True)
            part = jnp.dot(token_weight[at], back.reshape(slot_total, width), **f32)
            part = part.astype(jnp.bfloat16)
            parts[k] = rotated(part, "tp", -k) if k else part
    expert_mix = sum(parts[k].astype(jnp.float32) for k in order)
    return (residual.astype(jnp.float32) + rms_scale(expert_mix, post_gain)).astype(jnp.bfloat16)


def solution(mesh):
    in_specs = (
        P(("grp", "sp", "tp"), None),
        P(("grp", "sp"), "tp"),
        P(),
        P(),
        P(),
        P(),
        P(),
        P("sp", None, "tp"),
        P("sp", None, "tp"),
        P("sp", "tp", None),
        P(("grp", "sp", "tp"), None),
        P(("grp", "sp", "tp"), None),
        P(),
    )
    out_specs = P(("grp", "sp", "tp"), None)
    return jax.shard_map(
        per_device, mesh=mesh, in_specs=in_specs, out_specs=out_specs, check_vma=False
    )
```

```python
import jax
import jax.numpy as jnp
from jax import lax
from jax.experimental import pallas as pl
from jax.experimental.pallas import tpu as pltpu
from jax.sharding import PartitionSpec as P


GROUPS = 4
GROUP_DIM = 256
TOP = 2
CAP = 9


pool_windows = (2, 4, 8, 16)
reach_back = 15
norm_eps = 1e-06
clamp_limit = 7.0
glu_alpha = 1.702


def passed_along(x, axis, by):
    size = lax.axis_size(axis)
    pairs = [(i, i + by) for i in range(size) if 0 <= i + by < size]
    return lax.ppermute(x, axis, pairs)


def rotated(x, axis, by):
    size = lax.axis_size(axis)
    return lax.ppermute(x, axis, [(i, (i + by) % size) for i in range(size)])


def rms_scale(values, gain_vec):
    inverse = lax.rsqrt(jnp.mean(values * values, axis=-1, keepdims=True) + norm_eps)
    return values * inverse * gain_vec


def clamped_unit(gate_pre, upward):
    gate_clip = jnp.minimum(gate_pre, clamp_limit)
    linear = jnp.clip(upward, -clamp_limit, clamp_limit)
    return gate_clip * jax.nn.sigmoid(glu_alpha * gate_clip) * (linear + 1.0)


def mixed_window(pool_input):
    seg_rows, channels = pool_input.shape
    last_rows = pool_input[seg_rows - reach_back :]
    before = passed_along(last_rows, "sp", 1)
    extended = jnp.concatenate([before, pool_input], axis=0).astype(jnp.float32)
    first_chan = lax.axis_index("tp") * channels
    chan_group = (first_chan + lax.iota(jnp.int32, channels)) // GROUP_DIM
    positions = lax.axis_index("sp") * seg_rows + lax.iota(jnp.int32, seg_rows)
    window = jnp.zeros((channels,), jnp.int32)
    for group_level, win_len in enumerate(pool_windows):
        window = jnp.where(chan_group == group_level, win_len, window)
    running = jnp.zeros((seg_rows, channels), jnp.float32)
    window_sum = running
    for offset in range(pool_windows[-1]):
        running = running + extended[reach_back - offset : reach_back - offset + seg_rows]
        if offset + 1 in pool_windows:
            window_sum = jnp.where(window[None, :] == offset + 1, running, window_sum)
    divisor = jnp.minimum(positions[:, None] + 1, window[None, :]).astype(jnp.float32)
    return (window_sum / divisor - extended[reach_back:]).astype(jnp.bfloat16)


def reached(i, d, n):
    return i ^ d if n & (n - 1) == 0 else (i + d) % n


def offset_to(target, i, n):
    return target ^ i if n & (n - 1) == 0 else (target - i) % n


def moved(x, axis, d, back=False):
    size = lax.axis_size(axis)
    pairs = [(i, reached(i, d, size)) for i in range(size)]
    return lax.ppermute(x, axis, [(b, a) for a, b in pairs] if back else pairs)


LANES = 128
IN_VMEM = pl.BlockSpec(memory_space=pltpu.VMEM)


def load_body(*refs):
    half = len(refs) // 2
    sources, targets, done = refs[:half], refs[half:-1], refs[-1]
    copies = [
        pltpu.make_async_copy(source.at[e], target.at[e], done.at[i, e])
        for i, (source, target) in enumerate(zip(sources, targets))
        for e in range(source.shape[0])
    ]
    for copy in copies:
        copy.start()
    for copy in copies:
        copy.wait()


LOAD_LIMIT = 28


def load(*weights):
    return pl.pallas_call(
        load_body,
        in_specs=[pl.BlockSpec(memory_space=pltpu.HBM)] * len(weights),
        out_specs=[IN_VMEM] * len(weights),
        out_shape=[pltpu.VMEM(w.shape, w.dtype) for w in weights],
        scratch_shapes=[pltpu.SemaphoreType.DMA((len(weights), weights[0].shape[0]))],
        compiler_params=pltpu.CompilerParams(vmem_limit_bytes=LOAD_LIMIT << 20),
        name="load",
    )(*weights)


def pick_body(at, slot, block, *outs):
    rows = outs[0].shape[0]
    tokens = slot.shape[2]
    ids = lax.broadcasted_iota(jnp.int32, (len(outs) * rows, tokens), 0)
    hit = ids == slot[at, 0:1, :]
    for k in range(1, slot.shape[1]):
        hit = hit | (ids == slot[at, k : k + 1, :])
    chosen = jnp.where(hit, 1.0, 0.0).astype(jnp.bfloat16)
    for j in range(0, block.shape[1], 2 * LANES):
        cols = slice(j, j + 2 * LANES)
        taken = jnp.dot(chosen, block[:, cols], preferred_element_type=jnp.float32)
        for d, out in enumerate(outs):
            out[:, cols] = taken[d * rows : (d + 1) * rows].astype(out.dtype)


def pick(at, slot, block, n_sp, slot_rows):
    shape = jax.ShapeDtypeStruct((slot_rows, block.shape[1]), block.dtype)
    return pl.pallas_call(
        lambda *refs: pick_body(at, *refs),
        in_specs=[IN_VMEM] * 2,
        out_specs=[IN_VMEM] * n_sp,
        out_shape=[shape] * n_sp,
        compiler_params=pltpu.CompilerParams(vmem_limit_bytes=6 << 20),
        name="pick",
    )(slot, block)


def shares_of(at, slot, weight, d, rows):
    ids = lax.broadcasted_iota(jnp.int32, (slot.shape[1], rows), 1) + d * rows
    share = jnp.zeros((slot.shape[1], rows), jnp.float32)
    for k in range(slot.shape[2]):
        share = share + jnp.where(ids == slot[at, :, k : k + 1], weight[at, :, k : k + 1], 0.0)
    return share.astype(jnp.bfloat16)


def combine_body(at, slot, weight, *refs):
    backs, out = refs[:-1], refs[-1]
    rows = backs[0].shape[0]
    share = [shares_of(at, slot, weight, d, rows) for d in range(len(backs))]
    for j in range(0, out.shape[1], 2 * LANES):
        cols = slice(j, j + 2 * LANES)
        total = None
        for d, back in enumerate(backs):
            term = jnp.dot(share[d], back[:, cols], preferred_element_type=jnp.float32)
            total = term if total is None else total + term
        out[:, cols] = total.astype(out.dtype)


def combine(at, slot, weight, backs):
    shape = jax.ShapeDtypeStruct((slot.shape[1], backs[0].shape[1]), jnp.bfloat16)
    return pl.pallas_call(
        lambda *refs: combine_body(at, *refs),
        in_specs=[IN_VMEM] * (2 + len(backs)),
        out_specs=IN_VMEM,
        out_shape=shape,
        compiler_params=pltpu.CompilerParams(vmem_limit_bytes=6 << 20),
        name="combine",
    )(slot, weight, *backs)


def finish_body(at, n_back, slot, weight, resid, gain, *refs):
    backs, parts, (out, mix) = refs[:n_back], refs[n_back:-2], refs[-2:]
    rows, width = backs[0].shape[0], out.shape[1]
    share = [shares_of(at, slot, weight, d, rows) for d in range(n_back)]
    square = jnp.zeros((out.shape[0], LANES), jnp.float32)
    for j in range(0, width, 2 * LANES):
        cols = slice(j, j + 2 * LANES)
        total = parts[0][:, cols].astype(jnp.float32) if parts else 0.0
        for part in parts[1:]:
            total = total + part[:, cols].astype(jnp.float32)
        for d, back in enumerate(backs):
            total = total + jnp.dot(share[d], back[:, cols], preferred_element_type=jnp.float32)
        mix[:, cols] = total
        square = square + total[:, :LANES] * total[:, :LANES]
        square = square + total[:, LANES:] * total[:, LANES:]
    mean = jnp.sum(square, axis=1, keepdims=True) / width
    inverse = lax.rsqrt(mean + norm_eps)
    for j in range(0, width, 2 * LANES):
        cols = slice(j, j + 2 * LANES)
        scaled = mix[:, cols] * inverse * gain[:, cols]
        out[:, cols] = (resid[:, cols].astype(jnp.float32) + scaled).astype(out.dtype)


def finish(at, slot, weight, resid, gain, backs, parts):
    return pl.pallas_call(
        lambda *refs: finish_body(at, len(backs), *refs),
        in_specs=[IN_VMEM] * (4 + len(backs) + len(parts)),
        out_specs=IN_VMEM,
        out_shape=jax.ShapeDtypeStruct(resid.shape, resid.dtype),
        scratch_shapes=[pltpu.VMEM(resid.shape, jnp.float32)],
        compiler_params=pltpu.CompilerParams(vmem_limit_bytes=6 << 20),
        name="finish",
    )(slot, weight, resid, gain.reshape(1, -1), *backs, *parts)


def experts_body(n_src, *refs):
    xs, (wg, wu, wd) = refs[:n_src], refs[n_src : n_src + 3]
    outs, (into, outof) = refs[n_src + 3 : 2 * n_src + 3], refs[2 * n_src + 3 :]
    count, width = wg.shape[0], xs[0].shape[1]
    tiles, left = divmod(xs[0].shape[0] // count, 8)
    whole = count * tiles * 8
    for s, x in enumerate(xs):
        for j in range(width // LANES):
            cols = slice(j * LANES, (j + 1) * LANES)
            into[j, s * left * count : (s + 1) * left * count, :] = x[whole:, cols].astype(
                jnp.float32
            )

    def one(e, carry):
        own = [pl.ds(pl.multiple_of((e * tiles + i) * 8, 8), 8) for i in range(tiles)]
        apart = pl.ds(e, n_src * left, stride=count)
        taken = [x[at, :].astype(jnp.float32) for x in xs for at in own]
        taken.append(jnp.concatenate([into[j, apart, :] for j in range(width // LANES)], axis=1))
        taken = jnp.concatenate(taken, axis=0).astype(jnp.bfloat16)
        gate_pre = jnp.dot(taken, wg[e], preferred_element_type=jnp.float32)
        upward = jnp.dot(taken, wu[e], preferred_element_type=jnp.float32)
        activated = clamped_unit(gate_pre, upward).astype(jnp.bfloat16)
        result = jnp.dot(activated, wd[e], preferred_element_type=jnp.float32)
        row = 0
        for out in outs:
            for at in own:
                out[at, :] = result[row : row + 8].astype(out.dtype)
                row += 8
        for j in range(width // LANES):
            outof[j, apart, :] = result[row:, j * LANES : (j + 1) * LANES]
        return carry

    lax.fori_loop(0, count, one, 0, unroll=EXPERT_UNROLL)
    for s, out in enumerate(outs):
        for j in range(width // LANES):
            cols = slice(j * LANES, (j + 1) * LANES)
            out[whole:, cols] = outof[j, s * left * count : (s + 1) * left * count, :].astype(
                out.dtype
            )


EXPERT_UNROLL = 2


def experts(xs, w_gate, w_up, w_down):
    count, width, hidden = w_gate.shape
    rows, n_src = xs[0].shape[0], len(xs)
    left = rows // count % 8
    scratch = pltpu.VMEM((width // LANES, n_src * left * count, LANES), jnp.float32)
    flops = 6 * n_src * rows * width * hidden
    moved_bytes = 3 * count * width * hidden * 2 + 4 * n_src * rows * width
    return pl.pallas_call(
        lambda *refs: experts_body(n_src, *refs),
        in_specs=[IN_VMEM] * (n_src + 3),
        out_specs=[IN_VMEM] * n_src,
        out_shape=[jax.ShapeDtypeStruct((rows, width), jnp.bfloat16)] * n_src,
        scratch_shapes=[scratch, scratch],
        cost_estimate=pl.CostEstimate(flops=flops, bytes_accessed=moved_bytes, transcendentals=0),
        compiler_params=pltpu.CompilerParams(vmem_limit_bytes=6 << 20),
        name="experts",
    )(*xs, w_gate, w_up, w_down)


def per_device(
    resid_in,
    pool_input,
    pool_weight,
    pool_scale,
    out_weight,
    mix_gain,
    ffn_gain,
    w_gate,
    w_up,
    w_down,
    routes,
    route_weight,
    post_gain,
):
    n_sp = lax.axis_size("sp")
    n_tp = lax.axis_size("tp")
    tok_rows, width = resid_in.shape
    channels = pool_input.shape[1]
    local_experts = w_gate.shape[0]
    n_experts = local_experts * n_sp
    assert n_experts <= 256
    slot_rows = local_experts * CAP
    slot_total = n_sp * slot_rows

    fields = jnp.concatenate([routes.astype(jnp.bfloat16).T, route_weight.astype(jnp.bfloat16).T])
    n_fields = fields.size
    field_rows = -(-n_fields // (8 * channels)) * 8
    fields = jnp.pad(fields.reshape(-1), (0, field_rows * channels - n_fields))
    fields = jnp.broadcast_to(fields.reshape(1, field_rows, channels), (n_tp, field_rows, channels))
    mixed_rows = mixed_window(pool_input).reshape(n_tp, tok_rows, channels)
    sent = jnp.concatenate([mixed_rows, fields], axis=1)
    got = lax.all_to_all(sent, "tp", split_axis=0, concat_axis=0, tiled=True)
    token_mixed = got[:, :tok_rows].transpose(1, 0, 2).reshape(tok_rows, n_tp * channels)
    fields = got[:, tok_rows:].reshape(n_tp, -1)[:, :n_fields].reshape(n_tp, 2 * TOP, tok_rows)

    pooled = jnp.einsum(
        "tgc,gcd->tgd",
        token_mixed.reshape(tok_rows, GROUPS, GROUP_DIM),
        pool_weight,
        preferred_element_type=jnp.float32,
    )
    pooled = (
        (pooled * pool_scale.reshape(GROUPS, GROUP_DIM)).astype(jnp.bfloat16).reshape(tok_rows, -1)
    )
    mix_out = jnp.dot(pooled, out_weight, preferred_element_type=jnp.float32)
    residual = (resid_in.astype(jnp.float32) + rms_scale(mix_out, mix_gain)).astype(jnp.bfloat16)
    normed = rms_scale(residual.astype(jnp.float32), ffn_gain).astype(jnp.bfloat16)

    order = [0] + [k for pair in zip(range(1, n_tp), range(n_tp - 1, 0, -1)) for k in pair]
    order = list(dict.fromkeys(order))
    blocks = {}
    for k in order:
        blocks[k] = rotated(normed, "tp", k) if k else normed

    here = lax.axis_index("tp")
    sp_here = lax.axis_index("sp")
    fields = jnp.take(fields, (here - jnp.array(order)) % n_tp, axis=0)
    route = fields[:, :TOP].astype(jnp.int32)
    weight = fields[:, TOP:].astype(jnp.float32)
    onehot = route[..., None] == lax.iota(jnp.int32, n_experts)
    named = jnp.sum(onehot.astype(jnp.float32), axis=1)
    earlier = lax.iota(jnp.int32, tok_rows)[:, None] > lax.iota(jnp.int32, tok_rows)[None, :]
    rank = jnp.einsum(
        "ut,bte->bue",
        earlier.astype(jnp.bfloat16),
        named.astype(jnp.bfloat16),
        preferred_element_type=jnp.float32,
    )
    slot_rank = jnp.sum(rank[:, None] * onehot, axis=-1).astype(jnp.int32)

    if local_experts % 8 == 0 and CAP % 8 and n_sp <= 4:
        owner = offset_to(route // local_experts, sp_here, n_sp)
        expert = route % local_experts
        whole = CAP // 8 * 8
        in_tile = expert * whole + slot_rank
        apart = (local_experts - expert) * whole + (slot_rank - whole) * local_experts + expert
        slot = owner * slot_rows + jnp.where(slot_rank < whole, in_tile, expert * whole + apart)
        by_row = slot.transpose(0, 2, 1)
        weight = weight.transpose(0, 2, 1)
        size = max(1, n_tp // 2)
        weights = load(w_gate, w_up, w_down)
        arrived, backs, parts = [], {}, []
        for at, k in enumerate(order):
            rows = pick(at, slot, blocks[k], n_sp, slot_rows)
            arrived.append([moved(x, "sp", d) if d else x for d, x in enumerate(rows)])
        for first in range(0, n_tp, size):
            group = arrived[first : first + size]
            terms = experts([x for xs in group for x in xs], *weights)
            for at in range(first, first + size):
                back = terms[(at - first) * n_sp : (at - first + 1) * n_sp]
                backs[at] = [moved(x, "sp", d, True) if d else x for d, x in enumerate(back)]
        for at, k in enumerate(order):
            if k:
                part = combine(at, by_row, weight, backs[at])
                parts.append(rotated(part, "tp", -k))
        return finish(0, by_row, weight, residual, post_gain, backs[0], parts)
    else:
        slot_index = route * CAP + slot_rank
        picker = slot_index[..., None] == lax.iota(jnp.int32, slot_total)
        token_pick = jnp.sum(picker.astype(jnp.float32), axis=1).astype(jnp.bfloat16)
        token_weight = jnp.sum(jnp.where(picker, weight[..., None], 0.0), axis=1)
        token_weight = token_weight.astype(jnp.bfloat16)
        arrived = []
        for at, k in enumerate(order):
            rows = lax.dot_general(
                token_pick[at],
                blocks[k],
                (((0,), (0,)), ((), ())),
                preferred_element_type=jnp.float32,
            )
            rows = rows.astype(jnp.bfloat16).reshape(n_sp, slot_rows, width)
            arrived.append(lax.all_to_all(rows, "sp", split_axis=0, concat_axis=0, tiled=True))
        arrived = jnp.stack(arrived).reshape(n_tp, n_sp, local_experts, CAP, width)
        f32 = {"preferred_element_type": jnp.float32}
        gate_pre = jnp.einsum("sklcd,ldf->sklcf", arrived, w_gate, **f32)
        upward = jnp.einsum("sklcd,ldf->sklcf", arrived, w_up, **f32)
        activated = clamped_unit(gate_pre, upward).astype(jnp.bfloat16)
        terms = jnp.einsum("sklcf,lfd->sklcd", activated, w_down, **f32)
        terms = terms.astype(jnp.bfloat16).reshape(n_tp, n_sp, slot_rows, width)
        parts = {}
        for at, k in enumerate(order):
            back = lax.all_to_all(terms[at], "sp", split_axis=0, concat_axis=0, tiled=True)
            part = jnp.dot(token_weight[at], back.reshape(slot_total, width), **f32)
            part = part.astype(jnp.bfloat16)
            parts[k] = rotated(part, "tp", -k) if k else part
    expert_mix = sum(parts[k].astype(jnp.float32) for k in order)
    return (residual.astype(jnp.float32) + rms_scale(expert_mix, post_gain)).astype(jnp.bfloat16)


def solution(mesh):
    in_specs = (
        P(("grp", "sp", "tp"), None),
        P(("grp", "sp"), "tp"),
        P(),
        P(),
        P(),
        P(),
        P(),
        P("sp", None, "tp"),
        P("sp", None, "tp"),
        P("sp", "tp", None),
        P(("grp", "sp", "tp"), None),
        P(("grp", "sp", "tp"), None),
        P(),
    )
    out_specs = P(("grp", "sp", "tp"), None)

    return jax.shard_map(
        per_device, mesh=mesh, in_specs=in_specs, out_specs=out_specs, check_vma=False
    )
```

```python
import jax
import jax.numpy as jnp
from jax import lax
from jax.experimental import pallas as pl
from jax.experimental.pallas import tpu as pltpu
from jax.sharding import PartitionSpec as P


GROUPS = 4
GROUP_DIM = 256
TOP = 2
CAP = 9


pool_windows = (2, 4, 8, 16)
reach_back = 15
norm_eps = 1e-06
clamp_limit = 7.0
glu_alpha = 1.702


def passed_along(x, axis, by):
    size = lax.axis_size(axis)
    pairs = [(i, i + by) for i in range(size) if 0 <= i + by < size]
    return lax.ppermute(x, axis, pairs)


def rotated(x, axis, by):
    size = lax.axis_size(axis)
    return lax.ppermute(x, axis, [(i, (i + by) % size) for i in range(size)])


def rms_scale(values, gain_vec):
    inverse = lax.rsqrt(jnp.mean(values * values, axis=-1, keepdims=True) + norm_eps)
    return values * inverse * gain_vec


def clamped_unit(gate_pre, upward):
    gate_clip = jnp.minimum(gate_pre, clamp_limit)
    linear = jnp.clip(upward, -clamp_limit, clamp_limit)
    return gate_clip * jax.nn.sigmoid(glu_alpha * gate_clip) * (linear + 1.0)


def mixed_window(pool_input):
    seg_rows, channels = pool_input.shape
    last_rows = pool_input[seg_rows - reach_back :]
    before = passed_along(last_rows, "sp", 1)
    extended = jnp.concatenate([before, pool_input], axis=0).astype(jnp.float32)
    first_chan = lax.axis_index("tp") * channels
    chan_group = (first_chan + lax.iota(jnp.int32, channels)) // GROUP_DIM
    positions = lax.axis_index("sp") * seg_rows + lax.iota(jnp.int32, seg_rows)
    window = jnp.zeros((channels,), jnp.int32)
    for group_level, win_len in enumerate(pool_windows):
        window = jnp.where(chan_group == group_level, win_len, window)
    running = jnp.zeros((seg_rows, channels), jnp.float32)
    window_sum = running
    for offset in range(pool_windows[-1]):
        running = running + extended[reach_back - offset : reach_back - offset + seg_rows]
        if offset + 1 in pool_windows:
            window_sum = jnp.where(window[None, :] == offset + 1, running, window_sum)
    divisor = jnp.minimum(positions[:, None] + 1, window[None, :]).astype(jnp.float32)
    return (window_sum / divisor - extended[reach_back:]).astype(jnp.bfloat16)


def reached(i, d, n):
    return i ^ d if n & (n - 1) == 0 else (i + d) % n


def offset_to(target, i, n):
    return target ^ i if n & (n - 1) == 0 else (target - i) % n


def moved(x, axis, d, back=False):
    size = lax.axis_size(axis)
    pairs = [(i, reached(i, d, size)) for i in range(size)]
    return lax.ppermute(x, axis, [(b, a) for a, b in pairs] if back else pairs)


LANES = 128
IN_VMEM = pl.BlockSpec(memory_space=pltpu.VMEM)


def load_body(*refs):
    half = len(refs) // 2
    sources, targets, done = refs[:half], refs[half:-1], refs[-1]
    copies = [
        pltpu.make_async_copy(source.at[e], target.at[e], done.at[i, e])
        for i, (source, target) in enumerate(zip(sources, targets))
        for e in range(source.shape[0])
    ]
    for copy in copies:
        copy.start()
    for copy in copies:
        copy.wait()


LOAD_LIMIT = 28


def load(*weights):
    return pl.pallas_call(
        load_body,
        in_specs=[pl.BlockSpec(memory_space=pltpu.HBM)] * len(weights),
        out_specs=[IN_VMEM] * len(weights),
        out_shape=[pltpu.VMEM(w.shape, w.dtype) for w in weights],
        scratch_shapes=[pltpu.SemaphoreType.DMA((len(weights), weights[0].shape[0]))],
        compiler_params=pltpu.CompilerParams(vmem_limit_bytes=LOAD_LIMIT << 20),
        name="load",
    )(*weights)


def pick_body(at, slot, block, *outs):
    rows = outs[0].shape[0]
    tokens = slot.shape[2]
    ids = lax.broadcasted_iota(jnp.int32, (len(outs) * rows, tokens), 0)
    hit = ids == slot[at, 0:1, :]
    for k in range(1, slot.shape[1]):
        hit = hit | (ids == slot[at, k : k + 1, :])
    chosen = jnp.where(hit, 1.0, 0.0).astype(jnp.bfloat16)
    for j in range(0, block.shape[1], 2 * LANES):
        cols = slice(j, j + 2 * LANES)
        taken = jnp.dot(chosen, block[:, cols], preferred_element_type=jnp.float32)
        for d, out in enumerate(outs):
            out[:, cols] = taken[d * rows : (d + 1) * rows].astype(out.dtype)


def pick(at, slot, block, n_sp, slot_rows):
    shape = jax.ShapeDtypeStruct((slot_rows, block.shape[1]), block.dtype)
    return pl.pallas_call(
        lambda *refs: pick_body(at, *refs),
        in_specs=[IN_VMEM] * 2,
        out_specs=[IN_VMEM] * n_sp,
        out_shape=[shape] * n_sp,
        compiler_params=pltpu.CompilerParams(vmem_limit_bytes=6 << 20),
        name="pick",
    )(slot, block)


def shares_of(at, slot, weight, d, rows):
    ids = lax.broadcasted_iota(jnp.int32, (slot.shape[1], rows), 1) + d * rows
    share = jnp.zeros((slot.shape[1], rows), jnp.float32)
    for k in range(slot.shape[2]):
        share = share + jnp.where(ids == slot[at, :, k : k + 1], weight[at, :, k : k + 1], 0.0)
    return share.astype(jnp.bfloat16)


def combine_body(at, slot, weight, *refs):
    backs, out = refs[:-1], refs[-1]
    rows = backs[0].shape[0]
    share = [shares_of(at, slot, weight, d, rows) for d in range(len(backs))]
    for j in range(0, out.shape[1], 2 * LANES):
        cols = slice(j, j + 2 * LANES)
        total = None
        for d, back in enumerate(backs):
            term = jnp.dot(share[d], back[:, cols], preferred_element_type=jnp.float32)
            total = term if total is None else total + term
        out[:, cols] = total.astype(out.dtype)


def combine(at, slot, weight, backs):
    shape = jax.ShapeDtypeStruct((slot.shape[1], backs[0].shape[1]), jnp.bfloat16)
    return pl.pallas_call(
        lambda *refs: combine_body(at, *refs),
        in_specs=[IN_VMEM] * (2 + len(backs)),
        out_specs=IN_VMEM,
        out_shape=shape,
        compiler_params=pltpu.CompilerParams(vmem_limit_bytes=6 << 20),
        name="combine",
    )(slot, weight, *backs)


def finish_body(at, n_back, slot, weight, resid, gain, *refs):
    backs, parts, (out, mix) = refs[:n_back], refs[n_back:-2], refs[-2:]
    rows, width = backs[0].shape[0], out.shape[1]
    share = [shares_of(at, slot, weight, d, rows) for d in range(n_back)]
    square = jnp.zeros((out.shape[0], LANES), jnp.float32)
    for j in range(0, width, 2 * LANES):
        cols = slice(j, j + 2 * LANES)
        total = parts[0][:, cols].astype(jnp.float32) if parts else 0.0
        for part in parts[1:]:
            total = total + part[:, cols].astype(jnp.float32)
        for d, back in enumerate(backs):
            total = total + jnp.dot(share[d], back[:, cols], preferred_element_type=jnp.float32)
        mix[:, cols] = total
        square = square + total[:, :LANES] * total[:, :LANES]
        square = square + total[:, LANES:] * total[:, LANES:]
    mean = jnp.sum(square, axis=1, keepdims=True) / width
    inverse = lax.rsqrt(mean + norm_eps)
    for j in range(0, width, 2 * LANES):
        cols = slice(j, j + 2 * LANES)
        scaled = mix[:, cols] * inverse * gain[:, cols]
        out[:, cols] = (resid[:, cols].astype(jnp.float32) + scaled).astype(out.dtype)


def finish(at, slot, weight, resid, gain, backs, parts):
    return pl.pallas_call(
        lambda *refs: finish_body(at, len(backs), *refs),
        in_specs=[IN_VMEM] * (4 + len(backs) + len(parts)),
        out_specs=IN_VMEM,
        out_shape=jax.ShapeDtypeStruct(resid.shape, resid.dtype),
        scratch_shapes=[pltpu.VMEM(resid.shape, jnp.float32)],
        compiler_params=pltpu.CompilerParams(vmem_limit_bytes=6 << 20),
        name="finish",
    )(slot, weight, resid, gain.reshape(1, -1), *backs, *parts)


def experts_body(n_src, *refs):
    xs, (wg, wu, wd) = refs[:n_src], refs[n_src : n_src + 3]
    outs, (into, outof) = refs[n_src + 3 : 2 * n_src + 3], refs[2 * n_src + 3 :]
    count, width = wg.shape[0], xs[0].shape[1]
    tiles, left = divmod(xs[0].shape[0] // count, 8)
    whole = count * tiles * 8
    for s, x in enumerate(xs):
        for j in range(width // LANES):
            cols = slice(j * LANES, (j + 1) * LANES)
            into[j, s * left * count : (s + 1) * left * count, :] = x[whole:, cols].astype(
                jnp.float32
            )

    def one(e, carry):
        own = [pl.ds(pl.multiple_of((e * tiles + i) * 8, 8), 8) for i in range(tiles)]
        apart = pl.ds(e, n_src * left, stride=count)
        taken = [x[at, :].astype(jnp.float32) for x in xs for at in own]
        taken.append(jnp.concatenate([into[j, apart, :] for j in range(width // LANES)], axis=1))
        taken = jnp.concatenate(taken, axis=0).astype(jnp.bfloat16)
        gate_pre = jnp.dot(taken, wg[e], preferred_element_type=jnp.float32)
        upward = jnp.dot(taken, wu[e], preferred_element_type=jnp.float32)
        activated = clamped_unit(gate_pre, upward).astype(jnp.bfloat16)
        result = jnp.dot(activated, wd[e], preferred_element_type=jnp.float32)
        row = 0
        for out in outs:
            for at in own:
                out[at, :] = result[row : row + 8].astype(out.dtype)
                row += 8
        for j in range(width // LANES):
            outof[j, apart, :] = result[row:, j * LANES : (j + 1) * LANES]
        return carry

    lax.fori_loop(0, count, one, 0, unroll=EXPERT_UNROLL)
    for s, out in enumerate(outs):
        for j in range(width // LANES):
            cols = slice(j * LANES, (j + 1) * LANES)
            out[whole:, cols] = outof[j, s * left * count : (s + 1) * left * count, :].astype(
                out.dtype
            )


EXPERT_UNROLL = 2


def experts(xs, w_gate, w_up, w_down):
    count, width, hidden = w_gate.shape
    rows, n_src = xs[0].shape[0], len(xs)
    left = rows // count % 8
    scratch = pltpu.VMEM((width // LANES, n_src * left * count, LANES), jnp.float32)
    flops = 6 * n_src * rows * width * hidden
    moved_bytes = 3 * count * width * hidden * 2 + 4 * n_src * rows * width
    return pl.pallas_call(
        lambda *refs: experts_body(n_src, *refs),
        in_specs=[IN_VMEM] * (n_src + 3),
        out_specs=[IN_VMEM] * n_src,
        out_shape=[jax.ShapeDtypeStruct((rows, width), jnp.bfloat16)] * n_src,
        scratch_shapes=[scratch, scratch],
        cost_estimate=pl.CostEstimate(flops=flops, bytes_accessed=moved_bytes, transcendentals=0),
        compiler_params=pltpu.CompilerParams(vmem_limit_bytes=6 << 20),
        name="experts",
    )(*xs, w_gate, w_up, w_down)


def per_device(
    resid_in,
    pool_input,
    pool_weight,
    pool_scale,
    out_weight,
    mix_gain,
    ffn_gain,
    w_gate,
    w_up,
    w_down,
    routes,
    route_weight,
    post_gain,
):
    n_sp = lax.axis_size("sp")
    n_tp = lax.axis_size("tp")
    tok_rows, width = resid_in.shape
    channels = pool_input.shape[1]
    local_experts = w_gate.shape[0]
    n_experts = local_experts * n_sp
    assert n_experts <= 256
    slot_rows = local_experts * CAP
    slot_total = n_sp * slot_rows

    fields = jnp.concatenate([routes.astype(jnp.bfloat16).T, route_weight.astype(jnp.bfloat16).T])
    n_fields = fields.size
    field_rows = -(-n_fields // (8 * channels)) * 8
    fields = jnp.pad(fields.reshape(-1), (0, field_rows * channels - n_fields))
    fields = jnp.broadcast_to(fields.reshape(1, field_rows, channels), (n_tp, field_rows, channels))
    mixed_rows = mixed_window(pool_input).reshape(n_tp, tok_rows, channels)
    sent = jnp.concatenate([mixed_rows, fields], axis=1)
    got = lax.all_to_all(sent, "tp", split_axis=0, concat_axis=0, tiled=True)
    token_mixed = got[:, :tok_rows].transpose(1, 0, 2).reshape(tok_rows, n_tp * channels)
    fields = got[:, tok_rows:].reshape(n_tp, -1)[:, :n_fields].reshape(n_tp, 2 * TOP, tok_rows)

    pooled = jnp.einsum(
        "tgc,gcd->tgd",
        token_mixed.reshape(tok_rows, GROUPS, GROUP_DIM),
        pool_weight,
        preferred_element_type=jnp.float32,
    )
    pooled = (
        (pooled * pool_scale.reshape(GROUPS, GROUP_DIM)).astype(jnp.bfloat16).reshape(tok_rows, -1)
    )
    mix_out = jnp.dot(pooled, out_weight, preferred_element_type=jnp.float32)
    residual = (resid_in.astype(jnp.float32) + rms_scale(mix_out, mix_gain)).astype(jnp.bfloat16)
    normed = rms_scale(residual.astype(jnp.float32), ffn_gain).astype(jnp.bfloat16)

    order = [0] + [k for pair in zip(range(1, n_tp), range(n_tp - 1, 0, -1)) for k in pair]
    order = list(dict.fromkeys(order))
    blocks = {}
    for k in order:
        blocks[k] = rotated(normed, "tp", k) if k else normed

    here = lax.axis_index("tp")
    sp_here = lax.axis_index("sp")
    fields = jnp.take(fields, (here - jnp.array(order)) % n_tp, axis=0)
    route = fields[:, :TOP].astype(jnp.int32)
    weight = fields[:, TOP:].astype(jnp.float32)
    onehot = route[..., None] == lax.iota(jnp.int32, n_experts)
    named = jnp.sum(onehot.astype(jnp.float32), axis=1)
    earlier = lax.iota(jnp.int32, tok_rows)[:, None] > lax.iota(jnp.int32, tok_rows)[None, :]
    rank = jnp.einsum(
        "ut,bte->bue",
        earlier.astype(jnp.bfloat16),
        named.astype(jnp.bfloat16),
        preferred_element_type=jnp.float32,
    )
    slot_rank = jnp.sum(rank[:, None] * onehot, axis=-1).astype(jnp.int32)

    if local_experts % 8 == 0 and CAP % 8 and n_sp <= 4:
        owner = offset_to(route // local_experts, sp_here, n_sp)
        expert = route % local_experts
        whole = CAP // 8 * 8
        in_tile = expert * whole + slot_rank
        apart = (local_experts - expert) * whole + (slot_rank - whole) * local_experts + expert
        slot = owner * slot_rows + jnp.where(slot_rank < whole, in_tile, expert * whole + apart)
        by_row = slot.transpose(0, 2, 1)
        weight = weight.transpose(0, 2, 1)
        slot, by_row, weight = lax.optimization_barrier((slot, by_row, weight))
        weights = load(w_gate, w_up, w_down)
        arrived, backs, parts = [], {}, []
        for at, k in enumerate(order):
            rows = pick(at, slot, blocks[k], n_sp, slot_rows)
            arrived.append([moved(x, "sp", d) if d else x for d, x in enumerate(rows)])
        for first, stop in groups_of(n_tp):
            group = arrived[first:stop]
            terms = experts([x for xs in group for x in xs], *weights)
            for at in range(first, stop):
                back = terms[(at - first) * n_sp : (at - first + 1) * n_sp]
                backs[at] = [moved(x, "sp", d, True) if d else x for d, x in enumerate(back)]
        for at, k in enumerate(order):
            if k:
                part = combine(at, by_row, weight, backs[at])
                parts.append(rotated(part, "tp", -k))
        return finish(0, by_row, weight, residual, post_gain, backs[0], parts)
    else:
        slot_index = route * CAP + slot_rank
        picker = slot_index[..., None] == lax.iota(jnp.int32, slot_total)
        token_pick = jnp.sum(picker.astype(jnp.float32), axis=1).astype(jnp.bfloat16)
        token_weight = jnp.sum(jnp.where(picker, weight[..., None], 0.0), axis=1)
        token_weight = token_weight.astype(jnp.bfloat16)
        arrived = []
        for at, k in enumerate(order):
            rows = lax.dot_general(
                token_pick[at],
                blocks[k],
                (((0,), (0,)), ((), ())),
                preferred_element_type=jnp.float32,
            )
            rows = rows.astype(jnp.bfloat16).reshape(n_sp, slot_rows, width)
            arrived.append(lax.all_to_all(rows, "sp", split_axis=0, concat_axis=0, tiled=True))
        arrived = jnp.stack(arrived).reshape(n_tp, n_sp, local_experts, CAP, width)
        f32 = {"preferred_element_type": jnp.float32}
        gate_pre = jnp.einsum("sklcd,ldf->sklcf", arrived, w_gate, **f32)
        upward = jnp.einsum("sklcd,ldf->sklcf", arrived, w_up, **f32)
        activated = clamped_unit(gate_pre, upward).astype(jnp.bfloat16)
        terms = jnp.einsum("sklcf,lfd->sklcd", activated, w_down, **f32)
        terms = terms.astype(jnp.bfloat16).reshape(n_tp, n_sp, slot_rows, width)
        parts = {}
        for at, k in enumerate(order):
            back = lax.all_to_all(terms[at], "sp", split_axis=0, concat_axis=0, tiled=True)
            part = jnp.dot(token_weight[at], back.reshape(slot_total, width), **f32)
            part = part.astype(jnp.bfloat16)
            parts[k] = rotated(part, "tp", -k) if k else part
    expert_mix = sum(parts[k].astype(jnp.float32) for k in order)
    return (residual.astype(jnp.float32) + rms_scale(expert_mix, post_gain)).astype(jnp.bfloat16)


def groups_of(n_tp):
    first = min(2, n_tp)
    return [(0, first)] + [(at, at + 1) for at in range(first, n_tp)]


def solution(mesh):
    in_specs = (
        P(("grp", "sp", "tp"), None),
        P(("grp", "sp"), "tp"),
        P(),
        P(),
        P(),
        P(),
        P(),
        P("sp", None, "tp"),
        P("sp", None, "tp"),
        P("sp", "tp", None),
        P(("grp", "sp", "tp"), None),
        P(("grp", "sp", "tp"), None),
        P(),
    )
    out_specs = P(("grp", "sp", "tp"), None)

    return jax.shard_map(
        per_device, mesh=mesh, in_specs=in_specs, out_specs=out_specs, check_vma=False
    )
```

```python
import jax
import jax.numpy as jnp
from jax import lax
from jax.experimental import pallas as pl
from jax.experimental.pallas import tpu as pltpu
from jax.sharding import PartitionSpec as P


GROUPS = 4
GROUP_DIM = 256
TOP = 2
CAP = 9


pool_windows = (2, 4, 8, 16)
reach_back = 15
norm_eps = 1e-06
clamp_limit = 7.0
glu_alpha = 1.702


def passed_along(x, axis, by):
    size = lax.axis_size(axis)
    pairs = [(i, i + by) for i in range(size) if 0 <= i + by < size]
    return lax.ppermute(x, axis, pairs)


def rotated(x, axis, by):
    size = lax.axis_size(axis)
    return lax.ppermute(x, axis, [(i, (i + by) % size) for i in range(size)])


def rms_scale(values, gain_vec):
    inverse = lax.rsqrt(jnp.mean(values * values, axis=-1, keepdims=True) + norm_eps)
    return values * inverse * gain_vec


def clamped_unit(gate_pre, upward):
    gate_clip = jnp.minimum(gate_pre, clamp_limit)
    linear = jnp.clip(upward, -clamp_limit, clamp_limit)
    return gate_clip * jax.nn.sigmoid(glu_alpha * gate_clip) * (linear + 1.0)


def mixed_window(pool_input):
    seg_rows, channels = pool_input.shape
    last_rows = pool_input[seg_rows - reach_back :]
    before = passed_along(last_rows, "sp", 1)
    extended = jnp.concatenate([before, pool_input], axis=0).astype(jnp.float32)
    first_chan = lax.axis_index("tp") * channels
    chan_group = (first_chan + lax.iota(jnp.int32, channels)) // GROUP_DIM
    positions = lax.axis_index("sp") * seg_rows + lax.iota(jnp.int32, seg_rows)
    window = jnp.zeros((channels,), jnp.int32)
    for group_level, win_len in enumerate(pool_windows):
        window = jnp.where(chan_group == group_level, win_len, window)
    running = jnp.zeros((seg_rows, channels), jnp.float32)
    window_sum = running
    for offset in range(pool_windows[-1]):
        running = running + extended[reach_back - offset : reach_back - offset + seg_rows]
        if offset + 1 in pool_windows:
            window_sum = jnp.where(window[None, :] == offset + 1, running, window_sum)
    divisor = jnp.minimum(positions[:, None] + 1, window[None, :]).astype(jnp.float32)
    return (window_sum / divisor - extended[reach_back:]).astype(jnp.bfloat16)


def reached(i, d, n):
    return i ^ d if n & (n - 1) == 0 else (i + d) % n


def offset_to(target, i, n):
    return target ^ i if n & (n - 1) == 0 else (target - i) % n


def moved(x, axis, d, back=False):
    size = lax.axis_size(axis)
    pairs = [(i, reached(i, d, size)) for i in range(size)]
    return lax.ppermute(x, axis, [(b, a) for a, b in pairs] if back else pairs)


LANES = 128
IN_VMEM = pl.BlockSpec(memory_space=pltpu.VMEM)


def load_body(*refs):
    half = len(refs) // 2
    sources, targets, done = refs[:half], refs[half:-1], refs[-1]
    copies = [
        pltpu.make_async_copy(source.at[e], target.at[e], done.at[i, e])
        for i, (source, target) in enumerate(zip(sources, targets))
        for e in range(source.shape[0])
    ]
    for copy in copies:
        copy.start()
    for copy in copies:
        copy.wait()


LOAD_LIMIT = 28


def load(*weights):
    return pl.pallas_call(
        load_body,
        in_specs=[pl.BlockSpec(memory_space=pltpu.HBM)] * len(weights),
        out_specs=[IN_VMEM] * len(weights),
        out_shape=[pltpu.VMEM(w.shape, w.dtype) for w in weights],
        scratch_shapes=[pltpu.SemaphoreType.DMA((len(weights), weights[0].shape[0]))],
        compiler_params=pltpu.CompilerParams(vmem_limit_bytes=LOAD_LIMIT << 20),
        name="load",
    )(*weights)


def pick_body(at, slot, block, *outs):
    rows = outs[0].shape[0]
    tokens = slot.shape[2]
    ids = lax.broadcasted_iota(jnp.int32, (len(outs) * rows, tokens), 0)
    hit = ids == slot[at, 0:1, :]
    for k in range(1, slot.shape[1]):
        hit = hit | (ids == slot[at, k : k + 1, :])
    chosen = jnp.where(hit, 1.0, 0.0).astype(jnp.bfloat16)
    for j in range(0, block.shape[1], 2 * LANES):
        cols = slice(j, j + 2 * LANES)
        taken = jnp.dot(chosen, block[:, cols], preferred_element_type=jnp.float32)
        for d, out in enumerate(outs):
            out[:, cols] = taken[d * rows : (d + 1) * rows].astype(out.dtype)


def pick(at, slot, block, n_sp, slot_rows):
    shape = jax.ShapeDtypeStruct((slot_rows, block.shape[1]), block.dtype)
    return pl.pallas_call(
        lambda *refs: pick_body(at, *refs),
        in_specs=[IN_VMEM] * 2,
        out_specs=[IN_VMEM] * n_sp,
        out_shape=[shape] * n_sp,
        compiler_params=pltpu.CompilerParams(vmem_limit_bytes=6 << 20),
        name="pick",
    )(slot, block)


def shares_of(at, slot, weight, d, rows):
    ids = lax.broadcasted_iota(jnp.int32, (slot.shape[1], rows), 1) + d * rows
    share = jnp.zeros((slot.shape[1], rows), jnp.float32)
    for k in range(slot.shape[2]):
        share = share + jnp.where(ids == slot[at, :, k : k + 1], weight[at, :, k : k + 1], 0.0)
    return share.astype(jnp.bfloat16)


def combine_body(at, n_back, slot, weight, *refs):
    backs, joined, out = refs[:n_back], refs[n_back:-1], refs[-1]
    rows = backs[0].shape[0]
    share = [shares_of(at, slot, weight, d, rows) for d in range(len(backs))]
    for j in range(0, out.shape[1], 2 * LANES):
        cols = slice(j, j + 2 * LANES)
        total = None
        for d, back in enumerate(backs):
            term = jnp.dot(share[d], back[:, cols], preferred_element_type=jnp.float32)
            total = term if total is None else total + term
        for other in joined:
            total = total + other[:, cols].astype(jnp.float32)
        out[:, cols] = total.astype(out.dtype)


def combine(at, slot, weight, backs, joined):
    shape = jax.ShapeDtypeStruct((slot.shape[1], backs[0].shape[1]), jnp.bfloat16)
    return pl.pallas_call(
        lambda *refs: combine_body(at, len(backs), *refs),
        in_specs=[IN_VMEM] * (2 + len(backs) + len(joined)),
        out_specs=IN_VMEM,
        out_shape=shape,
        compiler_params=pltpu.CompilerParams(vmem_limit_bytes=6 << 20),
        name="combine",
    )(slot, weight, *backs, *joined)


def finish_body(at, n_back, slot, weight, resid, gain, *refs):
    backs, parts, (out, mix) = refs[:n_back], refs[n_back:-2], refs[-2:]
    rows, width = backs[0].shape[0], out.shape[1]
    share = [shares_of(at, slot, weight, d, rows) for d in range(n_back)]
    square = jnp.zeros((out.shape[0], LANES), jnp.float32)
    for j in range(0, width, 2 * LANES):
        cols = slice(j, j + 2 * LANES)
        total = parts[0][:, cols].astype(jnp.float32) if parts else 0.0
        for part in parts[1:]:
            total = total + part[:, cols].astype(jnp.float32)
        for d, back in enumerate(backs):
            total = total + jnp.dot(share[d], back[:, cols], preferred_element_type=jnp.float32)
        mix[:, cols] = total
        square = square + total[:, :LANES] * total[:, :LANES]
        square = square + total[:, LANES:] * total[:, LANES:]
    mean = jnp.sum(square, axis=1, keepdims=True) / width
    inverse = lax.rsqrt(mean + norm_eps)
    for j in range(0, width, 2 * LANES):
        cols = slice(j, j + 2 * LANES)
        scaled = mix[:, cols] * inverse * gain[:, cols]
        out[:, cols] = (resid[:, cols].astype(jnp.float32) + scaled).astype(out.dtype)


def finish(at, slot, weight, resid, gain, backs, parts):
    return pl.pallas_call(
        lambda *refs: finish_body(at, len(backs), *refs),
        in_specs=[IN_VMEM] * (4 + len(backs) + len(parts)),
        out_specs=IN_VMEM,
        out_shape=jax.ShapeDtypeStruct(resid.shape, resid.dtype),
        scratch_shapes=[pltpu.VMEM(resid.shape, jnp.float32)],
        compiler_params=pltpu.CompilerParams(vmem_limit_bytes=6 << 20),
        name="finish",
    )(slot, weight, resid, gain.reshape(1, -1), *backs, *parts)


def experts_body(n_src, *refs):
    xs, (wg, wu, wd) = refs[:n_src], refs[n_src : n_src + 3]
    outs, (into, outof) = refs[n_src + 3 : 2 * n_src + 3], refs[2 * n_src + 3 :]
    count, width = wg.shape[0], xs[0].shape[1]
    tiles, left = divmod(xs[0].shape[0] // count, 8)
    whole = count * tiles * 8
    for s, x in enumerate(xs):
        for j in range(width // LANES):
            cols = slice(j * LANES, (j + 1) * LANES)
            into[j, s * left * count : (s + 1) * left * count, :] = x[whole:, cols].astype(
                jnp.float32
            )

    def one(e, carry):
        own = [pl.ds(pl.multiple_of((e * tiles + i) * 8, 8), 8) for i in range(tiles)]
        apart = pl.ds(e, n_src * left, stride=count)
        taken = [x[at, :].astype(jnp.float32) for x in xs for at in own]
        taken.append(jnp.concatenate([into[j, apart, :] for j in range(width // LANES)], axis=1))
        taken = jnp.concatenate(taken, axis=0).astype(jnp.bfloat16)
        gate_pre = jnp.dot(taken, wg[e], preferred_element_type=jnp.float32)
        upward = jnp.dot(taken, wu[e], preferred_element_type=jnp.float32)
        activated = clamped_unit(gate_pre, upward).astype(jnp.bfloat16)
        result = jnp.dot(activated, wd[e], preferred_element_type=jnp.float32)
        row = 0
        for out in outs:
            for at in own:
                out[at, :] = result[row : row + 8].astype(out.dtype)
                row += 8
        for j in range(width // LANES):
            outof[j, apart, :] = result[row:, j * LANES : (j + 1) * LANES]
        return carry

    lax.fori_loop(0, count, one, 0, unroll=EXPERT_UNROLL)
    for s, out in enumerate(outs):
        for j in range(width // LANES):
            cols = slice(j * LANES, (j + 1) * LANES)
            out[whole:, cols] = outof[j, s * left * count : (s + 1) * left * count, :].astype(
                out.dtype
            )


EXPERT_UNROLL = 2


def experts(xs, w_gate, w_up, w_down):
    count, width, hidden = w_gate.shape
    rows, n_src = xs[0].shape[0], len(xs)
    left = rows // count % 8
    scratch = pltpu.VMEM((width // LANES, n_src * left * count, LANES), jnp.float32)
    flops = 6 * n_src * rows * width * hidden
    moved_bytes = 3 * count * width * hidden * 2 + 4 * n_src * rows * width
    return pl.pallas_call(
        lambda *refs: experts_body(n_src, *refs),
        in_specs=[IN_VMEM] * (n_src + 3),
        out_specs=[IN_VMEM] * n_src,
        out_shape=[jax.ShapeDtypeStruct((rows, width), jnp.bfloat16)] * n_src,
        scratch_shapes=[scratch, scratch],
        cost_estimate=pl.CostEstimate(flops=flops, bytes_accessed=moved_bytes, transcendentals=0),
        compiler_params=pltpu.CompilerParams(vmem_limit_bytes=6 << 20),
        name="experts",
    )(*xs, w_gate, w_up, w_down)


def per_device(
    resid_in,
    pool_input,
    pool_weight,
    pool_scale,
    out_weight,
    mix_gain,
    ffn_gain,
    w_gate,
    w_up,
    w_down,
    routes,
    route_weight,
    post_gain,
):
    n_sp = lax.axis_size("sp")
    n_tp = lax.axis_size("tp")
    tok_rows, width = resid_in.shape
    channels = pool_input.shape[1]
    local_experts = w_gate.shape[0]
    n_experts = local_experts * n_sp
    assert n_experts <= 256
    slot_rows = local_experts * CAP
    slot_total = n_sp * slot_rows

    fields = jnp.concatenate([routes.astype(jnp.bfloat16).T, route_weight.astype(jnp.bfloat16).T])
    n_fields = fields.size
    field_rows = -(-n_fields // (8 * channels)) * 8
    fields = jnp.pad(fields.reshape(-1), (0, field_rows * channels - n_fields))
    fields = jnp.broadcast_to(fields.reshape(1, field_rows, channels), (n_tp, field_rows, channels))
    mixed_rows = mixed_window(pool_input).reshape(n_tp, tok_rows, channels)
    sent = jnp.concatenate([mixed_rows, fields], axis=1)
    got = lax.all_to_all(sent, "tp", split_axis=0, concat_axis=0, tiled=True)
    token_mixed = got[:, :tok_rows].transpose(1, 0, 2).reshape(tok_rows, n_tp * channels)
    fields = got[:, tok_rows:].reshape(n_tp, -1)[:, :n_fields].reshape(n_tp, 2 * TOP, tok_rows)

    pooled = jnp.einsum(
        "tgc,gcd->tgd",
        token_mixed.reshape(tok_rows, GROUPS, GROUP_DIM),
        pool_weight,
        preferred_element_type=jnp.float32,
    )
    pooled = (
        (pooled * pool_scale.reshape(GROUPS, GROUP_DIM)).astype(jnp.bfloat16).reshape(tok_rows, -1)
    )
    mix_out = jnp.dot(pooled, out_weight, preferred_element_type=jnp.float32)
    residual = (resid_in.astype(jnp.float32) + rms_scale(mix_out, mix_gain)).astype(jnp.bfloat16)
    normed = rms_scale(residual.astype(jnp.float32), ffn_gain).astype(jnp.bfloat16)

    far = n_tp // 2
    order = list(range(far + 1)) + list(range(n_tp - 1, far, -1))
    blocks = {0: normed, n_tp: normed}
    for k in order:
        if k:
            by = 1 if k <= far else -1
            blocks[k] = rotated(blocks[k - by], "tp", by)

    here = lax.axis_index("tp")
    sp_here = lax.axis_index("sp")
    fields = jnp.take(fields, (here - jnp.array(order)) % n_tp, axis=0)
    route = fields[:, :TOP].astype(jnp.int32)
    weight = fields[:, TOP:].astype(jnp.float32)
    onehot = route[..., None] == lax.iota(jnp.int32, n_experts)
    named = jnp.sum(onehot.astype(jnp.float32), axis=1)
    earlier = lax.iota(jnp.int32, tok_rows)[:, None] > lax.iota(jnp.int32, tok_rows)[None, :]
    rank = jnp.einsum(
        "ut,bte->bue",
        earlier.astype(jnp.bfloat16),
        named.astype(jnp.bfloat16),
        preferred_element_type=jnp.float32,
    )
    slot_rank = jnp.sum(rank[:, None] * onehot, axis=-1).astype(jnp.int32)

    if local_experts % 8 == 0 and CAP % 8 and n_sp <= 4:
        owner = offset_to(route // local_experts, sp_here, n_sp)
        expert = route % local_experts
        whole = CAP // 8 * 8
        in_tile = expert * whole + slot_rank
        apart = (local_experts - expert) * whole + (slot_rank - whole) * local_experts + expert
        slot = owner * slot_rows + jnp.where(slot_rank < whole, in_tile, expert * whole + apart)
        by_row = slot.transpose(0, 2, 1)
        weight = weight.transpose(0, 2, 1)
        slot, by_row, weight = lax.optimization_barrier((slot, by_row, weight))
        weights = load(w_gate, w_up, w_down)
        arrived, backs, parts = [], {}, {}
        for at, k in enumerate(order):
            rows = pick(at, slot, blocks[k], n_sp, slot_rows)
            arrived.append([moved(x, "sp", d) if d else x for d, x in enumerate(rows)])
        for first, stop in groups_of(n_tp):
            group = arrived[first:stop]
            terms = experts([x for xs in group for x in xs], *weights)
            for at in range(first, stop):
                back = terms[(at - first) * n_sp : (at - first + 1) * n_sp]
                backs[at] = [moved(x, "sp", d, True) if d else x for d, x in enumerate(back)]
        for at in return_order(n_tp)[:-1]:
            k = order[at]
            by = -1 if k <= far else 1
            inner = k < far or k > far + 1
            joined = [parts.pop(k - by)] if inner else []
            part = combine(at, by_row, weight, backs[at], joined)
            parts[k] = rotated(part, "tp", by)
        return finish(0, by_row, weight, residual, post_gain, backs[0], list(parts.values()))
    else:
        slot_index = route * CAP + slot_rank
        picker = slot_index[..., None] == lax.iota(jnp.int32, slot_total)
        token_pick = jnp.sum(picker.astype(jnp.float32), axis=1).astype(jnp.bfloat16)
        token_weight = jnp.sum(jnp.where(picker, weight[..., None], 0.0), axis=1)
        token_weight = token_weight.astype(jnp.bfloat16)
        arrived = []
        for at, k in enumerate(order):
            rows = lax.dot_general(
                token_pick[at],
                blocks[k],
                (((0,), (0,)), ((), ())),
                preferred_element_type=jnp.float32,
            )
            rows = rows.astype(jnp.bfloat16).reshape(n_sp, slot_rows, width)
            arrived.append(lax.all_to_all(rows, "sp", split_axis=0, concat_axis=0, tiled=True))
        arrived = jnp.stack(arrived).reshape(n_tp, n_sp, local_experts, CAP, width)
        f32 = {"preferred_element_type": jnp.float32}
        gate_pre = jnp.einsum("sklcd,ldf->sklcf", arrived, w_gate, **f32)
        upward = jnp.einsum("sklcd,ldf->sklcf", arrived, w_up, **f32)
        activated = clamped_unit(gate_pre, upward).astype(jnp.bfloat16)
        terms = jnp.einsum("sklcf,lfd->sklcd", activated, w_down, **f32)
        terms = terms.astype(jnp.bfloat16).reshape(n_tp, n_sp, slot_rows, width)
        parts = {}
        for at, k in enumerate(order):
            back = lax.all_to_all(terms[at], "sp", split_axis=0, concat_axis=0, tiled=True)
            part = jnp.dot(token_weight[at], back.reshape(slot_total, width), **f32)
            part = part.astype(jnp.bfloat16)
            parts[k] = rotated(part, "tp", -k) if k else part
    expert_mix = sum(parts[k].astype(jnp.float32) for k in order)
    return (residual.astype(jnp.float32) + rms_scale(expert_mix, post_gain)).astype(jnp.bfloat16)


def groups_of(n_tp):
    first = min(2, n_tp)
    return [(0, first)] + [(at, at + 1) for at in range(first, n_tp)]


def return_order(n_tp):
    far = n_tp // 2
    return list(range(far, 1, -1)) + list(range(n_tp - 1, far, -1)) + list(range(min(2, n_tp)))[::-1]


def solution(mesh):
    in_specs = (
        P(("grp", "sp", "tp"), None),
        P(("grp", "sp"), "tp"),
        P(),
        P(),
        P(),
        P(),
        P(),
        P("sp", None, "tp"),
        P("sp", None, "tp"),
        P("sp", "tp", None),
        P(("grp", "sp", "tp"), None),
        P(("grp", "sp", "tp"), None),
        P(),
    )
    out_specs = P(("grp", "sp", "tp"), None)

    return jax.shard_map(
        per_device, mesh=mesh, in_specs=in_specs, out_specs=out_specs, check_vma=False
    )
```

```python
import jax
import jax.numpy as jnp
from jax import lax
from jax.experimental import pallas as pl
from jax.experimental.pallas import tpu as pltpu
from jax.sharding import PartitionSpec as P


GROUPS = 4
GROUP_DIM = 256
TOP = 2
CAP = 9


pool_windows = (2, 4, 8, 16)
reach_back = 15
norm_eps = 1e-06
clamp_limit = 7.0
glu_alpha = 1.702


def passed_along(x, axis, by):
    size = lax.axis_size(axis)
    pairs = [(i, i + by) for i in range(size) if 0 <= i + by < size]
    return lax.ppermute(x, axis, pairs)


def rotated(x, axis, by):
    size = lax.axis_size(axis)
    return lax.ppermute(x, axis, [(i, (i + by) % size) for i in range(size)])


def rms_scale(values, gain_vec):
    inverse = lax.rsqrt(jnp.mean(values * values, axis=-1, keepdims=True) + norm_eps)
    return values * inverse * gain_vec


def clamped_unit(gate_pre, upward):
    gate_clip = jnp.minimum(gate_pre, clamp_limit)
    linear = jnp.clip(upward, -clamp_limit, clamp_limit)
    return gate_clip * jax.nn.sigmoid(glu_alpha * gate_clip) * (linear + 1.0)


def mixed_window(pool_input):
    seg_rows, channels = pool_input.shape
    last_rows = pool_input[seg_rows - reach_back :]
    before = passed_along(last_rows, "sp", 1)
    extended = jnp.concatenate([before, pool_input], axis=0).astype(jnp.float32)
    first_chan = lax.axis_index("tp") * channels
    chan_group = (first_chan + lax.iota(jnp.int32, channels)) // GROUP_DIM
    positions = lax.axis_index("sp") * seg_rows + lax.iota(jnp.int32, seg_rows)
    window = jnp.zeros((channels,), jnp.int32)
    for group_level, win_len in enumerate(pool_windows):
        window = jnp.where(chan_group == group_level, win_len, window)
    running = jnp.zeros((seg_rows, channels), jnp.float32)
    window_sum = running
    for offset in range(pool_windows[-1]):
        running = running + extended[reach_back - offset : reach_back - offset + seg_rows]
        if offset + 1 in pool_windows:
            window_sum = jnp.where(window[None, :] == offset + 1, running, window_sum)
    divisor = jnp.minimum(positions[:, None] + 1, window[None, :]).astype(jnp.float32)
    return (window_sum / divisor - extended[reach_back:]).astype(jnp.bfloat16)


def reached(i, d, n):
    return i ^ d if n & (n - 1) == 0 else (i + d) % n


def offset_to(target, i, n):
    return target ^ i if n & (n - 1) == 0 else (target - i) % n


def moved(x, axis, d, back=False):
    size = lax.axis_size(axis)
    pairs = [(i, reached(i, d, size)) for i in range(size)]
    return lax.ppermute(x, axis, [(b, a) for a, b in pairs] if back else pairs)


LANES = 128
IN_VMEM = pl.BlockSpec(memory_space=pltpu.VMEM)
IN_SMEM = pl.BlockSpec(memory_space=pltpu.SMEM)


def load_body(*refs):
    half = len(refs) // 2
    sources, targets, done = refs[:half], refs[half:-1], refs[-1]
    copies = []
    for source, target in zip(sources, targets):
        parts = range(source.shape[0]) if len(source.shape) == 3 else [...]
        for e in parts:
            at = done.at[len(copies)]
            copies.append(pltpu.make_async_copy(source.at[e], target.at[e], at))
    for copy in copies:
        copy.start()
    for copy in copies:
        copy.wait()


LOAD_LIMIT = 28


def load(*weights):
    count = sum(w.shape[0] if w.ndim == 3 else 1 for w in weights)
    return pl.pallas_call(
        load_body,
        in_specs=[pl.BlockSpec(memory_space=pltpu.HBM)] * len(weights),
        out_specs=[IN_VMEM] * len(weights),
        out_shape=[pltpu.VMEM(w.shape, w.dtype) for w in weights],
        scratch_shapes=[pltpu.SemaphoreType.DMA((count,))],
        compiler_params=pltpu.CompilerParams(vmem_limit_bytes=LOAD_LIMIT << 20),
        name="load",
    )(*weights)


def pick_body(at, slot, block, *outs):
    rows = outs[0].shape[0]
    tokens = slot.shape[2]
    ids = lax.broadcasted_iota(jnp.int32, (len(outs) * rows, tokens), 0)
    hit = ids == slot[at, 0:1, :]
    for k in range(1, slot.shape[1]):
        hit = hit | (ids == slot[at, k : k + 1, :])
    chosen = jnp.where(hit, 1.0, 0.0).astype(jnp.bfloat16)
    for j in range(0, block.shape[1], 2 * LANES):
        cols = slice(j, j + 2 * LANES)
        taken = jnp.dot(chosen, block[:, cols], preferred_element_type=jnp.float32)
        for d, out in enumerate(outs):
            out[:, cols] = taken[d * rows : (d + 1) * rows].astype(out.dtype)


def pick(at, slot, block, n_sp, slot_rows):
    shape = jax.ShapeDtypeStruct((slot_rows, block.shape[1]), block.dtype)
    return pl.pallas_call(
        lambda *refs: pick_body(at, *refs),
        in_specs=[IN_VMEM] * 2,
        out_specs=[IN_VMEM] * n_sp,
        out_shape=[shape] * n_sp,
        compiler_params=pltpu.CompilerParams(vmem_limit_bytes=6 << 20),
        name="pick",
    )(slot, block)


def shares_of(at, slot, weight, d, rows):
    ids = lax.broadcasted_iota(jnp.int32, (slot.shape[1], rows), 1) + d * rows
    share = jnp.zeros((slot.shape[1], rows), jnp.float32)
    for k in range(slot.shape[2]):
        share = share + jnp.where(ids == slot[at, :, k : k + 1], weight[at, :, k : k + 1], 0.0)
    return share.astype(jnp.bfloat16)


def combine_body(at, n_back, slot, weight, *refs):
    backs, joined, out = refs[:n_back], refs[n_back:-1], refs[-1]
    rows = backs[0].shape[0]
    share = [shares_of(at, slot, weight, d, rows) for d in range(len(backs))]
    for j in range(0, out.shape[1], 2 * LANES):
        cols = slice(j, j + 2 * LANES)
        total = None
        for d, back in enumerate(backs):
            term = jnp.dot(share[d], back[:, cols], preferred_element_type=jnp.float32)
            total = term if total is None else total + term
        for other in joined:
            total = total + other[:, cols].astype(jnp.float32)
        out[:, cols] = total.astype(out.dtype)


def combine(at, slot, weight, backs, joined):
    shape = jax.ShapeDtypeStruct((slot.shape[1], backs[0].shape[1]), jnp.bfloat16)
    return pl.pallas_call(
        lambda *refs: combine_body(at, len(backs), *refs),
        in_specs=[IN_VMEM] * (2 + len(backs) + len(joined)),
        out_specs=IN_VMEM,
        out_shape=shape,
        compiler_params=pltpu.CompilerParams(vmem_limit_bytes=6 << 20),
        name="combine",
    )(slot, weight, *backs, *joined)


def finish_body(at, n_back, slot, weight, resid, gain, *refs):
    backs, parts, (out, mix) = refs[:n_back], refs[n_back:-2], refs[-2:]
    rows, width = backs[0].shape[0], out.shape[1]
    share = [shares_of(at, slot, weight, d, rows) for d in range(n_back)]
    square = jnp.zeros((out.shape[0], LANES), jnp.float32)
    for j in range(0, width, 2 * LANES):
        cols = slice(j, j + 2 * LANES)
        total = parts[0][:, cols].astype(jnp.float32) if parts else 0.0
        for part in parts[1:]:
            total = total + part[:, cols].astype(jnp.float32)
        for d, back in enumerate(backs):
            total = total + jnp.dot(share[d], back[:, cols], preferred_element_type=jnp.float32)
        mix[:, cols] = total
        square = square + total[:, :LANES] * total[:, :LANES]
        square = square + total[:, LANES:] * total[:, LANES:]
    mean = jnp.sum(square, axis=1, keepdims=True) / width
    inverse = lax.rsqrt(mean + norm_eps)
    for j in range(0, width, 2 * LANES):
        cols = slice(j, j + 2 * LANES)
        scaled = mix[:, cols] * inverse * gain[:, cols]
        out[:, cols] = (resid[:, cols].astype(jnp.float32) + scaled).astype(out.dtype)


def finish(at, slot, weight, resid, gain, backs, parts):
    return pl.pallas_call(
        lambda *refs: finish_body(at, len(backs), *refs),
        in_specs=[IN_VMEM] * (4 + len(backs) + len(parts)),
        out_specs=IN_VMEM,
        out_shape=jax.ShapeDtypeStruct(resid.shape, resid.dtype),
        scratch_shapes=[pltpu.VMEM(resid.shape, jnp.float32)],
        compiler_params=pltpu.CompilerParams(vmem_limit_bytes=6 << 20),
        name="finish",
    )(slot, weight, resid, gain.reshape(1, -1), *backs, *parts)


def experts_body(n_src, *refs):
    xs, (wg, wu, wd) = refs[:n_src], refs[n_src : n_src + 3]
    outs, (into, outof) = refs[n_src + 3 : 2 * n_src + 3], refs[2 * n_src + 3 :]
    count, width = wg.shape[0], xs[0].shape[1]
    tiles, left = divmod(xs[0].shape[0] // count, 8)
    whole = count * tiles * 8
    for s, x in enumerate(xs):
        for j in range(width // LANES):
            cols = slice(j * LANES, (j + 1) * LANES)
            into[j, s * left * count : (s + 1) * left * count, :] = x[whole:, cols].astype(
                jnp.float32
            )

    def one(e, carry):
        own = [pl.ds(pl.multiple_of((e * tiles + i) * 8, 8), 8) for i in range(tiles)]
        apart = pl.ds(e, n_src * left, stride=count)
        taken = [x[at, :].astype(jnp.float32) for x in xs for at in own]
        taken.append(jnp.concatenate([into[j, apart, :] for j in range(width // LANES)], axis=1))
        taken = jnp.concatenate(taken, axis=0).astype(jnp.bfloat16)
        gate_pre = jnp.dot(taken, wg[e], preferred_element_type=jnp.float32)
        upward = jnp.dot(taken, wu[e], preferred_element_type=jnp.float32)
        activated = clamped_unit(gate_pre, upward).astype(jnp.bfloat16)
        result = jnp.dot(activated, wd[e], preferred_element_type=jnp.float32)
        row = 0
        for out in outs:
            for at in own:
                out[at, :] = result[row : row + 8].astype(out.dtype)
                row += 8
        for j in range(width // LANES):
            outof[j, apart, :] = result[row:, j * LANES : (j + 1) * LANES]
        return carry

    lax.fori_loop(0, count, one, 0, unroll=EXPERT_UNROLL)
    for s, out in enumerate(outs):
        for j in range(width // LANES):
            cols = slice(j * LANES, (j + 1) * LANES)
            out[whole:, cols] = outof[j, s * left * count : (s + 1) * left * count, :].astype(
                out.dtype
            )


EXPERT_UNROLL = 2


def experts(xs, w_gate, w_up, w_down):
    count, width, hidden = w_gate.shape
    rows, n_src = xs[0].shape[0], len(xs)
    left = rows // count % 8
    scratch = pltpu.VMEM((width // LANES, n_src * left * count, LANES), jnp.float32)
    flops = 6 * n_src * rows * width * hidden
    moved_bytes = 3 * count * width * hidden * 2 + 4 * n_src * rows * width
    return pl.pallas_call(
        lambda *refs: experts_body(n_src, *refs),
        in_specs=[IN_VMEM] * (n_src + 3),
        out_specs=[IN_VMEM] * n_src,
        out_shape=[jax.ShapeDtypeStruct((rows, width), jnp.bfloat16)] * n_src,
        scratch_shapes=[scratch, scratch],
        cost_estimate=pl.CostEstimate(flops=flops, bytes_accessed=moved_bytes, transcendentals=0),
        compiler_params=pltpu.CompilerParams(vmem_limit_bytes=6 << 20),
        name="experts",
    )(*xs, w_gate, w_up, w_down)


def plain_path(
    resid_in,
    pool_input,
    pool_weight,
    pool_scale,
    out_weight,
    mix_gain,
    ffn_gain,
    w_gate,
    w_up,
    w_down,
    routes,
    route_weight,
    post_gain,
):
    n_sp = lax.axis_size("sp")
    n_tp = lax.axis_size("tp")
    tok_rows, width = resid_in.shape
    channels = pool_input.shape[1]
    local_experts = w_gate.shape[0]
    n_experts = local_experts * n_sp
    assert n_experts <= 256
    slot_rows = local_experts * CAP
    slot_total = n_sp * slot_rows

    fields = jnp.concatenate([routes.astype(jnp.bfloat16).T, route_weight.astype(jnp.bfloat16).T])
    n_fields = fields.size
    field_rows = -(-n_fields // (8 * channels)) * 8
    fields = jnp.pad(fields.reshape(-1), (0, field_rows * channels - n_fields))
    fields = jnp.broadcast_to(fields.reshape(1, field_rows, channels), (n_tp, field_rows, channels))
    mixed_rows = mixed_window(pool_input).reshape(n_tp, tok_rows, channels)
    sent = jnp.concatenate([mixed_rows, fields], axis=1)
    got = lax.all_to_all(sent, "tp", split_axis=0, concat_axis=0, tiled=True)
    token_mixed = got[:, :tok_rows].transpose(1, 0, 2).reshape(tok_rows, n_tp * channels)
    fields = got[:, tok_rows:].reshape(n_tp, -1)[:, :n_fields].reshape(n_tp, 2 * TOP, tok_rows)

    pooled = jnp.einsum(
        "tgc,gcd->tgd",
        token_mixed.reshape(tok_rows, GROUPS, GROUP_DIM),
        pool_weight,
        preferred_element_type=jnp.float32,
    )
    pooled = (
        (pooled * pool_scale.reshape(GROUPS, GROUP_DIM)).astype(jnp.bfloat16).reshape(tok_rows, -1)
    )
    mix_out = jnp.dot(pooled, out_weight, preferred_element_type=jnp.float32)
    residual = (resid_in.astype(jnp.float32) + rms_scale(mix_out, mix_gain)).astype(jnp.bfloat16)
    normed = rms_scale(residual.astype(jnp.float32), ffn_gain).astype(jnp.bfloat16)

    far = n_tp // 2
    order = list(range(far + 1)) + list(range(n_tp - 1, far, -1))
    blocks = {0: normed, n_tp: normed}
    for k in order:
        if k:
            by = 1 if k <= far else -1
            blocks[k] = rotated(blocks[k - by], "tp", by)

    here = lax.axis_index("tp")
    fields = jnp.take(fields, (here - jnp.array(order)) % n_tp, axis=0)
    route = fields[:, :TOP].astype(jnp.int32)
    weight = fields[:, TOP:].astype(jnp.float32)
    onehot = route[..., None] == lax.iota(jnp.int32, n_experts)
    named = jnp.sum(onehot.astype(jnp.float32), axis=1)
    earlier = lax.iota(jnp.int32, tok_rows)[:, None] > lax.iota(jnp.int32, tok_rows)[None, :]
    rank = jnp.einsum(
        "ut,bte->bue",
        earlier.astype(jnp.bfloat16),
        named.astype(jnp.bfloat16),
        preferred_element_type=jnp.float32,
    )
    slot_rank = jnp.sum(rank[:, None] * onehot, axis=-1).astype(jnp.int32)

    slot_index = route * CAP + slot_rank
    picker = slot_index[..., None] == lax.iota(jnp.int32, slot_total)
    token_pick = jnp.sum(picker.astype(jnp.float32), axis=1).astype(jnp.bfloat16)
    token_weight = jnp.sum(jnp.where(picker, weight[..., None], 0.0), axis=1)
    token_weight = token_weight.astype(jnp.bfloat16)
    arrived = []
    for at, k in enumerate(order):
        rows = lax.dot_general(
            token_pick[at],
            blocks[k],
            (((0,), (0,)), ((), ())),
            preferred_element_type=jnp.float32,
        )
        rows = rows.astype(jnp.bfloat16).reshape(n_sp, slot_rows, width)
        arrived.append(lax.all_to_all(rows, "sp", split_axis=0, concat_axis=0, tiled=True))
    arrived = jnp.stack(arrived).reshape(n_tp, n_sp, local_experts, CAP, width)
    f32 = {"preferred_element_type": jnp.float32}
    gate_pre = jnp.einsum("sklcd,ldf->sklcf", arrived, w_gate, **f32)
    upward = jnp.einsum("sklcd,ldf->sklcf", arrived, w_up, **f32)
    activated = clamped_unit(gate_pre, upward).astype(jnp.bfloat16)
    terms = jnp.einsum("sklcf,lfd->sklcd", activated, w_down, **f32)
    terms = terms.astype(jnp.bfloat16).reshape(n_tp, n_sp, slot_rows, width)
    parts = {}
    for at, k in enumerate(order):
        back = lax.all_to_all(terms[at], "sp", split_axis=0, concat_axis=0, tiled=True)
        part = jnp.dot(token_weight[at], back.reshape(slot_total, width), **f32)
        part = part.astype(jnp.bfloat16)
        parts[k] = rotated(part, "tp", -k) if k else part
    expert_mix = sum(parts[k].astype(jnp.float32) for k in order)
    return (residual.astype(jnp.float32) + rms_scale(expert_mix, post_gain)).astype(jnp.bfloat16)


AHEAD = 16


def cut_body(place, x, routes, weights, *outs):
    chunks, tail = outs[:-1], outs[-1]
    n_tp, rows = len(chunks), routes.shape[0]
    top = routes.shape[1]
    lane = lax.broadcasted_iota(jnp.int32, (rows, rows), 1)
    fields = jnp.zeros((rows, rows), jnp.float32)
    for k in range(top):
        fields = jnp.where(lane == k, routes[:, k : k + 1].astype(jnp.float32), fields)
        fields = jnp.where(lane == top + k, weights[:, k : k + 1], fields)
    fields = fields.T[:8].astype(jnp.bfloat16)
    for k, chunk in enumerate(chunks):
        first = (place[0] + k) % n_tp * rows
        before = pl.multiple_of(jnp.maximum(first - AHEAD, 0), AHEAD)
        chunk[:AHEAD, :] = x[pl.ds(before, AHEAD), :]
        chunk[AHEAD : AHEAD + rows, :] = x[pl.ds(pl.multiple_of(first, AHEAD), rows), :]
        chunk[AHEAD + rows :, :] = jnp.zeros((8, chunk.shape[1]), jnp.bfloat16)
        chunk[AHEAD + rows :, :rows] = fields
    tail[...] = x[x.shape[0] - AHEAD :, :]


def cut(place, x, routes, weights, n_tp):
    rows, channels = routes.shape[0], x.shape[1]
    chunk = jax.ShapeDtypeStruct((AHEAD + rows + 8, channels), x.dtype)
    return pl.pallas_call(
        cut_body,
        in_specs=[IN_SMEM] + [IN_VMEM] * 3,
        out_specs=[IN_VMEM] * (n_tp + 1),
        out_shape=[chunk] * n_tp + [jax.ShapeDtypeStruct((AHEAD, channels), x.dtype)],
        compiler_params=pltpu.CompilerParams(vmem_limit_bytes=6 << 20),
        name="cut",
    )(place, x, routes, weights)


def mix_body(n_tp, place, *refs):
    chunks, halos = refs[:n_tp], refs[n_tp : 2 * n_tp]
    pool_w, scale, out_w, mix_gain, ffn_gain, resid = refs[2 * n_tp : 2 * n_tp + 6]
    residual, normed, raw, pooled, mix = refs[2 * n_tp + 6 :]
    rows, width = resid.shape
    channels = chunks[0].shape[1]
    tp, sp = place[0], place[1]
    for k, chunk in enumerate(chunks):
        source = (tp - k + n_tp) % n_tp
        cols = pl.ds(pl.multiple_of(source * channels, LANES), channels)
        raw[:, cols] = chunk[: AHEAD + rows, :].astype(jnp.float32)

    @pl.when(tp == 0)
    def _():
        for j, halo in enumerate(halos):
            raw[:AHEAD, j * channels : (j + 1) * channels] = halo[...].astype(jnp.float32)

    start = (sp * n_tp + tp) * rows
    position = start + lax.broadcasted_iota(jnp.int32, (rows, GROUP_DIM), 0) + 1
    for g, window in enumerate(pool_windows):
        cols = slice(g * GROUP_DIM, (g + 1) * GROUP_DIM)
        own = raw[:, cols]
        total, reach = own, 1
        while reach < window:
            total = total + pltpu.roll(total, reach, 0)
            reach = 2 * reach
        divisor = jnp.minimum(position, window).astype(jnp.float32)
        mixed = (total[AHEAD:] / divisor - own[AHEAD:]).astype(jnp.bfloat16)
        part = jnp.dot(mixed, pool_w[g], preferred_element_type=jnp.float32)
        pooled[:, cols] = (part * scale[:, cols]).astype(jnp.bfloat16)

    def columns():
        return [slice(j, j + 2 * LANES) for j in range(0, width, 2 * LANES)]

    def inverse_of(square):
        return lax.rsqrt(jnp.sum(square, axis=1, keepdims=True) / width + norm_eps)

    square = jnp.zeros((rows, LANES), jnp.float32)
    for cols in columns():
        part = jnp.dot(pooled[...], out_w[:, cols], preferred_element_type=jnp.float32)
        mix[:, cols] = part
        square = square + part[:, :LANES] * part[:, :LANES] + part[:, LANES:] * part[:, LANES:]
    inverse = inverse_of(square)
    square = jnp.zeros((rows, LANES), jnp.float32)
    for cols in columns():
        part = resid[:, cols].astype(jnp.float32) + mix[:, cols] * inverse * mix_gain[:, cols]
        part = part.astype(jnp.bfloat16)
        residual[:, cols] = part
        part = part.astype(jnp.float32)
        square = square + part[:, :LANES] * part[:, :LANES] + part[:, LANES:] * part[:, LANES:]
    inverse = inverse_of(square)
    for cols in columns():
        part = residual[:, cols].astype(jnp.float32) * inverse * ffn_gain[:, cols]
        normed[:, cols] = part.astype(normed.dtype)


def mix_tokens(place, chunks, halos, pool_w, scale, out_w, mix_gain, ffn_gain, resid):
    rows, width = resid.shape
    total = out_w.shape[0]
    return pl.pallas_call(
        lambda *refs: mix_body(len(chunks), *refs),
        in_specs=[IN_SMEM] + [IN_VMEM] * (2 * len(chunks) + 6),
        out_specs=[IN_VMEM] * 2,
        out_shape=[jax.ShapeDtypeStruct(resid.shape, resid.dtype)] * 2,
        scratch_shapes=[
            pltpu.VMEM((AHEAD + rows, total), jnp.float32),
            pltpu.VMEM((rows, total), jnp.bfloat16),
            pltpu.VMEM((rows, width), jnp.float32),
        ],
        compiler_params=pltpu.CompilerParams(vmem_limit_bytes=12 << 20),
        name="mix",
    )(
        place,
        *chunks,
        *halos,
        pool_w,
        scale,
        out_w,
        mix_gain,
        ffn_gain,
        resid,
    )


def slots_body(n_sp, local, place, *refs):
    chunks, (slot, by_row, weight) = refs[:-3], refs[-3:]
    top, tokens = slot.shape[1], slot.shape[2]
    n_experts = n_sp * local
    expert = lax.broadcasted_iota(jnp.int32, (n_experts, tokens), 0)
    row = lax.broadcasted_iota(jnp.int32, (tokens, tokens), 0)
    lane = lax.broadcasted_iota(jnp.int32, (tokens, tokens), 1)
    before = jnp.where(row < lane, 1.0, 0.0).astype(jnp.bfloat16)
    whole = CAP // 8 * 8
    for at, chunk in enumerate(chunks):
        first = chunk.shape[0] - 8
        fields = chunk[first:, :tokens].astype(jnp.float32)
        hits = [
            jnp.where(expert == fields[k : k + 1].astype(jnp.int32), 1.0, 0.0) for k in range(top)
        ]
        named = sum(hits).astype(jnp.bfloat16)
        rank = jnp.dot(named, before, preferred_element_type=jnp.float32)
        found = []
        for k, hit in enumerate(hits):
            mine = jnp.sum(rank * hit, axis=0, keepdims=True).astype(jnp.int32)
            route = jnp.sum(expert.astype(jnp.float32) * hit, axis=0, keepdims=True)
            owner = jnp.sum(
                (expert // local).astype(jnp.float32) * hit, axis=0, keepdims=True
            ).astype(jnp.int32)
            inside = route.astype(jnp.int32) - owner * local
            owner = offset_to(owner, place[1], n_sp)
            in_tile = inside * whole + mine
            apart = local * whole + (mine - whole) * local + inside
            found.append(owner * local * CAP + jnp.where(mine < whole, in_tile, apart))
            slot[at, k : k + 1, :] = found[-1]
        rows8 = [x.astype(jnp.float32) for x in found] + [fields[top : 2 * top]]
        rows8.append(jnp.zeros((tokens - 2 * top, tokens), jnp.float32))
        turned = jnp.concatenate(rows8, axis=0).T
        by_row[at] = turned[:, :top].astype(jnp.int32)
        weight[at] = turned[:, top : 2 * top]


def slots(place, chunks, n_sp, local, top, tokens):
    n = len(chunks)
    return pl.pallas_call(
        lambda *refs: slots_body(n_sp, local, *refs),
        in_specs=[IN_SMEM] + [IN_VMEM] * n,
        out_specs=[IN_VMEM] * 3,
        out_shape=[
            jax.ShapeDtypeStruct((n, top, tokens), jnp.int32),
            jax.ShapeDtypeStruct((n, tokens, top), jnp.int32),
            jax.ShapeDtypeStruct((n, tokens, top), jnp.float32),
        ],
        compiler_params=pltpu.CompilerParams(vmem_limit_bytes=6 << 20),
        name="slots",
    )(place, *chunks)


def kernel_path(
    resid_in,
    pool_input,
    pool_weight,
    pool_scale,
    out_weight,
    mix_gain,
    ffn_gain,
    w_gate,
    w_up,
    w_down,
    routes,
    route_weight,
    post_gain,
):
    n_sp = lax.axis_size("sp")
    n_tp = lax.axis_size("tp")
    tok_rows = resid_in.shape[0]
    local_experts = w_gate.shape[0]
    slot_rows = local_experts * CAP

    place = jnp.stack([lax.axis_index("tp"), lax.axis_index("sp")]).astype(jnp.int32)
    *chunks, tail = cut(place, pool_input, routes, route_weight, n_tp)
    halos = []
    for j in range(n_tp):
        pairs = [(s * n_tp + j, (s + 1) * n_tp) for s in range(n_sp - 1)]
        halos.append(lax.ppermute(tail, ("sp", "tp"), pairs))
    chunks = [rotated(x, "tp", k) if k else x for k, x in enumerate(chunks)]
    small = [x.reshape(1, -1) for x in (pool_scale, mix_gain, ffn_gain)]
    scale, mix_gain, ffn_gain, pool_weight, out_weight, resid_in = load(
        *small, pool_weight, out_weight, resid_in
    )
    residual, normed = mix_tokens(
        place, chunks, halos, pool_weight, scale, out_weight, mix_gain, ffn_gain, resid_in
    )

    far = n_tp // 2
    order = list(range(far + 1)) + list(range(n_tp - 1, far, -1))
    blocks = {0: normed, n_tp: normed}
    for k in order:
        if k:
            by = 1 if k <= far else -1
            blocks[k] = rotated(blocks[k - by], "tp", by)

    slot, by_row, weight = slots(
        place, [chunks[k] for k in order], n_sp, local_experts, TOP, tok_rows
    )
    weights = load(w_gate, w_up, w_down)
    arrived, backs, parts = [], {}, {}
    for at, k in enumerate(order):
        rows = pick(at, slot, blocks[k], n_sp, slot_rows)
        arrived.append([moved(x, "sp", d) if d else x for d, x in enumerate(rows)])
    for first, stop in groups_of(n_tp):
        group = arrived[first:stop]
        terms = experts([x for xs in group for x in xs], *weights)
        for at in range(first, stop):
            back = terms[(at - first) * n_sp : (at - first + 1) * n_sp]
            backs[at] = [moved(x, "sp", d, True) if d else x for d, x in enumerate(back)]
    for at in return_order(n_tp)[:-1]:
        k = order[at]
        by = -1 if k <= far else 1
        inner = k < far or k > far + 1
        joined = [parts.pop(k - by)] if inner else []
        part = combine(at, by_row, weight, backs[at], joined)
        parts[k] = rotated(part, "tp", by)
    return finish(0, by_row, weight, residual, post_gain, backs[0], list(parts.values()))


def per_device(*args):
    pool_input, w_gate, routes = args[1], args[7], args[10]
    n_sp = lax.axis_size("sp")
    fits = w_gate.shape[0] % 8 == 0 and CAP % 8 and n_sp <= 4 and w_gate.shape[0] * n_sp <= 256
    fits = fits and routes.shape[0] == LANES and pool_input.shape[1] % LANES == 0
    return kernel_path(*args) if fits else plain_path(*args)


def groups_of(n_tp):
    first = min(2, n_tp)
    return [(0, first)] + [(at, at + 1) for at in range(first, n_tp)]


def return_order(n_tp):
    far = n_tp // 2
    return list(range(far, 1, -1)) + list(range(n_tp - 1, far, -1)) + list(range(min(2, n_tp)))[::-1]


def solution(mesh):
    in_specs = (
        P(("grp", "sp", "tp"), None),
        P(("grp", "sp"), "tp"),
        P(),
        P(),
        P(),
        P(),
        P(),
        P("sp", None, "tp"),
        P("sp", None, "tp"),
        P("sp", "tp", None),
        P(("grp", "sp", "tp"), None),
        P(("grp", "sp", "tp"), None),
        P(),
    )
    out_specs = P(("grp", "sp", "tp"), None)

    return jax.shard_map(
        per_device, mesh=mesh, in_specs=in_specs, out_specs=out_specs, check_vma=False
    )
```

```python
import jax
import jax.numpy as jnp
from jax import lax
from jax.experimental import pallas as pl
from jax.experimental.pallas import tpu as pltpu
from jax.sharding import PartitionSpec as P


GROUPS = 4
GROUP_DIM = 256
TOP = 2
CAP = 9


pool_windows = (2, 4, 8, 16)
reach_back = 15
norm_eps = 1e-06
clamp_limit = 7.0
glu_alpha = 1.702


def passed_along(x, axis, by):
    size = lax.axis_size(axis)
    pairs = [(i, i + by) for i in range(size) if 0 <= i + by < size]
    return lax.ppermute(x, axis, pairs)


def rotated(x, axis, by):
    size = lax.axis_size(axis)
    return lax.ppermute(x, axis, [(i, (i + by) % size) for i in range(size)])


def rms_scale(values, gain_vec):
    inverse = lax.rsqrt(jnp.mean(values * values, axis=-1, keepdims=True) + norm_eps)
    return values * inverse * gain_vec


def clamped_unit(gate_pre, upward):
    gate_clip = jnp.minimum(gate_pre, clamp_limit)
    linear = jnp.clip(upward, -clamp_limit, clamp_limit)
    return gate_clip * jax.nn.sigmoid(glu_alpha * gate_clip) * (linear + 1.0)


def mixed_window(pool_input):
    seg_rows, channels = pool_input.shape
    last_rows = pool_input[seg_rows - reach_back :]
    before = passed_along(last_rows, "sp", 1)
    extended = jnp.concatenate([before, pool_input], axis=0).astype(jnp.float32)
    first_chan = lax.axis_index("tp") * channels
    chan_group = (first_chan + lax.iota(jnp.int32, channels)) // GROUP_DIM
    positions = lax.axis_index("sp") * seg_rows + lax.iota(jnp.int32, seg_rows)
    window = jnp.zeros((channels,), jnp.int32)
    for group_level, win_len in enumerate(pool_windows):
        window = jnp.where(chan_group == group_level, win_len, window)
    running = jnp.zeros((seg_rows, channels), jnp.float32)
    window_sum = running
    for offset in range(pool_windows[-1]):
        running = running + extended[reach_back - offset : reach_back - offset + seg_rows]
        if offset + 1 in pool_windows:
            window_sum = jnp.where(window[None, :] == offset + 1, running, window_sum)
    divisor = jnp.minimum(positions[:, None] + 1, window[None, :]).astype(jnp.float32)
    return (window_sum / divisor - extended[reach_back:]).astype(jnp.bfloat16)


def reached(i, d, n):
    return i ^ d if n & (n - 1) == 0 else (i + d) % n


def offset_to(target, i, n):
    return target ^ i if n & (n - 1) == 0 else (target - i) % n


def moved(x, axis, d, back=False):
    size = lax.axis_size(axis)
    pairs = [(i, reached(i, d, size)) for i in range(size)]
    return lax.ppermute(x, axis, [(b, a) for a, b in pairs] if back else pairs)


LANES = 128
IN_VMEM = pl.BlockSpec(memory_space=pltpu.VMEM)
IN_SMEM = pl.BlockSpec(memory_space=pltpu.SMEM)


def load_body(*refs):
    half = len(refs) // 2
    sources, targets, done = refs[:half], refs[half:-1], refs[-1]
    copies = []
    for source, target in zip(sources, targets):
        parts = range(source.shape[0]) if len(source.shape) == 3 else [...]
        for e in parts:
            at = done.at[len(copies)]
            copies.append(pltpu.make_async_copy(source.at[e], target.at[e], at))
    for copy in copies:
        copy.start()
    for copy in copies:
        copy.wait()


LOAD_LIMIT = 28
EARLY_LIMIT = 55
CUT_LIMIT = 60


def load(*weights, limit=LOAD_LIMIT):
    count = sum(w.shape[0] if w.ndim == 3 else 1 for w in weights)
    return pl.pallas_call(
        load_body,
        in_specs=[pl.BlockSpec(memory_space=pltpu.HBM)] * len(weights),
        out_specs=[IN_VMEM] * len(weights),
        out_shape=[pltpu.VMEM(w.shape, w.dtype) for w in weights],
        scratch_shapes=[pltpu.SemaphoreType.DMA((count,))],
        compiler_params=pltpu.CompilerParams(vmem_limit_bytes=limit << 20),
        name="load",
    )(*weights)


def pick_body(at, slot, block, *outs):
    rows = outs[0].shape[0]
    tokens = slot.shape[2]
    ids = lax.broadcasted_iota(jnp.int32, (len(outs) * rows, tokens), 0)
    hit = ids == slot[at, 0:1, :]
    for k in range(1, slot.shape[1]):
        hit = hit | (ids == slot[at, k : k + 1, :])
    chosen = jnp.where(hit, 1.0, 0.0).astype(jnp.bfloat16)
    for j in range(0, block.shape[1], 2 * LANES):
        cols = slice(j, j + 2 * LANES)
        taken = jnp.dot(chosen, block[:, cols], preferred_element_type=jnp.float32)
        for d, out in enumerate(outs):
            out[:, cols] = taken[d * rows : (d + 1) * rows].astype(out.dtype)


def pick(at, slot, block, n_sp, slot_rows):
    shape = jax.ShapeDtypeStruct((slot_rows, block.shape[1]), block.dtype)
    return pl.pallas_call(
        lambda *refs: pick_body(at, *refs),
        in_specs=[IN_VMEM] * 2,
        out_specs=[IN_VMEM] * n_sp,
        out_shape=[shape] * n_sp,
        compiler_params=pltpu.CompilerParams(vmem_limit_bytes=6 << 20),
        name="pick",
    )(slot, block)


def shares_of(at, slot, weight, d, rows):
    ids = lax.broadcasted_iota(jnp.int32, (slot.shape[1], rows), 1) + d * rows
    share = jnp.zeros((slot.shape[1], rows), jnp.float32)
    for k in range(slot.shape[2]):
        share = share + jnp.where(ids == slot[at, :, k : k + 1], weight[at, :, k : k + 1], 0.0)
    return share.astype(jnp.bfloat16)


def combine_body(at, n_back, slot, weight, *refs):
    backs, joined, out = refs[:n_back], refs[n_back:-1], refs[-1]
    rows = backs[0].shape[0]
    share = [shares_of(at, slot, weight, d, rows) for d in range(len(backs))]
    for j in range(0, out.shape[1], 2 * LANES):
        cols = slice(j, j + 2 * LANES)
        total = None
        for d, back in enumerate(backs):
            term = jnp.dot(share[d], back[:, cols], preferred_element_type=jnp.float32)
            total = term if total is None else total + term
        for other in joined:
            total = total + other[:, cols].astype(jnp.float32)
        out[:, cols] = total.astype(out.dtype)


def combine(at, slot, weight, backs, joined):
    shape = jax.ShapeDtypeStruct((slot.shape[1], backs[0].shape[1]), jnp.bfloat16)
    return pl.pallas_call(
        lambda *refs: combine_body(at, len(backs), *refs),
        in_specs=[IN_VMEM] * (2 + len(backs) + len(joined)),
        out_specs=IN_VMEM,
        out_shape=shape,
        compiler_params=pltpu.CompilerParams(vmem_limit_bytes=6 << 20),
        name="combine",
    )(slot, weight, *backs, *joined)


def finish_body(at, n_back, slot, weight, resid, gain, *refs):
    backs, parts, (out, mix) = refs[:n_back], refs[n_back:-2], refs[-2:]
    rows, width = backs[0].shape[0], out.shape[1]
    share = [shares_of(at, slot, weight, d, rows) for d in range(n_back)]
    square = jnp.zeros((out.shape[0], LANES), jnp.float32)
    for j in range(0, width, 2 * LANES):
        cols = slice(j, j + 2 * LANES)
        total = parts[0][:, cols].astype(jnp.float32) if parts else 0.0
        for part in parts[1:]:
            total = total + part[:, cols].astype(jnp.float32)
        for d, back in enumerate(backs):
            total = total + jnp.dot(share[d], back[:, cols], preferred_element_type=jnp.float32)
        mix[:, cols] = total
        square = square + total[:, :LANES] * total[:, :LANES]
        square = square + total[:, LANES:] * total[:, LANES:]
    mean = jnp.sum(square, axis=1, keepdims=True) / width
    inverse = lax.rsqrt(mean + norm_eps)
    for j in range(0, width, 2 * LANES):
        cols = slice(j, j + 2 * LANES)
        scaled = mix[:, cols] * inverse * gain[:, cols]
        out[:, cols] = (resid[:, cols].astype(jnp.float32) + scaled).astype(out.dtype)


def finish(at, slot, weight, resid, gain, backs, parts):
    return pl.pallas_call(
        lambda *refs: finish_body(at, len(backs), *refs),
        in_specs=[IN_VMEM] * (4 + len(backs) + len(parts)),
        out_specs=IN_VMEM,
        out_shape=jax.ShapeDtypeStruct(resid.shape, resid.dtype),
        scratch_shapes=[pltpu.VMEM(resid.shape, jnp.float32)],
        compiler_params=pltpu.CompilerParams(vmem_limit_bytes=6 << 20),
        name="finish",
    )(slot, weight, resid, gain.reshape(1, -1), *backs, *parts)


def experts_body(n_src, *refs):
    xs, (wg, wu, wd) = refs[:n_src], refs[n_src : n_src + 3]
    outs, (into, outof) = refs[n_src + 3 : 2 * n_src + 3], refs[2 * n_src + 3 :]
    count, width = wg.shape[0], xs[0].shape[1]
    tiles, left = divmod(xs[0].shape[0] // count, 8)
    whole = count * tiles * 8
    for s, x in enumerate(xs):
        for j in range(width // LANES):
            cols = slice(j * LANES, (j + 1) * LANES)
            into[j, s * left * count : (s + 1) * left * count, :] = x[whole:, cols].astype(
                jnp.float32
            )

    def one(e, carry):
        own = [pl.ds(pl.multiple_of((e * tiles + i) * 8, 8), 8) for i in range(tiles)]
        apart = pl.ds(e, n_src * left, stride=count)
        taken = [x[at, :].astype(jnp.float32) for x in xs for at in own]
        taken.append(jnp.concatenate([into[j, apart, :] for j in range(width // LANES)], axis=1))
        taken = jnp.concatenate(taken, axis=0).astype(jnp.bfloat16)
        gate_pre = jnp.dot(taken, wg[e], preferred_element_type=jnp.float32)
        upward = jnp.dot(taken, wu[e], preferred_element_type=jnp.float32)
        activated = clamped_unit(gate_pre, upward).astype(jnp.bfloat16)
        result = jnp.dot(activated, wd[e], preferred_element_type=jnp.float32)
        row = 0
        for out in outs:
            for at in own:
                out[at, :] = result[row : row + 8].astype(out.dtype)
                row += 8
        for j in range(width // LANES):
            outof[j, apart, :] = result[row:, j * LANES : (j + 1) * LANES]
        return carry

    lax.fori_loop(0, count, one, 0, unroll=EXPERT_UNROLL)
    for s, out in enumerate(outs):
        for j in range(width // LANES):
            cols = slice(j * LANES, (j + 1) * LANES)
            out[whole:, cols] = outof[j, s * left * count : (s + 1) * left * count, :].astype(
                out.dtype
            )


EXPERT_UNROLL = 2


def experts(xs, w_gate, w_up, w_down):
    count, width, hidden = w_gate.shape
    rows, n_src = xs[0].shape[0], len(xs)
    left = rows // count % 8
    scratch = pltpu.VMEM((width // LANES, n_src * left * count, LANES), jnp.float32)
    flops = 6 * n_src * rows * width * hidden
    moved_bytes = 3 * count * width * hidden * 2 + 4 * n_src * rows * width
    return pl.pallas_call(
        lambda *refs: experts_body(n_src, *refs),
        in_specs=[IN_VMEM] * (n_src + 3),
        out_specs=[IN_VMEM] * n_src,
        out_shape=[jax.ShapeDtypeStruct((rows, width), jnp.bfloat16)] * n_src,
        scratch_shapes=[scratch, scratch],
        cost_estimate=pl.CostEstimate(flops=flops, bytes_accessed=moved_bytes, transcendentals=0),
        compiler_params=pltpu.CompilerParams(vmem_limit_bytes=6 << 20),
        name="experts",
    )(*xs, w_gate, w_up, w_down)


def plain_path(
    resid_in,
    pool_input,
    pool_weight,
    pool_scale,
    out_weight,
    mix_gain,
    ffn_gain,
    w_gate,
    w_up,
    w_down,
    routes,
    route_weight,
    post_gain,
):
    n_sp = lax.axis_size("sp")
    n_tp = lax.axis_size("tp")
    tok_rows, width = resid_in.shape
    channels = pool_input.shape[1]
    local_experts = w_gate.shape[0]
    n_experts = local_experts * n_sp
    assert n_experts <= 256
    slot_rows = local_experts * CAP
    slot_total = n_sp * slot_rows

    fields = jnp.concatenate([routes.astype(jnp.bfloat16).T, route_weight.astype(jnp.bfloat16).T])
    n_fields = fields.size
    field_rows = -(-n_fields // (8 * channels)) * 8
    fields = jnp.pad(fields.reshape(-1), (0, field_rows * channels - n_fields))
    fields = jnp.broadcast_to(fields.reshape(1, field_rows, channels), (n_tp, field_rows, channels))
    mixed_rows = mixed_window(pool_input).reshape(n_tp, tok_rows, channels)
    sent = jnp.concatenate([mixed_rows, fields], axis=1)
    got = lax.all_to_all(sent, "tp", split_axis=0, concat_axis=0, tiled=True)
    token_mixed = got[:, :tok_rows].transpose(1, 0, 2).reshape(tok_rows, n_tp * channels)
    fields = got[:, tok_rows:].reshape(n_tp, -1)[:, :n_fields].reshape(n_tp, 2 * TOP, tok_rows)

    pooled = jnp.einsum(
        "tgc,gcd->tgd",
        token_mixed.reshape(tok_rows, GROUPS, GROUP_DIM),
        pool_weight,
        preferred_element_type=jnp.float32,
    )
    pooled = (
        (pooled * pool_scale.reshape(GROUPS, GROUP_DIM)).astype(jnp.bfloat16).reshape(tok_rows, -1)
    )
    mix_out = jnp.dot(pooled, out_weight, preferred_element_type=jnp.float32)
    residual = (resid_in.astype(jnp.float32) + rms_scale(mix_out, mix_gain)).astype(jnp.bfloat16)
    normed = rms_scale(residual.astype(jnp.float32), ffn_gain).astype(jnp.bfloat16)

    far = n_tp // 2
    order = list(range(far + 1)) + list(range(n_tp - 1, far, -1))
    blocks = {0: normed, n_tp: normed}
    for k in order:
        if k:
            by = 1 if k <= far else -1
            blocks[k] = rotated(blocks[k - by], "tp", by)

    here = lax.axis_index("tp")
    fields = jnp.take(fields, (here - jnp.array(order)) % n_tp, axis=0)
    route = fields[:, :TOP].astype(jnp.int32)
    weight = fields[:, TOP:].astype(jnp.float32)
    onehot = route[..., None] == lax.iota(jnp.int32, n_experts)
    named = jnp.sum(onehot.astype(jnp.float32), axis=1)
    earlier = lax.iota(jnp.int32, tok_rows)[:, None] > lax.iota(jnp.int32, tok_rows)[None, :]
    rank = jnp.einsum(
        "ut,bte->bue",
        earlier.astype(jnp.bfloat16),
        named.astype(jnp.bfloat16),
        preferred_element_type=jnp.float32,
    )
    slot_rank = jnp.sum(rank[:, None] * onehot, axis=-1).astype(jnp.int32)

    slot_index = route * CAP + slot_rank
    picker = slot_index[..., None] == lax.iota(jnp.int32, slot_total)
    token_pick = jnp.sum(picker.astype(jnp.float32), axis=1).astype(jnp.bfloat16)
    token_weight = jnp.sum(jnp.where(picker, weight[..., None], 0.0), axis=1)
    token_weight = token_weight.astype(jnp.bfloat16)
    arrived = []
    for at, k in enumerate(order):
        rows = lax.dot_general(
            token_pick[at],
            blocks[k],
            (((0,), (0,)), ((), ())),
            preferred_element_type=jnp.float32,
        )
        rows = rows.astype(jnp.bfloat16).reshape(n_sp, slot_rows, width)
        arrived.append(lax.all_to_all(rows, "sp", split_axis=0, concat_axis=0, tiled=True))
    arrived = jnp.stack(arrived).reshape(n_tp, n_sp, local_experts, CAP, width)
    f32 = {"preferred_element_type": jnp.float32}
    gate_pre = jnp.einsum("sklcd,ldf->sklcf", arrived, w_gate, **f32)
    upward = jnp.einsum("sklcd,ldf->sklcf", arrived, w_up, **f32)
    activated = clamped_unit(gate_pre, upward).astype(jnp.bfloat16)
    terms = jnp.einsum("sklcf,lfd->sklcd", activated, w_down, **f32)
    terms = terms.astype(jnp.bfloat16).reshape(n_tp, n_sp, slot_rows, width)
    parts = {}
    for at, k in enumerate(order):
        back = lax.all_to_all(terms[at], "sp", split_axis=0, concat_axis=0, tiled=True)
        part = jnp.dot(token_weight[at], back.reshape(slot_total, width), **f32)
        part = part.astype(jnp.bfloat16)
        parts[k] = rotated(part, "tp", -k) if k else part
    expert_mix = sum(parts[k].astype(jnp.float32) for k in order)
    return (residual.astype(jnp.float32) + rms_scale(expert_mix, post_gain)).astype(jnp.bfloat16)


AHEAD = 16


def cut_body(place, x, routes, weights, *refs):
    (own_routes, own_weights, done), (*chunks, tail) = refs[-3:], refs[:-3]
    n_tp, (top, rows) = len(chunks), routes.shape
    moves = [(routes, own_routes), (weights, own_weights)]
    for k, chunk in enumerate(chunks):
        first = (place[0] + k) % n_tp * rows
        before = pl.multiple_of(jnp.maximum(first - AHEAD, 0), AHEAD)
        first = pl.multiple_of(first, AHEAD)
        moves.append((x.at[pl.ds(first, rows), :], chunk.at[pl.ds(AHEAD, rows), :]))
        moves.append((x.at[pl.ds(before, AHEAD), :], chunk.at[pl.ds(0, AHEAD), :]))
    moves.append((x.at[pl.ds(x.shape[0] - AHEAD, AHEAD), :], tail))
    copies = [pltpu.make_async_copy(a, b, done.at[i]) for i, (a, b) in enumerate(moves)]
    for copy in copies:
        copy.start()
    for copy in copies:
        copy.wait()
    fields = [own_routes[...].astype(jnp.float32), own_weights[...]]
    fields.append(jnp.zeros((8 - 2 * top, rows), jnp.float32))
    fields = jnp.concatenate(fields, axis=0).astype(jnp.bfloat16)
    for chunk in chunks:
        chunk[AHEAD + rows :, :] = jnp.zeros((8, chunk.shape[1]), jnp.bfloat16)
        chunk[AHEAD + rows :, :rows] = fields


def cut(place, x, routes, weights, n_tp):
    rows, channels = routes.shape[1], x.shape[1]
    chunk = jax.ShapeDtypeStruct((AHEAD + rows + 8, channels), x.dtype)
    return pl.pallas_call(
        cut_body,
        in_specs=[IN_SMEM] + [pl.BlockSpec(memory_space=pltpu.HBM)] * 3,
        out_specs=[IN_VMEM] * (n_tp + 1),
        out_shape=[pltpu.VMEM(chunk.shape, x.dtype)] * n_tp
        + [pltpu.VMEM((AHEAD, channels), x.dtype)],
        scratch_shapes=[
            pltpu.VMEM(routes.shape, routes.dtype),
            pltpu.VMEM(weights.shape, weights.dtype),
            pltpu.SemaphoreType.DMA((2 * n_tp + 3,)),
        ],
        compiler_params=pltpu.CompilerParams(vmem_limit_bytes=CUT_LIMIT << 20),
        name="cut",
    )(place, x, routes, weights)


def mix_body(n_tp, place, *refs):
    chunks, halos = refs[:n_tp], refs[n_tp : 2 * n_tp]
    pool_w, scale, out_w, mix_gain, ffn_gain, resid = refs[2 * n_tp : 2 * n_tp + 6]
    residual, normed, raw, pooled, mix = refs[2 * n_tp + 6 :]
    rows, width = resid.shape
    channels = chunks[0].shape[1]
    tp, sp = place[0], place[1]
    for k, chunk in enumerate(chunks):
        source = (tp - k + n_tp) % n_tp
        cols = pl.ds(pl.multiple_of(source * channels, LANES), channels)
        raw[:, cols] = chunk[: AHEAD + rows, :].astype(jnp.float32)

    @pl.when(tp == 0)
    def _():
        for j, halo in enumerate(halos):
            raw[:AHEAD, j * channels : (j + 1) * channels] = halo[...].astype(jnp.float32)

    start = (sp * n_tp + tp) * rows
    position = start + lax.broadcasted_iota(jnp.int32, (rows, GROUP_DIM), 0) + 1
    for g, window in enumerate(pool_windows):
        cols = slice(g * GROUP_DIM, (g + 1) * GROUP_DIM)
        own = raw[:, cols]
        total, reach = own, 1
        while reach < window:
            total = total + pltpu.roll(total, reach, 0)
            reach = 2 * reach
        divisor = jnp.minimum(position, window).astype(jnp.float32)
        mixed = (total[AHEAD:] / divisor - own[AHEAD:]).astype(jnp.bfloat16)
        part = jnp.dot(mixed, pool_w[g], preferred_element_type=jnp.float32)
        pooled[:, cols] = (part * scale[:, cols]).astype(jnp.bfloat16)

    def columns():
        return [slice(j, j + 2 * LANES) for j in range(0, width, 2 * LANES)]

    def inverse_of(square):
        return lax.rsqrt(jnp.sum(square, axis=1, keepdims=True) / width + norm_eps)

    square = jnp.zeros((rows, LANES), jnp.float32)
    for cols in columns():
        part = jnp.dot(pooled[...], out_w[:, cols], preferred_element_type=jnp.float32)
        mix[:, cols] = part
        square = square + part[:, :LANES] * part[:, :LANES] + part[:, LANES:] * part[:, LANES:]
    inverse = inverse_of(square)
    square = jnp.zeros((rows, LANES), jnp.float32)
    for cols in columns():
        part = resid[:, cols].astype(jnp.float32) + mix[:, cols] * inverse * mix_gain[:, cols]
        part = part.astype(jnp.bfloat16)
        residual[:, cols] = part
        part = part.astype(jnp.float32)
        square = square + part[:, :LANES] * part[:, :LANES] + part[:, LANES:] * part[:, LANES:]
    inverse = inverse_of(square)
    for cols in columns():
        part = residual[:, cols].astype(jnp.float32) * inverse * ffn_gain[:, cols]
        normed[:, cols] = part.astype(normed.dtype)


def mix_tokens(place, chunks, halos, pool_w, scale, out_w, mix_gain, ffn_gain, resid):
    rows, width = resid.shape
    total = out_w.shape[0]
    return pl.pallas_call(
        lambda *refs: mix_body(len(chunks), *refs),
        in_specs=[IN_SMEM] + [IN_VMEM] * (2 * len(chunks) + 6),
        out_specs=[IN_VMEM] * 2,
        out_shape=[jax.ShapeDtypeStruct(resid.shape, resid.dtype)] * 2,
        scratch_shapes=[
            pltpu.VMEM((AHEAD + rows, total), jnp.float32),
            pltpu.VMEM((rows, total), jnp.bfloat16),
            pltpu.VMEM((rows, width), jnp.float32),
        ],
        compiler_params=pltpu.CompilerParams(vmem_limit_bytes=12 << 20),
        name="mix",
    )(
        place,
        *chunks,
        *halos,
        pool_w,
        scale,
        out_w,
        mix_gain,
        ffn_gain,
        resid,
    )


def slots_body(n_sp, local, place, *refs):
    chunks, (slot, by_row, weight) = refs[:-3], refs[-3:]
    top, tokens = slot.shape[1], slot.shape[2]
    n_experts = n_sp * local
    expert = lax.broadcasted_iota(jnp.int32, (n_experts, tokens), 0)
    row = lax.broadcasted_iota(jnp.int32, (tokens, tokens), 0)
    lane = lax.broadcasted_iota(jnp.int32, (tokens, tokens), 1)
    before = jnp.where(row < lane, 1.0, 0.0).astype(jnp.bfloat16)
    whole = CAP // 8 * 8
    for at, chunk in enumerate(chunks):
        first = chunk.shape[0] - 8
        fields = chunk[first:, :tokens].astype(jnp.float32)
        hits = [
            jnp.where(expert == fields[k : k + 1].astype(jnp.int32), 1.0, 0.0) for k in range(top)
        ]
        named = sum(hits).astype(jnp.bfloat16)
        rank = jnp.dot(named, before, preferred_element_type=jnp.float32)
        found = []
        for k, hit in enumerate(hits):
            mine = jnp.sum(rank * hit, axis=0, keepdims=True).astype(jnp.int32)
            route = jnp.sum(expert.astype(jnp.float32) * hit, axis=0, keepdims=True)
            owner = jnp.sum(
                (expert // local).astype(jnp.float32) * hit, axis=0, keepdims=True
            ).astype(jnp.int32)
            inside = route.astype(jnp.int32) - owner * local
            owner = offset_to(owner, place[1], n_sp)
            in_tile = inside * whole + mine
            apart = local * whole + (mine - whole) * local + inside
            found.append(owner * local * CAP + jnp.where(mine < whole, in_tile, apart))
            slot[at, k : k + 1, :] = found[-1]
        rows8 = [x.astype(jnp.float32) for x in found] + [fields[top : 2 * top]]
        rows8.append(jnp.zeros((tokens - 2 * top, tokens), jnp.float32))
        turned = jnp.concatenate(rows8, axis=0).T
        by_row[at] = turned[:, :top].astype(jnp.int32)
        weight[at] = turned[:, top : 2 * top]


def slots(place, chunks, n_sp, local, top, tokens):
    n = len(chunks)
    return pl.pallas_call(
        lambda *refs: slots_body(n_sp, local, *refs),
        in_specs=[IN_SMEM] + [IN_VMEM] * n,
        out_specs=[IN_VMEM] * 3,
        out_shape=[
            jax.ShapeDtypeStruct((n, top, tokens), jnp.int32),
            jax.ShapeDtypeStruct((n, tokens, top), jnp.int32),
            jax.ShapeDtypeStruct((n, tokens, top), jnp.float32),
        ],
        compiler_params=pltpu.CompilerParams(vmem_limit_bytes=6 << 20),
        name="slots",
    )(place, *chunks)


def kernel_path(
    resid_in,
    pool_input,
    pool_weight,
    pool_scale,
    out_weight,
    mix_gain,
    ffn_gain,
    w_gate,
    w_up,
    w_down,
    routes,
    route_weight,
    post_gain,
):
    n_sp = lax.axis_size("sp")
    n_tp = lax.axis_size("tp")
    tok_rows = resid_in.shape[0]
    local_experts = w_gate.shape[0]
    slot_rows = local_experts * CAP

    place = jnp.stack([lax.axis_index("tp"), lax.axis_index("sp")]).astype(jnp.int32)
    *chunks, tail = cut(place, pool_input, routes.T, route_weight.T, n_tp)
    halos = []
    for j in range(n_tp):
        pairs = [(s * n_tp + j, (s + 1) * n_tp) for s in range(n_sp - 1)]
        halos.append(lax.ppermute(tail, ("sp", "tp"), pairs))
    chunks = [rotated(x, "tp", k) if k else x for k, x in enumerate(chunks)]
    small = [x.reshape(1, -1) for x in (pool_scale, mix_gain, ffn_gain)]
    scale, mix_gain, ffn_gain, pool_weight, out_weight, resid_in = load(
        *small, pool_weight, out_weight, resid_in, limit=EARLY_LIMIT
    )
    residual, normed = mix_tokens(
        place, chunks, halos, pool_weight, scale, out_weight, mix_gain, ffn_gain, resid_in
    )

    far = n_tp // 2
    order = list(range(far + 1)) + list(range(n_tp - 1, far, -1))
    blocks = {0: normed, n_tp: normed}
    for k in order:
        if k:
            by = 1 if k <= far else -1
            blocks[k] = rotated(blocks[k - by], "tp", by)

    slot, by_row, weight = slots(
        place, [chunks[k] for k in order], n_sp, local_experts, TOP, tok_rows
    )
    weights = load(w_gate, w_up, w_down)
    arrived, backs, parts = [], {}, {}
    for at, k in enumerate(order):
        rows = pick(at, slot, blocks[k], n_sp, slot_rows)
        arrived.append([moved(x, "sp", d) if d else x for d, x in enumerate(rows)])
    for first, stop in groups_of(n_tp):
        group = arrived[first:stop]
        terms = experts([x for xs in group for x in xs], *weights)
        for at in range(first, stop):
            back = terms[(at - first) * n_sp : (at - first + 1) * n_sp]
            backs[at] = [moved(x, "sp", d, True) if d else x for d, x in enumerate(back)]
    for at in return_order(n_tp)[:-1]:
        k = order[at]
        by = -1 if k <= far else 1
        inner = k < far or k > far + 1
        joined = [parts.pop(k - by)] if inner else []
        part = combine(at, by_row, weight, backs[at], joined)
        parts[k] = rotated(part, "tp", by)
    return finish(0, by_row, weight, residual, post_gain, backs[0], list(parts.values()))


def per_device(*args):
    pool_input, w_gate, routes = args[1], args[7], args[10]
    n_sp = lax.axis_size("sp")
    fits = w_gate.shape[0] % 8 == 0 and CAP % 8 and n_sp <= 4 and w_gate.shape[0] * n_sp <= 256
    fits = fits and routes.shape[0] == LANES and pool_input.shape[1] % LANES == 0
    return kernel_path(*args) if fits else plain_path(*args)


def groups_of(n_tp):
    first = min(2, n_tp)
    return [(0, first)] + [(at, at + 1) for at in range(first, n_tp)]


def return_order(n_tp):
    far = n_tp // 2
    return list(range(far, 1, -1)) + list(range(n_tp - 1, far, -1)) + list(range(min(2, n_tp)))[::-1]


def solution(mesh):
    in_specs = (
        P(("grp", "sp", "tp"), None),
        P(("grp", "sp"), "tp"),
        P(),
        P(),
        P(),
        P(),
        P(),
        P("sp", None, "tp"),
        P("sp", None, "tp"),
        P("sp", "tp", None),
        P(("grp", "sp", "tp"), None),
        P(("grp", "sp", "tp"), None),
        P(),
    )
    out_specs = P(("grp", "sp", "tp"), None)

    return jax.shard_map(
        per_device, mesh=mesh, in_specs=in_specs, out_specs=out_specs, check_vma=False
    )
```

```python
import jax
import jax.numpy as jnp
from jax import lax
from jax.experimental import pallas as pl
from jax.experimental.pallas import tpu as pltpu
from jax.sharding import PartitionSpec as P


GROUPS = 4
GROUP_DIM = 256
TOP = 2
CAP = 9


pool_windows = (2, 4, 8, 16)
reach_back = 15
norm_eps = 1e-06
clamp_limit = 7.0
glu_alpha = 1.702


def passed_along(x, axis, by):
    size = lax.axis_size(axis)
    pairs = [(i, i + by) for i in range(size) if 0 <= i + by < size]
    return lax.ppermute(x, axis, pairs)


def rotated(x, axis, by):
    size = lax.axis_size(axis)
    return lax.ppermute(x, axis, [(i, (i + by) % size) for i in range(size)])


def rms_scale(values, gain_vec):
    inverse = lax.rsqrt(jnp.mean(values * values, axis=-1, keepdims=True) + norm_eps)
    return values * inverse * gain_vec


def clamped_unit(gate_pre, upward):
    gate_clip = jnp.minimum(gate_pre, clamp_limit)
    linear = jnp.clip(upward, -clamp_limit, clamp_limit)
    return gate_clip * jax.nn.sigmoid(glu_alpha * gate_clip) * (linear + 1.0)


def mixed_window(pool_input):
    seg_rows, channels = pool_input.shape
    last_rows = pool_input[seg_rows - reach_back :]
    before = passed_along(last_rows, "sp", 1)
    extended = jnp.concatenate([before, pool_input], axis=0).astype(jnp.float32)
    first_chan = lax.axis_index("tp") * channels
    chan_group = (first_chan + lax.iota(jnp.int32, channels)) // GROUP_DIM
    positions = lax.axis_index("sp") * seg_rows + lax.iota(jnp.int32, seg_rows)
    window = jnp.zeros((channels,), jnp.int32)
    for group_level, win_len in enumerate(pool_windows):
        window = jnp.where(chan_group == group_level, win_len, window)
    running = jnp.zeros((seg_rows, channels), jnp.float32)
    window_sum = running
    for offset in range(pool_windows[-1]):
        running = running + extended[reach_back - offset : reach_back - offset + seg_rows]
        if offset + 1 in pool_windows:
            window_sum = jnp.where(window[None, :] == offset + 1, running, window_sum)
    divisor = jnp.minimum(positions[:, None] + 1, window[None, :]).astype(jnp.float32)
    return (window_sum / divisor - extended[reach_back:]).astype(jnp.bfloat16)


def reached(i, d, n):
    return i ^ d if n & (n - 1) == 0 else (i + d) % n


def offset_to(target, i, n):
    return target ^ i if n & (n - 1) == 0 else (target - i) % n


def moved(x, axis, d, back=False):
    size = lax.axis_size(axis)
    pairs = [(i, reached(i, d, size)) for i in range(size)]
    return lax.ppermute(x, axis, [(b, a) for a, b in pairs] if back else pairs)


LANES = 128
IN_VMEM = pl.BlockSpec(memory_space=pltpu.VMEM)
IN_SMEM = pl.BlockSpec(memory_space=pltpu.SMEM)


def load_body(*refs):
    half = len(refs) // 2
    sources, targets, done = refs[:half], refs[half:-1], refs[-1]
    copies = []
    for source, target in zip(sources, targets):
        parts = range(source.shape[0]) if len(source.shape) == 3 else [...]
        for e in parts:
            at = done.at[len(copies)]
            copies.append(pltpu.make_async_copy(source.at[e], target.at[e], at))
    for copy in copies:
        copy.start()
    for copy in copies:
        copy.wait()


LOAD_LIMIT = 28
EARLY_LIMIT = 55
CUT_LIMIT = 60


def load(*weights, limit=LOAD_LIMIT):
    count = sum(w.shape[0] if w.ndim == 3 else 1 for w in weights)
    return pl.pallas_call(
        load_body,
        in_specs=[pl.BlockSpec(memory_space=pltpu.HBM)] * len(weights),
        out_specs=[IN_VMEM] * len(weights),
        out_shape=[pltpu.VMEM(w.shape, w.dtype) for w in weights],
        scratch_shapes=[pltpu.SemaphoreType.DMA((count,))],
        compiler_params=pltpu.CompilerParams(vmem_limit_bytes=limit << 20),
        name="load",
    )(*weights)


def pick_body(at, slot, block, *outs):
    rows = outs[0].shape[0]
    tokens = slot.shape[2]
    ids = lax.broadcasted_iota(jnp.int32, (len(outs) * rows, tokens), 0)
    hit = ids == slot[at, 0:1, :]
    for k in range(1, slot.shape[1]):
        hit = hit | (ids == slot[at, k : k + 1, :])
    chosen = jnp.where(hit, 1.0, 0.0).astype(jnp.bfloat16)
    for j in range(0, block.shape[1], 2 * LANES):
        cols = slice(j, j + 2 * LANES)
        taken = jnp.dot(chosen, block[:, cols], preferred_element_type=jnp.float32)
        for d, out in enumerate(outs):
            out[:, cols] = taken[d * rows : (d + 1) * rows].astype(out.dtype)


def pick(at, slot, block, n_sp, slot_rows):
    shape = jax.ShapeDtypeStruct((slot_rows, block.shape[1]), block.dtype)
    return pl.pallas_call(
        lambda *refs: pick_body(at, *refs),
        in_specs=[IN_VMEM] * 2,
        out_specs=[IN_VMEM] * n_sp,
        out_shape=[shape] * n_sp,
        compiler_params=pltpu.CompilerParams(vmem_limit_bytes=6 << 20),
        name="pick",
    )(slot, block)


def shares_of(at, slot, weight, d, rows):
    ids = lax.broadcasted_iota(jnp.int32, (slot.shape[1], rows), 1) + d * rows
    share = jnp.zeros((slot.shape[1], rows), jnp.float32)
    for k in range(slot.shape[2]):
        share = share + jnp.where(ids == slot[at, :, k : k + 1], weight[at, :, k : k + 1], 0.0)
    return share.astype(jnp.bfloat16)


def combine_body(at, n_back, slot, weight, *refs):
    backs, joined, out = refs[:n_back], refs[n_back:-1], refs[-1]
    rows = backs[0].shape[0]
    share = [shares_of(at, slot, weight, d, rows) for d in range(len(backs))]
    for j in range(0, out.shape[1], 2 * LANES):
        cols = slice(j, j + 2 * LANES)
        total = None
        for d, back in enumerate(backs):
            term = jnp.dot(share[d], back[:, cols], preferred_element_type=jnp.float32)
            total = term if total is None else total + term
        for other in joined:
            total = total + other[:, cols].astype(jnp.float32)
        out[:, cols] = total.astype(out.dtype)


def combine(at, slot, weight, backs, joined):
    shape = jax.ShapeDtypeStruct((slot.shape[1], backs[0].shape[1]), jnp.bfloat16)
    return pl.pallas_call(
        lambda *refs: combine_body(at, len(backs), *refs),
        in_specs=[IN_VMEM] * (2 + len(backs) + len(joined)),
        out_specs=IN_VMEM,
        out_shape=shape,
        compiler_params=pltpu.CompilerParams(vmem_limit_bytes=6 << 20),
        name="combine",
    )(slot, weight, *backs, *joined)


def finish_body(at, n_back, slot, weight, resid, gain, *refs):
    backs, apart = refs[:n_back], refs[n_back : 2 * n_back]
    parts, (out, mix) = refs[2 * n_back : -2], refs[-2:]
    rows, width = backs[0].shape[0], out.shape[1]
    apart_from = backs[0].shape[1]
    share = [shares_of(at, slot, weight, d, rows) for d in range(n_back)]
    square = jnp.zeros((out.shape[0], LANES), jnp.float32)
    for j in range(0, width, 2 * LANES):
        near = j < apart_from
        first = j if near else j - apart_from
        cols = slice(first, first + 2 * LANES)
        total = jnp.zeros((out.shape[0], 2 * LANES), jnp.float32)
        for part in parts if near else ():
            total = total + part[:, cols].astype(jnp.float32)
        for d, back in enumerate(backs if near else apart):
            total = total + jnp.dot(share[d], back[:, cols], preferred_element_type=jnp.float32)
        mix[:, j : j + 2 * LANES] = total
        square = square + total[:, :LANES] * total[:, :LANES]
        square = square + total[:, LANES:] * total[:, LANES:]
    mean = jnp.sum(square, axis=1, keepdims=True) / width
    inverse = lax.rsqrt(mean + norm_eps)
    for j in range(0, width, 2 * LANES):
        cols = slice(j, j + 2 * LANES)
        scaled = mix[:, cols] * inverse * gain[:, cols]
        out[:, cols] = (resid[:, cols].astype(jnp.float32) + scaled).astype(out.dtype)


def finish(at, slot, weight, resid, gain, backs, apart, parts):
    return pl.pallas_call(
        lambda *refs: finish_body(at, len(backs), *refs),
        in_specs=[IN_VMEM] * (4 + 2 * len(backs) + len(parts)),
        out_specs=IN_VMEM,
        out_shape=jax.ShapeDtypeStruct(resid.shape, resid.dtype),
        scratch_shapes=[pltpu.VMEM(resid.shape, jnp.float32)],
        compiler_params=pltpu.CompilerParams(vmem_limit_bytes=6 << 20),
        name="finish",
    )(slot, weight, resid, gain.reshape(1, -1), *backs, *apart, *parts)


def experts_body(n_src, n_sp, *refs):
    xs, (wg, wu, wd) = refs[:n_src], refs[n_src : n_src + 3]
    outs, sums, (into, outof) = refs[n_src + 3 : 2 * n_src + 3], refs[2 * n_src + 3 : -2], refs[-2:]
    count, (rows, width) = wg.shape[0], xs[0].shape
    apart_from = outs[0].shape[1]
    tiles, left = divmod(rows // count, 8)
    whole = count * tiles * 8
    for s, x in enumerate(xs):
        for j in range(width // LANES):
            cols = slice(j * LANES, (j + 1) * LANES)
            into[j, s * left * count : (s + 1) * left * count, :] = x[whole:, cols].astype(
                jnp.float32
            )

    def one(e, carry):
        starts = [pl.multiple_of((e * tiles + i) * 8, 8) for i in range(tiles)]
        apart = pl.ds(e, n_src * left, stride=count)
        taken = [x[pl.ds(at, 8), :].astype(jnp.float32) for x in xs for at in starts]
        taken.append(jnp.concatenate([into[j, apart, :] for j in range(width // LANES)], axis=1))
        taken = jnp.concatenate(taken, axis=0).astype(jnp.bfloat16)
        gate_pre = jnp.dot(taken, wg[e], preferred_element_type=jnp.float32)
        upward = jnp.dot(taken, wu[e], preferred_element_type=jnp.float32)
        activated = clamped_unit(gate_pre, upward).astype(jnp.bfloat16)
        result = jnp.dot(activated, wd[e], preferred_element_type=jnp.float32)
        row = 0
        for s, out in enumerate(outs):
            block, d = divmod(s, n_sp)
            for at in starts:
                part = result[row : row + 8].astype(out.dtype)
                out[pl.ds(at, 8), :] = part[:, :apart_from]
                sums[block][pl.ds(pl.multiple_of(d * rows + at, 8), 8), :] = part[:, apart_from:]
                row += 8
        for j in range(width // LANES):
            outof[j, apart, :] = result[row:, j * LANES : (j + 1) * LANES]
        return carry

    lax.fori_loop(0, count, one, 0, unroll=EXPERT_UNROLL)
    for s, out in enumerate(outs):
        block, d = divmod(s, n_sp)
        for j in range(width // LANES):
            part = outof[j, s * left * count : (s + 1) * left * count, :].astype(out.dtype)
            first = j * LANES
            if first < apart_from:
                out[whole:, first : first + LANES] = part
            else:
                first -= apart_from
                sums[block][d * rows + whole : (d + 1) * rows, first : first + LANES] = part


EXPERT_UNROLL = 2


def experts(xs, w_gate, w_up, w_down, n_sp, apart_from):
    count, width, hidden = w_gate.shape
    rows, n_src = xs[0].shape[0], len(xs)
    blocks = n_src // n_sp
    left = rows // count % 8
    scratch = pltpu.VMEM((width // LANES, n_src * left * count, LANES), jnp.float32)
    out = jax.ShapeDtypeStruct((rows, apart_from), jnp.bfloat16)
    summed = jax.ShapeDtypeStruct((n_sp * rows, width - apart_from), jnp.bfloat16)
    flops = 6 * n_src * rows * width * hidden
    moved_bytes = 3 * count * width * hidden * 2 + 4 * n_src * rows * width
    cost = pl.CostEstimate(flops=flops, bytes_accessed=moved_bytes, transcendentals=0)
    outs = pl.pallas_call(
        lambda *refs: experts_body(n_src, n_sp, *refs),
        in_specs=[IN_VMEM] * (n_src + 3),
        out_specs=[IN_VMEM] * (n_src + blocks),
        out_shape=[out] * n_src + [summed] * blocks,
        scratch_shapes=[scratch, scratch],
        cost_estimate=cost,
        compiler_params=pltpu.CompilerParams(vmem_limit_bytes=6 << 20),
        name="experts",
    )(*xs, w_gate, w_up, w_down)
    return outs[:n_src], outs[n_src:]


def join_body(n_in, *refs):
    total = sum(x[...].astype(jnp.float32) for x in refs[:n_in])
    outs = refs[n_in:]
    rows = outs[0].shape[0]
    for i, out in enumerate(outs):
        out[...] = total[i * rows : (i + 1) * rows].astype(out.dtype)


def join(arrays, pieces=1):
    rows, width = arrays[0].shape
    out = jax.ShapeDtypeStruct((rows // pieces, width), arrays[0].dtype)
    return pl.pallas_call(
        lambda *refs: join_body(len(arrays), *refs),
        in_specs=[IN_VMEM] * len(arrays),
        out_specs=[IN_VMEM] * pieces,
        out_shape=[out] * pieces,
        compiler_params=pltpu.CompilerParams(vmem_limit_bytes=6 << 20),
        name="join",
    )(*arrays)


def plain_path(
    resid_in,
    pool_input,
    pool_weight,
    pool_scale,
    out_weight,
    mix_gain,
    ffn_gain,
    w_gate,
    w_up,
    w_down,
    routes,
    route_weight,
    post_gain,
):
    n_sp = lax.axis_size("sp")
    n_tp = lax.axis_size("tp")
    tok_rows, width = resid_in.shape
    channels = pool_input.shape[1]
    local_experts = w_gate.shape[0]
    n_experts = local_experts * n_sp
    assert n_experts <= 256
    slot_rows = local_experts * CAP
    slot_total = n_sp * slot_rows

    fields = jnp.concatenate([routes.astype(jnp.bfloat16).T, route_weight.astype(jnp.bfloat16).T])
    n_fields = fields.size
    field_rows = -(-n_fields // (8 * channels)) * 8
    fields = jnp.pad(fields.reshape(-1), (0, field_rows * channels - n_fields))
    fields = jnp.broadcast_to(fields.reshape(1, field_rows, channels), (n_tp, field_rows, channels))
    mixed_rows = mixed_window(pool_input).reshape(n_tp, tok_rows, channels)
    sent = jnp.concatenate([mixed_rows, fields], axis=1)
    got = lax.all_to_all(sent, "tp", split_axis=0, concat_axis=0, tiled=True)
    token_mixed = got[:, :tok_rows].transpose(1, 0, 2).reshape(tok_rows, n_tp * channels)
    fields = got[:, tok_rows:].reshape(n_tp, -1)[:, :n_fields].reshape(n_tp, 2 * TOP, tok_rows)

    pooled = jnp.einsum(
        "tgc,gcd->tgd",
        token_mixed.reshape(tok_rows, GROUPS, GROUP_DIM),
        pool_weight,
        preferred_element_type=jnp.float32,
    )
    pooled = (
        (pooled * pool_scale.reshape(GROUPS, GROUP_DIM)).astype(jnp.bfloat16).reshape(tok_rows, -1)
    )
    mix_out = jnp.dot(pooled, out_weight, preferred_element_type=jnp.float32)
    residual = (resid_in.astype(jnp.float32) + rms_scale(mix_out, mix_gain)).astype(jnp.bfloat16)
    normed = rms_scale(residual.astype(jnp.float32), ffn_gain).astype(jnp.bfloat16)

    far = n_tp // 2
    order = list(range(far + 1)) + list(range(n_tp - 1, far, -1))
    blocks = {0: normed, n_tp: normed}
    for k in order:
        if k:
            by = 1 if k <= far else -1
            blocks[k] = rotated(blocks[k - by], "tp", by)

    here = lax.axis_index("tp")
    fields = jnp.take(fields, (here - jnp.array(order)) % n_tp, axis=0)
    route = fields[:, :TOP].astype(jnp.int32)
    weight = fields[:, TOP:].astype(jnp.float32)
    onehot = route[..., None] == lax.iota(jnp.int32, n_experts)
    named = jnp.sum(onehot.astype(jnp.float32), axis=1)
    earlier = lax.iota(jnp.int32, tok_rows)[:, None] > lax.iota(jnp.int32, tok_rows)[None, :]
    rank = jnp.einsum(
        "ut,bte->bue",
        earlier.astype(jnp.bfloat16),
        named.astype(jnp.bfloat16),
        preferred_element_type=jnp.float32,
    )
    slot_rank = jnp.sum(rank[:, None] * onehot, axis=-1).astype(jnp.int32)

    slot_index = route * CAP + slot_rank
    picker = slot_index[..., None] == lax.iota(jnp.int32, slot_total)
    token_pick = jnp.sum(picker.astype(jnp.float32), axis=1).astype(jnp.bfloat16)
    token_weight = jnp.sum(jnp.where(picker, weight[..., None], 0.0), axis=1)
    token_weight = token_weight.astype(jnp.bfloat16)
    arrived = []
    for at, k in enumerate(order):
        rows = lax.dot_general(
            token_pick[at],
            blocks[k],
            (((0,), (0,)), ((), ())),
            preferred_element_type=jnp.float32,
        )
        rows = rows.astype(jnp.bfloat16).reshape(n_sp, slot_rows, width)
        arrived.append(lax.all_to_all(rows, "sp", split_axis=0, concat_axis=0, tiled=True))
    arrived = jnp.stack(arrived).reshape(n_tp, n_sp, local_experts, CAP, width)
    f32 = {"preferred_element_type": jnp.float32}
    gate_pre = jnp.einsum("sklcd,ldf->sklcf", arrived, w_gate, **f32)
    upward = jnp.einsum("sklcd,ldf->sklcf", arrived, w_up, **f32)
    activated = clamped_unit(gate_pre, upward).astype(jnp.bfloat16)
    terms = jnp.einsum("sklcf,lfd->sklcd", activated, w_down, **f32)
    terms = terms.astype(jnp.bfloat16).reshape(n_tp, n_sp, slot_rows, width)
    parts = {}
    for at, k in enumerate(order):
        back = lax.all_to_all(terms[at], "sp", split_axis=0, concat_axis=0, tiled=True)
        part = jnp.dot(token_weight[at], back.reshape(slot_total, width), **f32)
        part = part.astype(jnp.bfloat16)
        parts[k] = rotated(part, "tp", -k) if k else part
    expert_mix = sum(parts[k].astype(jnp.float32) for k in order)
    return (residual.astype(jnp.float32) + rms_scale(expert_mix, post_gain)).astype(jnp.bfloat16)


AHEAD = 16


def cut_body(place, x, routes, weights, *refs):
    (own_routes, own_weights, done), (*chunks, tail) = refs[-3:], refs[:-3]
    n_tp, (top, rows) = len(chunks), routes.shape
    moves = [(routes, own_routes), (weights, own_weights)]
    for k, chunk in enumerate(chunks):
        first = (place[0] + k) % n_tp * rows
        before = pl.multiple_of(jnp.maximum(first - AHEAD, 0), AHEAD)
        first = pl.multiple_of(first, AHEAD)
        moves.append((x.at[pl.ds(first, rows), :], chunk.at[pl.ds(AHEAD, rows), :]))
        moves.append((x.at[pl.ds(before, AHEAD), :], chunk.at[pl.ds(0, AHEAD), :]))
    moves.append((x.at[pl.ds(x.shape[0] - AHEAD, AHEAD), :], tail))
    copies = [pltpu.make_async_copy(a, b, done.at[i]) for i, (a, b) in enumerate(moves)]
    for copy in copies:
        copy.start()
    for copy in copies:
        copy.wait()
    fields = [own_routes[...].astype(jnp.float32), own_weights[...]]
    fields.append(jnp.zeros((8 - 2 * top, rows), jnp.float32))
    fields = jnp.concatenate(fields, axis=0).astype(jnp.bfloat16)
    for chunk in chunks:
        chunk[AHEAD + rows :, :] = jnp.zeros((8, chunk.shape[1]), jnp.bfloat16)
        chunk[AHEAD + rows :, :rows] = fields


def cut(place, x, routes, weights, n_tp):
    rows, channels = routes.shape[1], x.shape[1]
    chunk = jax.ShapeDtypeStruct((AHEAD + rows + 8, channels), x.dtype)
    return pl.pallas_call(
        cut_body,
        in_specs=[IN_SMEM] + [pl.BlockSpec(memory_space=pltpu.HBM)] * 3,
        out_specs=[IN_VMEM] * (n_tp + 1),
        out_shape=[pltpu.VMEM(chunk.shape, x.dtype)] * n_tp
        + [pltpu.VMEM((AHEAD, channels), x.dtype)],
        scratch_shapes=[
            pltpu.VMEM(routes.shape, routes.dtype),
            pltpu.VMEM(weights.shape, weights.dtype),
            pltpu.SemaphoreType.DMA((2 * n_tp + 3,)),
        ],
        compiler_params=pltpu.CompilerParams(vmem_limit_bytes=CUT_LIMIT << 20),
        name="cut",
    )(place, x, routes, weights)


def mix_body(n_tp, place, *refs):
    chunks, halos = refs[:n_tp], refs[n_tp : 2 * n_tp]
    pool_w, scale, out_w, mix_gain, ffn_gain, resid = refs[2 * n_tp : 2 * n_tp + 6]
    residual, normed, raw, pooled, mix = refs[2 * n_tp + 6 :]
    rows, width = resid.shape
    channels = chunks[0].shape[1]
    tp, sp = place[0], place[1]
    for k, chunk in enumerate(chunks):
        source = (tp - k + n_tp) % n_tp
        cols = pl.ds(pl.multiple_of(source * channels, LANES), channels)
        raw[:, cols] = chunk[: AHEAD + rows, :].astype(jnp.float32)

    @pl.when(tp == 0)
    def _():
        for j, halo in enumerate(halos):
            raw[:AHEAD, j * channels : (j + 1) * channels] = halo[...].astype(jnp.float32)

    start = (sp * n_tp + tp) * rows
    position = start + lax.broadcasted_iota(jnp.int32, (rows, GROUP_DIM), 0) + 1
    for g, window in enumerate(pool_windows):
        cols = slice(g * GROUP_DIM, (g + 1) * GROUP_DIM)
        own = raw[:, cols]
        total, reach = own, 1
        while reach < window:
            total = total + pltpu.roll(total, reach, 0)
            reach = 2 * reach
        divisor = jnp.minimum(position, window).astype(jnp.float32)
        mixed = (total[AHEAD:] / divisor - own[AHEAD:]).astype(jnp.bfloat16)
        part = jnp.dot(mixed, pool_w[g], preferred_element_type=jnp.float32)
        pooled[:, cols] = (part * scale[:, cols]).astype(jnp.bfloat16)

    def columns():
        return [slice(j, j + 2 * LANES) for j in range(0, width, 2 * LANES)]

    def inverse_of(square):
        return lax.rsqrt(jnp.sum(square, axis=1, keepdims=True) / width + norm_eps)

    square = jnp.zeros((rows, LANES), jnp.float32)
    for cols in columns():
        part = jnp.dot(pooled[...], out_w[:, cols], preferred_element_type=jnp.float32)
        mix[:, cols] = part
        square = square + part[:, :LANES] * part[:, :LANES] + part[:, LANES:] * part[:, LANES:]
    inverse = inverse_of(square)
    square = jnp.zeros((rows, LANES), jnp.float32)
    for cols in columns():
        part = resid[:, cols].astype(jnp.float32) + mix[:, cols] * inverse * mix_gain[:, cols]
        part = part.astype(jnp.bfloat16)
        residual[:, cols] = part
        part = part.astype(jnp.float32)
        square = square + part[:, :LANES] * part[:, :LANES] + part[:, LANES:] * part[:, LANES:]
    inverse = inverse_of(square)
    for cols in columns():
        part = residual[:, cols].astype(jnp.float32) * inverse * ffn_gain[:, cols]
        normed[:, cols] = part.astype(normed.dtype)


def mix_tokens(place, chunks, halos, pool_w, scale, out_w, mix_gain, ffn_gain, resid):
    rows, width = resid.shape
    total = out_w.shape[0]
    return pl.pallas_call(
        lambda *refs: mix_body(len(chunks), *refs),
        in_specs=[IN_SMEM] + [IN_VMEM] * (2 * len(chunks) + 6),
        out_specs=[IN_VMEM] * 2,
        out_shape=[jax.ShapeDtypeStruct(resid.shape, resid.dtype)] * 2,
        scratch_shapes=[
            pltpu.VMEM((AHEAD + rows, total), jnp.float32),
            pltpu.VMEM((rows, total), jnp.bfloat16),
            pltpu.VMEM((rows, width), jnp.float32),
        ],
        compiler_params=pltpu.CompilerParams(vmem_limit_bytes=12 << 20),
        name="mix",
    )(
        place,
        *chunks,
        *halos,
        pool_w,
        scale,
        out_w,
        mix_gain,
        ffn_gain,
        resid,
    )


def slots_body(n_sp, local, place, *refs):
    chunks, (slot, by_row, weight) = refs[:-3], refs[-3:]
    top, tokens = slot.shape[1], slot.shape[2]
    n_experts = n_sp * local
    expert = lax.broadcasted_iota(jnp.int32, (n_experts, tokens), 0)
    row = lax.broadcasted_iota(jnp.int32, (tokens, tokens), 0)
    lane = lax.broadcasted_iota(jnp.int32, (tokens, tokens), 1)
    before = jnp.where(row < lane, 1.0, 0.0).astype(jnp.bfloat16)
    whole = CAP // 8 * 8
    for at, chunk in enumerate(chunks):
        first = chunk.shape[0] - 8
        fields = chunk[first:, :tokens].astype(jnp.float32)
        hits = [
            jnp.where(expert == fields[k : k + 1].astype(jnp.int32), 1.0, 0.0) for k in range(top)
        ]
        named = sum(hits).astype(jnp.bfloat16)
        rank = jnp.dot(named, before, preferred_element_type=jnp.float32)
        found = []
        for k, hit in enumerate(hits):
            mine = jnp.sum(rank * hit, axis=0, keepdims=True).astype(jnp.int32)
            route = jnp.sum(expert.astype(jnp.float32) * hit, axis=0, keepdims=True)
            owner = jnp.sum(
                (expert // local).astype(jnp.float32) * hit, axis=0, keepdims=True
            ).astype(jnp.int32)
            inside = route.astype(jnp.int32) - owner * local
            owner = offset_to(owner, place[1], n_sp)
            in_tile = inside * whole + mine
            apart = local * whole + (mine - whole) * local + inside
            found.append(owner * local * CAP + jnp.where(mine < whole, in_tile, apart))
            slot[at, k : k + 1, :] = found[-1]
        rows8 = [x.astype(jnp.float32) for x in found] + [fields[top : 2 * top]]
        rows8.append(jnp.zeros((tokens - 2 * top, tokens), jnp.float32))
        turned = jnp.concatenate(rows8, axis=0).T
        by_row[at] = turned[:, :top].astype(jnp.int32)
        weight[at] = turned[:, top : 2 * top]


def slots(place, chunks, n_sp, local, top, tokens):
    n = len(chunks)
    return pl.pallas_call(
        lambda *refs: slots_body(n_sp, local, *refs),
        in_specs=[IN_SMEM] + [IN_VMEM] * n,
        out_specs=[IN_VMEM] * 3,
        out_shape=[
            jax.ShapeDtypeStruct((n, top, tokens), jnp.int32),
            jax.ShapeDtypeStruct((n, tokens, top), jnp.int32),
            jax.ShapeDtypeStruct((n, tokens, top), jnp.float32),
        ],
        compiler_params=pltpu.CompilerParams(vmem_limit_bytes=6 << 20),
        name="slots",
    )(place, *chunks)


def kernel_path(
    resid_in,
    pool_input,
    pool_weight,
    pool_scale,
    out_weight,
    mix_gain,
    ffn_gain,
    w_gate,
    w_up,
    w_down,
    routes,
    route_weight,
    post_gain,
):
    n_sp = lax.axis_size("sp")
    n_tp = lax.axis_size("tp")
    tok_rows = resid_in.shape[0]
    local_experts = w_gate.shape[0]
    slot_rows = local_experts * CAP

    place = jnp.stack([lax.axis_index("tp"), lax.axis_index("sp")]).astype(jnp.int32)
    *chunks, tail = cut(place, pool_input, routes.T, route_weight.T, n_tp)
    halos = []
    for j in range(n_tp):
        pairs = [(s * n_tp + j, (s + 1) * n_tp) for s in range(n_sp - 1)]
        halos.append(lax.ppermute(tail, ("sp", "tp"), pairs))
    chunks = [rotated(x, "tp", k) if k else x for k, x in enumerate(chunks)]
    small = [x.reshape(1, -1) for x in (pool_scale, mix_gain, ffn_gain)]
    scale, mix_gain, ffn_gain, pool_weight, out_weight, resid_in = load(
        *small, pool_weight, out_weight, resid_in, limit=EARLY_LIMIT
    )
    residual, normed = mix_tokens(
        place, chunks, halos, pool_weight, scale, out_weight, mix_gain, ffn_gain, resid_in
    )

    far = n_tp // 2
    order = list(range(far + 1)) + list(range(n_tp - 1, far, -1))
    blocks = {0: normed, n_tp: normed}
    for k in order:
        if k:
            by = 1 if k <= far else -1
            blocks[k] = rotated(blocks[k - by], "tp", by)

    slot, by_row, weight = slots(
        place, [chunks[k] for k in order], n_sp, local_experts, TOP, tok_rows
    )
    weights = load(w_gate, w_up, w_down)
    arrived, backs, parts = [], {}, {}
    for at, k in enumerate(order):
        rows = pick(at, slot, blocks[k], n_sp, slot_rows)
        arrived.append([moved(x, "sp", d) if d else x for d, x in enumerate(rows)])
    apart_from = apart_column(resid_in.shape[1])
    sums = []
    for first, stop in groups_of(n_tp):
        group = arrived[first:stop]
        xs = [x for xs in group for x in xs]
        terms, summed = experts(xs, *weights, n_sp, apart_from)
        sums += summed
        for at in range(first, stop):
            back = terms[(at - first) * n_sp : (at - first + 1) * n_sp]
            backs[at] = [moved(x, "sp", d, True) if d else x for d, x in enumerate(back)]
    passed = {}
    for at in return_order(n_tp)[:-1]:
        k = order[at]
        by = -1 if k <= far else 1
        inner = k < far or k > far + 1
        part = join([sums[at], passed.pop(k - by)])[0] if inner else sums[at]
        passed[k] = rotated(part, "tp", by)
    apart = join([sums[0], *passed.values()], n_sp)
    apart = [moved(x, "sp", d, True) if d else x for d, x in enumerate(apart)]
    for at in return_order(n_tp)[:-1]:
        k = order[at]
        by = -1 if k <= far else 1
        inner = k < far or k > far + 1
        joined = [parts.pop(k - by)] if inner else []
        part = combine(at, by_row, weight, backs[at], joined)
        parts[k] = rotated(part, "tp", by)
    return finish(
        0, by_row, weight, residual, post_gain, backs[0], apart, list(parts.values())
    )


def per_device(*args):
    pool_input, w_gate, routes = args[1], args[7], args[10]
    n_sp = lax.axis_size("sp")
    fits = w_gate.shape[0] % 8 == 0 and CAP % 8 and n_sp <= 4 and w_gate.shape[0] * n_sp <= 256
    fits = fits and routes.shape[0] == LANES and pool_input.shape[1] % LANES == 0
    return kernel_path(*args) if fits else plain_path(*args)


def groups_of(n_tp):
    first = min(2, n_tp)
    return [(0, first)] + [(at, at + 1) for at in range(first, n_tp)]


def apart_column(width):
    step = 2 * LANES
    return width - width // (APART * step) * step


APART = 4


def return_order(n_tp):
    far = n_tp // 2
    return list(range(far, 1, -1)) + list(range(n_tp - 1, far, -1)) + list(range(min(2, n_tp)))[::-1]


def solution(mesh):
    in_specs = (
        P(("grp", "sp", "tp"), None),
        P(("grp", "sp"), "tp"),
        P(),
        P(),
        P(),
        P(),
        P(),
        P("sp", None, "tp"),
        P("sp", None, "tp"),
        P("sp", "tp", None),
        P(("grp", "sp", "tp"), None),
        P(("grp", "sp", "tp"), None),
        P(),
    )
    out_specs = P(("grp", "sp", "tp"), None)

    return jax.shard_map(
        per_device, mesh=mesh, in_specs=in_specs, out_specs=out_specs, check_vma=False
    )
```

```python
import jax
import jax.numpy as jnp
from jax import lax
from jax.experimental import pallas as pl
from jax.experimental.pallas import tpu as pltpu
from jax.sharding import PartitionSpec as P


GROUPS = 4
GROUP_DIM = 256
TOP = 2
CAP = 9


pool_windows = (2, 4, 8, 16)
reach_back = 15
norm_eps = 1e-06
clamp_limit = 7.0
glu_alpha = 1.702


def passed_along(x, axis, by):
    size = lax.axis_size(axis)
    pairs = [(i, i + by) for i in range(size) if 0 <= i + by < size]
    return lax.ppermute(x, axis, pairs)


def rotated(x, axis, by):
    size = lax.axis_size(axis)
    return lax.ppermute(x, axis, [(i, (i + by) % size) for i in range(size)])


def rms_scale(values, gain_vec):
    inverse = lax.rsqrt(jnp.mean(values * values, axis=-1, keepdims=True) + norm_eps)
    return values * inverse * gain_vec


def clamped_unit(gate_pre, upward):
    gate_clip = jnp.minimum(gate_pre, clamp_limit)
    linear = jnp.clip(upward, -clamp_limit, clamp_limit)
    return gate_clip * jax.nn.sigmoid(glu_alpha * gate_clip) * (linear + 1.0)


def mixed_window(pool_input):
    seg_rows, channels = pool_input.shape
    last_rows = pool_input[seg_rows - reach_back :]
    before = passed_along(last_rows, "sp", 1)
    extended = jnp.concatenate([before, pool_input], axis=0).astype(jnp.float32)
    first_chan = lax.axis_index("tp") * channels
    chan_group = (first_chan + lax.iota(jnp.int32, channels)) // GROUP_DIM
    positions = lax.axis_index("sp") * seg_rows + lax.iota(jnp.int32, seg_rows)
    window = jnp.zeros((channels,), jnp.int32)
    for group_level, win_len in enumerate(pool_windows):
        window = jnp.where(chan_group == group_level, win_len, window)
    running = jnp.zeros((seg_rows, channels), jnp.float32)
    window_sum = running
    for offset in range(pool_windows[-1]):
        running = running + extended[reach_back - offset : reach_back - offset + seg_rows]
        if offset + 1 in pool_windows:
            window_sum = jnp.where(window[None, :] == offset + 1, running, window_sum)
    divisor = jnp.minimum(positions[:, None] + 1, window[None, :]).astype(jnp.float32)
    return (window_sum / divisor - extended[reach_back:]).astype(jnp.bfloat16)


def reached(i, d, n):
    return i ^ d if n & (n - 1) == 0 else (i + d) % n


def offset_to(target, i, n):
    return target ^ i if n & (n - 1) == 0 else (target - i) % n


def moved(x, axis, d, back=False):
    size = lax.axis_size(axis)
    pairs = [(i, reached(i, d, size)) for i in range(size)]
    return lax.ppermute(x, axis, [(b, a) for a, b in pairs] if back else pairs)


LANES = 128
IN_VMEM = pl.BlockSpec(memory_space=pltpu.VMEM)
IN_SMEM = pl.BlockSpec(memory_space=pltpu.SMEM)


def load_body(*refs):
    half = len(refs) // 2
    sources, targets, done = refs[:half], refs[half:-1], refs[-1]
    copies = []
    for source, target in zip(sources, targets):
        parts = range(source.shape[0]) if len(source.shape) == 3 else [...]
        for e in parts:
            at = done.at[len(copies)]
            copies.append(pltpu.make_async_copy(source.at[e], target.at[e], at))
    for copy in copies:
        copy.start()
    for copy in copies:
        copy.wait()


LOAD_LIMIT = 28
EARLY_LIMIT = 55
CUT_LIMIT = 60


def load(*weights, limit=LOAD_LIMIT):
    count = sum(w.shape[0] if w.ndim == 3 else 1 for w in weights)
    return pl.pallas_call(
        load_body,
        in_specs=[pl.BlockSpec(memory_space=pltpu.HBM)] * len(weights),
        out_specs=[IN_VMEM] * len(weights),
        out_shape=[pltpu.VMEM(w.shape, w.dtype) for w in weights],
        scratch_shapes=[pltpu.SemaphoreType.DMA((count,))],
        compiler_params=pltpu.CompilerParams(vmem_limit_bytes=limit << 20),
        name="load",
    )(*weights)


def pick_body(at, slot, block, *outs):
    rows = outs[0].shape[0]
    tokens = slot.shape[2]
    ids = lax.broadcasted_iota(jnp.int32, (len(outs) * rows, tokens), 0)
    hit = ids == slot[at, 0:1, :]
    for k in range(1, slot.shape[1]):
        hit = hit | (ids == slot[at, k : k + 1, :])
    chosen = jnp.where(hit, 1.0, 0.0).astype(jnp.bfloat16)
    for j in range(0, block.shape[1], 2 * LANES):
        cols = slice(j, j + 2 * LANES)
        taken = jnp.dot(chosen, block[:, cols], preferred_element_type=jnp.float32)
        for d, out in enumerate(outs):
            out[:, cols] = taken[d * rows : (d + 1) * rows].astype(out.dtype)


def pick(at, slot, block, n_sp, slot_rows):
    shape = jax.ShapeDtypeStruct((slot_rows, block.shape[1]), block.dtype)
    return pl.pallas_call(
        lambda *refs: pick_body(at, *refs),
        in_specs=[IN_VMEM] * 2,
        out_specs=[IN_VMEM] * n_sp,
        out_shape=[shape] * n_sp,
        compiler_params=pltpu.CompilerParams(vmem_limit_bytes=6 << 20),
        name="pick",
    )(slot, block)


def shares_of(at, slot, weight, d, rows):
    ids = lax.broadcasted_iota(jnp.int32, (slot.shape[1], rows), 1) + d * rows
    share = jnp.zeros((slot.shape[1], rows), jnp.float32)
    for k in range(slot.shape[2]):
        share = share + jnp.where(ids == slot[at, :, k : k + 1], weight[at, :, k : k + 1], 0.0)
    return share.astype(jnp.bfloat16)


def combine_body(at, n_back, slot, weight, *refs):
    backs, joined, out = refs[:n_back], refs[n_back:-1], refs[-1]
    rows = backs[0].shape[0]
    share = [shares_of(at, slot, weight, d, rows) for d in range(len(backs))]
    for j in range(0, out.shape[1], 2 * LANES):
        cols = slice(j, j + 2 * LANES)
        total = None
        for d, back in enumerate(backs):
            term = jnp.dot(share[d], back[:, cols], preferred_element_type=jnp.float32)
            total = term if total is None else total + term
        for other in joined:
            total = total + other[:, cols].astype(jnp.float32)
        out[:, cols] = total.astype(out.dtype)


def combine(at, slot, weight, backs, joined):
    shape = jax.ShapeDtypeStruct((slot.shape[1], backs[0].shape[1]), jnp.bfloat16)
    return pl.pallas_call(
        lambda *refs: combine_body(at, len(backs), *refs),
        in_specs=[IN_VMEM] * (2 + len(backs) + len(joined)),
        out_specs=IN_VMEM,
        out_shape=shape,
        compiler_params=pltpu.CompilerParams(vmem_limit_bytes=6 << 20),
        name="combine",
    )(slot, weight, *backs, *joined)


def finish_body(at, n_back, slot, weight, resid, gain, *refs):
    backs, apart = refs[:n_back], refs[n_back : 2 * n_back]
    parts, (out, mix) = refs[2 * n_back : -2], refs[-2:]
    rows, width = backs[0].shape[0], out.shape[1]
    apart_from = backs[0].shape[1]
    share = [shares_of(at, slot, weight, d, rows) for d in range(n_back)]
    square = jnp.zeros((out.shape[0], LANES), jnp.float32)
    for j in range(0, width, 2 * LANES):
        near = j < apart_from
        first = j if near else j - apart_from
        cols = slice(first, first + 2 * LANES)
        total = jnp.zeros((out.shape[0], 2 * LANES), jnp.float32)
        for part in parts if near else ():
            total = total + part[:, cols].astype(jnp.float32)
        for d, back in enumerate(backs if near else apart):
            total = total + jnp.dot(share[d], back[:, cols], preferred_element_type=jnp.float32)
        mix[:, j : j + 2 * LANES] = total
        square = square + total[:, :LANES] * total[:, :LANES]
        square = square + total[:, LANES:] * total[:, LANES:]
    mean = jnp.sum(square, axis=1, keepdims=True) / width
    inverse = lax.rsqrt(mean + norm_eps)
    for j in range(0, width, 2 * LANES):
        cols = slice(j, j + 2 * LANES)
        scaled = mix[:, cols] * inverse * gain[:, cols]
        out[:, cols] = (resid[:, cols].astype(jnp.float32) + scaled).astype(out.dtype)


def finish(at, slot, weight, resid, gain, backs, apart, parts):
    return pl.pallas_call(
        lambda *refs: finish_body(at, len(backs), *refs),
        in_specs=[IN_VMEM] * (4 + 2 * len(backs) + len(parts)),
        out_specs=IN_VMEM,
        out_shape=jax.ShapeDtypeStruct(resid.shape, resid.dtype),
        scratch_shapes=[pltpu.VMEM(resid.shape, jnp.float32)],
        compiler_params=pltpu.CompilerParams(vmem_limit_bytes=6 << 20),
        name="finish",
    )(slot, weight, resid, gain.reshape(1, -1), *backs, *apart, *parts)


def experts_body(n_src, n_sp, *refs):
    xs, (wg, wu, wd) = refs[:n_src], refs[n_src : n_src + 3]
    outs, sums, (into, outof) = refs[n_src + 3 : 2 * n_src + 3], refs[2 * n_src + 3 : -2], refs[-2:]
    count, (rows, width) = wg.shape[0], xs[0].shape
    apart_from = outs[0].shape[1]
    tiles, left = divmod(rows // count, 8)
    whole = count * tiles * 8
    for s, x in enumerate(xs):
        for j in range(width // LANES):
            cols = slice(j * LANES, (j + 1) * LANES)
            into[j, s * left * count : (s + 1) * left * count, :] = x[whole:, cols].astype(
                jnp.float32
            )

    def one(e, carry):
        starts = [pl.multiple_of((e * tiles + i) * 8, 8) for i in range(tiles)]
        apart = pl.ds(e, n_src * left, stride=count)
        taken = [x[pl.ds(at, 8), :].astype(jnp.float32) for x in xs for at in starts]
        taken.append(jnp.concatenate([into[j, apart, :] for j in range(width // LANES)], axis=1))
        taken = jnp.concatenate(taken, axis=0).astype(jnp.bfloat16)
        gate_pre = jnp.dot(taken, wg[e], preferred_element_type=jnp.float32)
        upward = jnp.dot(taken, wu[e], preferred_element_type=jnp.float32)
        activated = clamped_unit(gate_pre, upward).astype(jnp.bfloat16)
        result = jnp.dot(activated, wd[e], preferred_element_type=jnp.float32)
        row = 0
        for s, out in enumerate(outs):
            block, d = divmod(s, n_sp)
            for at in starts:
                part = result[row : row + 8].astype(out.dtype)
                out[pl.ds(at, 8), :] = part[:, :apart_from]
                sums[block][pl.ds(pl.multiple_of(d * rows + at, 8), 8), :] = part[:, apart_from:]
                row += 8
        for j in range(width // LANES):
            outof[j, apart, :] = result[row:, j * LANES : (j + 1) * LANES]
        return carry

    lax.fori_loop(0, count, one, 0, unroll=EXPERT_UNROLL)
    for s, out in enumerate(outs):
        block, d = divmod(s, n_sp)
        for j in range(width // LANES):
            part = outof[j, s * left * count : (s + 1) * left * count, :].astype(out.dtype)
            first = j * LANES
            if first < apart_from:
                out[whole:, first : first + LANES] = part
            else:
                first -= apart_from
                sums[block][d * rows + whole : (d + 1) * rows, first : first + LANES] = part


EXPERT_UNROLL = 2


def experts(xs, w_gate, w_up, w_down, n_sp, apart_from):
    count, width, hidden = w_gate.shape
    rows, n_src = xs[0].shape[0], len(xs)
    blocks = n_src // n_sp
    left = rows // count % 8
    scratch = pltpu.VMEM((width // LANES, n_src * left * count, LANES), jnp.float32)
    out = jax.ShapeDtypeStruct((rows, apart_from), jnp.bfloat16)
    summed = jax.ShapeDtypeStruct((n_sp * rows, width - apart_from), jnp.bfloat16)
    flops = 6 * n_src * rows * width * hidden
    moved_bytes = 3 * count * width * hidden * 2 + 4 * n_src * rows * width
    cost = pl.CostEstimate(flops=flops, bytes_accessed=moved_bytes, transcendentals=0)
    outs = pl.pallas_call(
        lambda *refs: experts_body(n_src, n_sp, *refs),
        in_specs=[IN_VMEM] * (n_src + 3),
        out_specs=[IN_VMEM] * (n_src + blocks),
        out_shape=[out] * n_src + [summed] * blocks,
        scratch_shapes=[scratch, scratch],
        cost_estimate=cost,
        compiler_params=pltpu.CompilerParams(vmem_limit_bytes=6 << 20),
        name="experts",
    )(*xs, w_gate, w_up, w_down)
    return outs[:n_src], outs[n_src:]


def join_body(n_in, *refs):
    total = sum(x[...].astype(jnp.float32) for x in refs[:n_in])
    outs = refs[n_in:]
    rows = outs[0].shape[0]
    for i, out in enumerate(outs):
        out[...] = total[i * rows : (i + 1) * rows].astype(out.dtype)


def join(arrays, pieces=1):
    rows, width = arrays[0].shape
    out = jax.ShapeDtypeStruct((rows // pieces, width), arrays[0].dtype)
    return pl.pallas_call(
        lambda *refs: join_body(len(arrays), *refs),
        in_specs=[IN_VMEM] * len(arrays),
        out_specs=[IN_VMEM] * pieces,
        out_shape=[out] * pieces,
        compiler_params=pltpu.CompilerParams(vmem_limit_bytes=6 << 20),
        name="join",
    )(*arrays)


def plain_path(
    resid_in,
    pool_input,
    pool_weight,
    pool_scale,
    out_weight,
    mix_gain,
    ffn_gain,
    w_gate,
    w_up,
    w_down,
    routes,
    route_weight,
    post_gain,
):
    n_sp = lax.axis_size("sp")
    n_tp = lax.axis_size("tp")
    tok_rows, width = resid_in.shape
    channels = pool_input.shape[1]
    local_experts = w_gate.shape[0]
    n_experts = local_experts * n_sp
    assert n_experts <= 256
    slot_rows = local_experts * CAP
    slot_total = n_sp * slot_rows

    fields = jnp.concatenate([routes.astype(jnp.bfloat16).T, route_weight.astype(jnp.bfloat16).T])
    n_fields = fields.size
    field_rows = -(-n_fields // (8 * channels)) * 8
    fields = jnp.pad(fields.reshape(-1), (0, field_rows * channels - n_fields))
    fields = jnp.broadcast_to(fields.reshape(1, field_rows, channels), (n_tp, field_rows, channels))
    mixed_rows = mixed_window(pool_input).reshape(n_tp, tok_rows, channels)
    sent = jnp.concatenate([mixed_rows, fields], axis=1)
    got = lax.all_to_all(sent, "tp", split_axis=0, concat_axis=0, tiled=True)
    token_mixed = got[:, :tok_rows].transpose(1, 0, 2).reshape(tok_rows, n_tp * channels)
    fields = got[:, tok_rows:].reshape(n_tp, -1)[:, :n_fields].reshape(n_tp, 2 * TOP, tok_rows)

    pooled = jnp.einsum(
        "tgc,gcd->tgd",
        token_mixed.reshape(tok_rows, GROUPS, GROUP_DIM),
        pool_weight,
        preferred_element_type=jnp.float32,
    )
    pooled = (
        (pooled * pool_scale.reshape(GROUPS, GROUP_DIM)).astype(jnp.bfloat16).reshape(tok_rows, -1)
    )
    mix_out = jnp.dot(pooled, out_weight, preferred_element_type=jnp.float32)
    residual = (resid_in.astype(jnp.float32) + rms_scale(mix_out, mix_gain)).astype(jnp.bfloat16)
    normed = rms_scale(residual.astype(jnp.float32), ffn_gain).astype(jnp.bfloat16)

    far = n_tp // 2
    order = list(range(far + 1)) + list(range(n_tp - 1, far, -1))
    blocks = {0: normed, n_tp: normed}
    for k in order:
        if k:
            by = 1 if k <= far else -1
            blocks[k] = rotated(blocks[k - by], "tp", by)

    here = lax.axis_index("tp")
    fields = jnp.take(fields, (here - jnp.array(order)) % n_tp, axis=0)
    route = fields[:, :TOP].astype(jnp.int32)
    weight = fields[:, TOP:].astype(jnp.float32)
    onehot = route[..., None] == lax.iota(jnp.int32, n_experts)
    named = jnp.sum(onehot.astype(jnp.float32), axis=1)
    earlier = lax.iota(jnp.int32, tok_rows)[:, None] > lax.iota(jnp.int32, tok_rows)[None, :]
    rank = jnp.einsum(
        "ut,bte->bue",
        earlier.astype(jnp.bfloat16),
        named.astype(jnp.bfloat16),
        preferred_element_type=jnp.float32,
    )
    slot_rank = jnp.sum(rank[:, None] * onehot, axis=-1).astype(jnp.int32)

    slot_index = route * CAP + slot_rank
    picker = slot_index[..., None] == lax.iota(jnp.int32, slot_total)
    token_pick = jnp.sum(picker.astype(jnp.float32), axis=1).astype(jnp.bfloat16)
    token_weight = jnp.sum(jnp.where(picker, weight[..., None], 0.0), axis=1)
    token_weight = token_weight.astype(jnp.bfloat16)
    arrived = []
    for at, k in enumerate(order):
        rows = lax.dot_general(
            token_pick[at],
            blocks[k],
            (((0,), (0,)), ((), ())),
            preferred_element_type=jnp.float32,
        )
        rows = rows.astype(jnp.bfloat16).reshape(n_sp, slot_rows, width)
        arrived.append(lax.all_to_all(rows, "sp", split_axis=0, concat_axis=0, tiled=True))
    arrived = jnp.stack(arrived).reshape(n_tp, n_sp, local_experts, CAP, width)
    f32 = {"preferred_element_type": jnp.float32}
    gate_pre = jnp.einsum("sklcd,ldf->sklcf", arrived, w_gate, **f32)
    upward = jnp.einsum("sklcd,ldf->sklcf", arrived, w_up, **f32)
    activated = clamped_unit(gate_pre, upward).astype(jnp.bfloat16)
    terms = jnp.einsum("sklcf,lfd->sklcd", activated, w_down, **f32)
    terms = terms.astype(jnp.bfloat16).reshape(n_tp, n_sp, slot_rows, width)
    parts = {}
    for at, k in enumerate(order):
        back = lax.all_to_all(terms[at], "sp", split_axis=0, concat_axis=0, tiled=True)
        part = jnp.dot(token_weight[at], back.reshape(slot_total, width), **f32)
        part = part.astype(jnp.bfloat16)
        parts[k] = rotated(part, "tp", -k) if k else part
    expert_mix = sum(parts[k].astype(jnp.float32) for k in order)
    return (residual.astype(jnp.float32) + rms_scale(expert_mix, post_gain)).astype(jnp.bfloat16)


AHEAD = 16


def cut_body(place, x, routes, weights, *refs):
    (own_routes, own_weights, done), (*chunks, tail) = refs[-3:], refs[:-3]
    n_tp, (top, rows) = len(chunks), routes.shape
    moves = [(routes, own_routes), (weights, own_weights)]
    for k, chunk in enumerate(chunks):
        first = (place[0] % n_tp + k) % n_tp * rows
        before = pl.multiple_of(jnp.maximum(first - AHEAD, 0), AHEAD)
        first = pl.multiple_of(first, AHEAD)
        moves.append((x.at[pl.ds(first, rows), :], chunk.at[pl.ds(AHEAD, rows), :]))
        moves.append((x.at[pl.ds(before, AHEAD), :], chunk.at[pl.ds(0, AHEAD), :]))
    moves.append((x.at[pl.ds(x.shape[0] - AHEAD, AHEAD), :], tail))
    copies = [pltpu.make_async_copy(a, b, done.at[i]) for i, (a, b) in enumerate(moves)]
    for copy in copies:
        copy.start()
    for copy in copies:
        copy.wait()
    fields = [own_routes[...].astype(jnp.float32), own_weights[...]]
    fields.append(jnp.zeros((8 - 2 * top, rows), jnp.float32))
    fields = jnp.concatenate(fields, axis=0).astype(jnp.bfloat16)
    for chunk in chunks:
        chunk[AHEAD + rows :, :] = jnp.zeros((8, chunk.shape[1]), jnp.bfloat16)
        chunk[AHEAD + rows :, :rows] = fields


def cut(place, x, routes, weights, n_tp):
    rows, channels = routes.shape[1], x.shape[1]
    chunk = jax.ShapeDtypeStruct((AHEAD + rows + 8, channels), x.dtype)
    return pl.pallas_call(
        cut_body,
        in_specs=[IN_SMEM] + [pl.BlockSpec(memory_space=pltpu.HBM)] * 3,
        out_specs=[IN_VMEM] * (n_tp + 1),
        out_shape=[pltpu.VMEM(chunk.shape, x.dtype)] * n_tp
        + [pltpu.VMEM((AHEAD, channels), x.dtype)],
        scratch_shapes=[
            pltpu.VMEM(routes.shape, routes.dtype),
            pltpu.VMEM(weights.shape, weights.dtype),
            pltpu.SemaphoreType.DMA((2 * n_tp + 3,)),
        ],
        compiler_params=pltpu.CompilerParams(vmem_limit_bytes=CUT_LIMIT << 20),
        name="cut",
    )(place, x, routes, weights)


def mix_body(n_tp, place, *refs):
    chunks, halos = refs[:n_tp], refs[n_tp : 2 * n_tp]
    pool_w, scale, out_w, mix_gain, ffn_gain, resid = refs[2 * n_tp : 2 * n_tp + 6]
    residual, normed, raw, pooled, mix = refs[2 * n_tp + 6 :]
    rows, width = resid.shape
    channels = chunks[0].shape[1]
    tp, sp = place[0] % n_tp, place[0] // n_tp
    for k, chunk in enumerate(chunks):
        source = (tp - k + n_tp) % n_tp
        cols = pl.ds(pl.multiple_of(source * channels, LANES), channels)
        raw[:, cols] = chunk[: AHEAD + rows, :].astype(jnp.float32)

    @pl.when(tp == 0)
    def _():
        for j, halo in enumerate(halos):
            raw[:AHEAD, j * channels : (j + 1) * channels] = halo[...].astype(jnp.float32)

    start = (sp * n_tp + tp) * rows
    position = start + lax.broadcasted_iota(jnp.int32, (rows, GROUP_DIM), 0) + 1
    for g, window in enumerate(pool_windows):
        cols = slice(g * GROUP_DIM, (g + 1) * GROUP_DIM)
        own = raw[:, cols]
        total, reach = own, 1
        while reach < window:
            total = total + pltpu.roll(total, reach, 0)
            reach = 2 * reach
        divisor = jnp.minimum(position, window).astype(jnp.float32)
        mixed = (total[AHEAD:] / divisor - own[AHEAD:]).astype(jnp.bfloat16)
        part = jnp.dot(mixed, pool_w[g], preferred_element_type=jnp.float32)
        pooled[:, cols] = (part * scale[:, cols]).astype(jnp.bfloat16)

    def columns():
        return [slice(j, j + 2 * LANES) for j in range(0, width, 2 * LANES)]

    def inverse_of(square):
        return lax.rsqrt(jnp.sum(square, axis=1, keepdims=True) / width + norm_eps)

    square = jnp.zeros((rows, LANES), jnp.float32)
    for cols in columns():
        part = jnp.dot(pooled[...], out_w[:, cols], preferred_element_type=jnp.float32)
        mix[:, cols] = part
        square = square + part[:, :LANES] * part[:, :LANES] + part[:, LANES:] * part[:, LANES:]
    inverse = inverse_of(square)
    square = jnp.zeros((rows, LANES), jnp.float32)
    for cols in columns():
        part = resid[:, cols].astype(jnp.float32) + mix[:, cols] * inverse * mix_gain[:, cols]
        part = part.astype(jnp.bfloat16)
        residual[:, cols] = part
        part = part.astype(jnp.float32)
        square = square + part[:, :LANES] * part[:, :LANES] + part[:, LANES:] * part[:, LANES:]
    inverse = inverse_of(square)
    for cols in columns():
        part = residual[:, cols].astype(jnp.float32) * inverse * ffn_gain[:, cols]
        normed[:, cols] = part.astype(normed.dtype)


def mix_tokens(place, chunks, halos, pool_w, scale, out_w, mix_gain, ffn_gain, resid):
    rows, width = resid.shape
    total = out_w.shape[0]
    return pl.pallas_call(
        lambda *refs: mix_body(len(chunks), *refs),
        in_specs=[IN_SMEM] + [IN_VMEM] * (2 * len(chunks) + 6),
        out_specs=[IN_VMEM] * 2,
        out_shape=[jax.ShapeDtypeStruct(resid.shape, resid.dtype)] * 2,
        scratch_shapes=[
            pltpu.VMEM((AHEAD + rows, total), jnp.float32),
            pltpu.VMEM((rows, total), jnp.bfloat16),
            pltpu.VMEM((rows, width), jnp.float32),
        ],
        compiler_params=pltpu.CompilerParams(vmem_limit_bytes=12 << 20),
        name="mix",
    )(
        place,
        *chunks,
        *halos,
        pool_w,
        scale,
        out_w,
        mix_gain,
        ffn_gain,
        resid,
    )


def slots_body(n_sp, local, place, *refs):
    chunks, (slot, by_row, weight) = refs[:-3], refs[-3:]
    top, tokens = slot.shape[1], slot.shape[2]
    n_experts = n_sp * local
    expert = lax.broadcasted_iota(jnp.int32, (n_experts, tokens), 0)
    row = lax.broadcasted_iota(jnp.int32, (tokens, tokens), 0)
    lane = lax.broadcasted_iota(jnp.int32, (tokens, tokens), 1)
    before = jnp.where(row < lane, 1.0, 0.0).astype(jnp.bfloat16)
    whole = CAP // 8 * 8
    for at, chunk in enumerate(chunks):
        first = chunk.shape[0] - 8
        fields = chunk[first:, :tokens].astype(jnp.float32)
        hits = [
            jnp.where(expert == fields[k : k + 1].astype(jnp.int32), 1.0, 0.0) for k in range(top)
        ]
        named = sum(hits).astype(jnp.bfloat16)
        rank = jnp.dot(named, before, preferred_element_type=jnp.float32)
        found = []
        for k, hit in enumerate(hits):
            mine = jnp.sum(rank * hit, axis=0, keepdims=True).astype(jnp.int32)
            route = jnp.sum(expert.astype(jnp.float32) * hit, axis=0, keepdims=True)
            owner = jnp.sum(
                (expert // local).astype(jnp.float32) * hit, axis=0, keepdims=True
            ).astype(jnp.int32)
            inside = route.astype(jnp.int32) - owner * local
            owner = offset_to(owner, place[0] // len(chunks), n_sp)
            in_tile = inside * whole + mine
            apart = local * whole + (mine - whole) * local + inside
            found.append(owner * local * CAP + jnp.where(mine < whole, in_tile, apart))
            slot[at, k : k + 1, :] = found[-1]
        rows8 = [x.astype(jnp.float32) for x in found] + [fields[top : 2 * top]]
        rows8.append(jnp.zeros((tokens - 2 * top, tokens), jnp.float32))
        turned = jnp.concatenate(rows8, axis=0).T
        by_row[at] = turned[:, :top].astype(jnp.int32)
        weight[at] = turned[:, top : 2 * top]


def slots(place, chunks, n_sp, local, top, tokens):
    n = len(chunks)
    return pl.pallas_call(
        lambda *refs: slots_body(n_sp, local, *refs),
        in_specs=[IN_SMEM] + [IN_VMEM] * n,
        out_specs=[IN_VMEM] * 3,
        out_shape=[
            jax.ShapeDtypeStruct((n, top, tokens), jnp.int32),
            jax.ShapeDtypeStruct((n, tokens, top), jnp.int32),
            jax.ShapeDtypeStruct((n, tokens, top), jnp.float32),
        ],
        compiler_params=pltpu.CompilerParams(vmem_limit_bytes=6 << 20),
        name="slots",
    )(place, *chunks)


def kernel_path(
    resid_in,
    pool_input,
    pool_weight,
    pool_scale,
    out_weight,
    mix_gain,
    ffn_gain,
    w_gate,
    w_up,
    w_down,
    routes,
    route_weight,
    post_gain,
):
    n_sp = lax.axis_size("sp")
    n_tp = lax.axis_size("tp")
    tok_rows = resid_in.shape[0]
    local_experts = w_gate.shape[0]
    slot_rows = local_experts * CAP

    place = (lax.axis_index("sp") * n_tp + lax.axis_index("tp")).reshape(1)
    *chunks, tail = cut(place, pool_input, routes.T, route_weight.T, n_tp)
    halos = []
    for j in range(n_tp):
        pairs = [(s * n_tp + j, (s + 1) * n_tp) for s in range(n_sp - 1)]
        halos.append(lax.ppermute(tail, ("sp", "tp"), pairs))
    chunks = [rotated(x, "tp", k) if k else x for k, x in enumerate(chunks)]
    small = [x.reshape(1, -1) for x in (pool_scale, mix_gain, ffn_gain)]
    scale, mix_gain, ffn_gain, pool_weight, out_weight, resid_in = load(
        *small, pool_weight, out_weight, resid_in, limit=EARLY_LIMIT
    )
    residual, normed = mix_tokens(
        place, chunks, halos, pool_weight, scale, out_weight, mix_gain, ffn_gain, resid_in
    )

    far = n_tp // 2
    order = list(range(far + 1)) + list(range(n_tp - 1, far, -1))
    blocks = {0: normed, n_tp: normed}
    for k in order:
        if k:
            by = 1 if k <= far else -1
            blocks[k] = rotated(blocks[k - by], "tp", by)

    slot, by_row, weight = slots(
        place, [chunks[k] for k in order], n_sp, local_experts, TOP, tok_rows
    )
    weights = load(w_gate, w_up, w_down)
    arrived, backs, parts = [], {}, {}
    for at, k in enumerate(order):
        rows = pick(at, slot, blocks[k], n_sp, slot_rows)
        arrived.append([moved(x, "sp", d) if d else x for d, x in enumerate(rows)])
    apart_from = apart_column(resid_in.shape[1])
    sums = []
    for first, stop in groups_of(n_tp):
        group = arrived[first:stop]
        xs = [x for xs in group for x in xs]
        terms, summed = experts(xs, *weights, n_sp, apart_from)
        sums += summed
        for at in range(first, stop):
            back = terms[(at - first) * n_sp : (at - first + 1) * n_sp]
            backs[at] = [moved(x, "sp", d, True) if d else x for d, x in enumerate(back)]
    passed = {}
    for at in return_order(n_tp)[:-1]:
        k = order[at]
        by = -1 if k <= far else 1
        inner = k < far or k > far + 1
        part = join([sums[at], passed.pop(k - by)])[0] if inner else sums[at]
        passed[k] = rotated(part, "tp", by)
    apart = join([sums[0], *passed.values()], n_sp)
    apart = [moved(x, "sp", d, True) if d else x for d, x in enumerate(apart)]
    for at in return_order(n_tp)[:-1]:
        k = order[at]
        by = -1 if k <= far else 1
        inner = k < far or k > far + 1
        joined = [parts.pop(k - by)] if inner else []
        part = combine(at, by_row, weight, backs[at], joined)
        parts[k] = rotated(part, "tp", by)
    return finish(
        0, by_row, weight, residual, post_gain, backs[0], apart, list(parts.values())
    )


def per_device(*args):
    pool_input, w_gate, routes = args[1], args[7], args[10]
    n_sp = lax.axis_size("sp")
    fits = w_gate.shape[0] % 8 == 0 and CAP % 8 and n_sp <= 4 and w_gate.shape[0] * n_sp <= 256
    fits = fits and routes.shape[0] == LANES and pool_input.shape[1] % LANES == 0
    return kernel_path(*args) if fits else plain_path(*args)


def groups_of(n_tp):
    first = min(2, n_tp)
    return [(0, first)] + [(at, at + 1) for at in range(first, n_tp)]


def apart_column(width):
    step = 2 * LANES
    return width - width * APART // (8 * step) * step


APART = 3


def return_order(n_tp):
    far = n_tp // 2
    return list(range(far, 0, -1)) + list(range(far + 1, n_tp)) + [0]


def solution(mesh):
    in_specs = (
        P(("grp", "sp", "tp"), None),
        P(("grp", "sp"), "tp"),
        P(),
        P(),
        P(),
        P(),
        P(),
        P("sp", None, "tp"),
        P("sp", None, "tp"),
        P("sp", "tp", None),
        P(("grp", "sp", "tp"), None),
        P(("grp", "sp", "tp"), None),
        P(),
    )
    out_specs = P(("grp", "sp", "tp"), None)

    return jax.shard_map(
        per_device, mesh=mesh, in_specs=in_specs, out_specs=out_specs, check_vma=False
    )
```
